32 devices in a mesh: ep: 4 (over y, x), tp: 8 (over z, core).
Axes of the slice: x: 2, y: 2, z: 4, core: 2. Of those that a mesh axis runs over, the one named last changes fastest.
Arguments:
- query_heads: bfloat16 [1024, 2048], P('ep', 'tp'), may hold values from -60 to 60
- key_heads: bfloat16 [1024, 2048], P('ep', 'tp'), may hold values from -40.5 to 40.5
- value_heads: bfloat16 [1024, 2048], P('ep', 'tp'), may hold values from -6 to 6
- diff_lambda: float32 [16], P('tp'), may hold values from 0.3 to 0.8
- sub_gain: float32 [128], replicated, may hold values from 0.1 to 1.9
- out_weight: bfloat16 [2048, 4096], P('tp'), may hold values from -0.125 to 0.125
- routed_input: bfloat16 [1024, 4096], P('ep', 'tp'), may hold values from -40 to 40
- routes: int32 [1024, 2], P('ep'), may hold values from 0 to 3, all different within a row; in each aligned block of 256 rows (0 to 255, 256 to 511, ...) at most 256 rows name the same one
- route_weights: float32 [1024, 2], P('ep'), may hold values from 0.3 to 1.5
- expert_gate: bfloat16 [4, 4096, 4096], P('ep', None, 'tp'), may hold values from -0.09375 to 0.09375
- expert_up: bfloat16 [4, 4096, 4096], P('ep', None, 'tp'), may hold values from -0.09375 to 0.09375
- expert_down: bfloat16 [4, 4096, 4096], P('ep', 'tp'), may hold values from -0.09375 to 0.09375
- shared_gate: bfloat16 [4096, 2048], P(None, 'tp'), may hold values from -0.09375 to 0.09375
- shared_up: bfloat16 [4096, 2048], P(None, 'tp'), may hold values from -0.09375 to 0.09375
- shared_down: bfloat16 [2048, 4096], P('tp'), may hold values from -0.125 to 0.125
Outputs:
- mixer_output: bfloat16 [1024, 4096], P('ep', 'tp')
- routed_output: bfloat16 [1024, 4096], P('ep', 'tp')
The draws below stay inside these ranges and needn't reach their ends.
Inputs may be any that keep to these rules, and one draw needn't show every extreme that they name: `routes`: each row names 2 different experts. In each aligned block of 256 rows no expert is named by more than 256 rows, a bound that some block reaches.
All inputs are finite; a program needn't handle non-finite values.
Results may differ from the reference program's by a relative error of at most 0.02.
Values may be sent and summed in bfloat16 or wider, within the bound.
A program may use at most 128 MiB of HBM per device.

```python
import math
import jax
import jax.numpy as jnp
import numpy as np
from jax import lax

D = 4096
HEADS = 16
QK = 64
VD = 128
FF = 4096
FS = 2048
TOPK = 2
EXPERTS = 4
ROWS_B = 256
TOKENS_A = 1024
TOKENS_B = 1024
CAP = 256
N_EP = 4
N_TP = 8


def draw_query_heads(key, part):
    base_key = jax.random.fold_in(jax.random.fold_in(key, 11), 0)
    values = 1.3 * jnp.clip(jax.random.normal(base_key, (TOKENS_A, HEADS * 2 * QK), jnp.float32), -6.0, 6.0)
    return values.astype(jnp.bfloat16)


def draw_key_heads(key, part):
    base_key = jax.random.fold_in(jax.random.fold_in(key, 23), 0)
    values = 1.3 * jnp.clip(jax.random.normal(base_key, (TOKENS_A, HEADS * 2 * QK), jnp.float32), -6.0, 6.0)
    return values.astype(jnp.bfloat16)


def draw_routed_input(key, part):
    base_key, row_key = jax.random.split(jax.random.fold_in(key, 37))
    column_pos = jnp.arange(D, dtype=jnp.float32)[None, :] / D
    column_scale = 0.6 * jnp.exp(column_pos * jnp.log(3.0))
    row_scale = jnp.exp(jax.random.uniform(row_key, (TOKENS_B, 1), jnp.float32, jnp.log(0.7), jnp.log(1.4)))
    entries = jnp.clip(jax.random.normal(base_key, (TOKENS_B, D), jnp.float32), -6.0, 6.0)
    return (entries * column_scale * row_scale).astype(jnp.bfloat16)


def level_of(stream_key, shape, cuts, low, top_value):
    loudness = 1.0
    for axis_at, shards_of in cuts:
        draws = jax.random.uniform(jax.random.fold_in(jax.random.fold_in(stream_key, 6), axis_at), (shards_of,), jnp.float32, low / len(cuts), top_value / len(cuts))
        loudness = loudness * jnp.repeat(jnp.exp(draws), shape[axis_at] // shards_of).reshape((-1,) + (1,) * (len(shape) - 1 - axis_at))
    return loudness


def deal_out(rng, own, number, rows, amount, top, bound, lean):
    sequence = jax.random.permutation(rng, amount)
    heavy_load, common = shares(amount, rows * top, bound, lean, True), shares(amount, rows * top, bound, lean, False)
    places = jnp.arange(amount)

    def named(tallies, rotation):
        used = int((tallies > 0).sum())
        fixed = max(1, used // 4)
        passed = fixed + (places - fixed + rotation * (used - fixed)) % max(1, amount - fixed)
        return jnp.zeros((amount,), jnp.int32).at[sequence[jnp.where(places < fixed, places, passed)]].set(jnp.asarray(tallies, jnp.int32))

    tallies = jnp.where(number % 4 == 0, named(heavy_load, number // 4), named(common, number - number // 4 - 1))
    mixed = jax.random.permutation(jax.random.fold_in(own, 3), amount)
    giver, receiver = mixed[0:amount // 2 * 2:2], mixed[1:amount // 2 * 2:2]
    slack = jnp.minimum(tallies[giver] - 1, bound - tallies[receiver]) // 2
    slack = jnp.where((giver == sequence[0]) | (receiver == sequence[0]) | (tallies[receiver] == 0), 0, jnp.maximum(slack, 0))
    passed = jax.random.randint(jax.random.fold_in(own, 4), (amount // 2,), 0, 1 << 20) % (slack + 1)
    tallies = tallies.at[giver].add(-passed).at[receiver].add(passed)
    items = jnp.searchsorted(jnp.cumsum(tallies), jnp.arange(rows * top), side="right").astype(jnp.int32)
    grid = items.reshape(top, rows).T
    grid = grid[jax.random.permutation(jax.random.fold_in(own, 1), rows)]
    rotation = jax.random.randint(jax.random.fold_in(own, 2), (rows, 1), 0, top)
    return jnp.take_along_axis(grid, (jnp.arange(top)[None, :] + rotation) % top, axis=1)


def shares(amount, total, limit, skew, full):
    weights = [(1 << 20) // math.isqrt(rank ** skew) + 1 for rank in range(1, amount + 1)]
    largest = limit if full else min(limit, max(-(-total // amount), total * weights[0] // sum(weights)))
    least = 1 if total - largest >= amount - 1 else 0
    given, spare = [largest] + [least] * (amount - 1), total - largest - least * (amount - 1)
    while spare > 0:
        candidates = [i for i in range(1, amount) if given[i] < largest] or [i for i in range(1, amount) if given[i] < limit]
        pool, budget = sum([weights[i] for i in candidates]), spare
        for i in candidates:
            more = min(limit - given[i], max(1, budget * weights[i] // pool), spare)
            given[i] = given[i] + more
            spare = spare - more
    return np.array(given)


def normal_values(key, extent, deviation, bound, pieces=(), kind=jnp.bfloat16):
    drawn = jax.random.normal(key, extent, jnp.float32) * deviation
    if len(pieces) > 0:
        drawn = level_of(key, extent, pieces, -0.22, 0.18) * drawn
    return jnp.clip(drawn, min=-bound, max=bound).astype(kind)


def setup_inputs(seed: int = 0) -> dict:
    arg_keys = jax.random.split(jax.random.key(seed), 16)
    query_heads = draw_query_heads(jax.random.fold_in(arg_keys[15], 71), 0)
    key_heads = draw_key_heads(jax.random.fold_in(arg_keys[15], 71), 0)
    value_heads = normal_values(arg_keys[2], (TOKENS_A, HEADS * VD), 1.0, 6.0, ((0, 4), (1, 8)))
    diff_lambda = jnp.clip(0.3 + 0.5 * jax.random.uniform(arg_keys[3], (HEADS,), jnp.float32) ** level_of(arg_keys[3], (HEADS,), ((0, 8),), -0.2, 0.2), 0.3, 0.8)
    sub_gain = jnp.clip(1.0 + 0.18 * jax.random.normal(arg_keys[4], (VD,), jnp.float32), 0.1, 1.9)
    out_weight = normal_values(arg_keys[5], (HEADS * VD, D), (HEADS * VD) ** -0.5, 0.125, ((0, 8),))
    routed_input = draw_routed_input(jax.random.fold_in(arg_keys[15], 71), 0)
    routes_keys = jax.random.split(jax.random.fold_in(arg_keys[7], 1), TOKENS_B // ROWS_B)
    routes_turns = jax.random.permutation(jax.random.fold_in(arg_keys[7], 3), TOKENS_B // ROWS_B)
    routes = jax.vmap(lambda own, number: deal_out(jax.random.fold_in(arg_keys[7], 2), own, number, ROWS_B, EXPERTS, TOPK, CAP, 2))(routes_keys, routes_turns).reshape((TOKENS_B, TOPK))
    route_weights = jnp.clip(jnp.exp(math.log(1.5) - 1.60943787 * jax.random.uniform(arg_keys[8], (TOKENS_B, TOPK), jnp.float32) ** level_of(arg_keys[8], (TOKENS_B, TOPK), ((0, 4),), -0.2, 0.2)), 0.3, 1.5)
    expert_gate = normal_values(arg_keys[9], (EXPERTS, D, FF), D ** -0.5, 0.09375, ((0, 4), (2, 8)))
    expert_up = normal_values(arg_keys[10], (EXPERTS, D, FF), D ** -0.5, 0.09375, ((0, 4), (2, 8)))
    expert_down = normal_values(arg_keys[11], (EXPERTS, FF, D), FF ** -0.5, 0.09375, ((0, 4), (1, 8)))
    shared_gate = normal_values(arg_keys[12], (D, FS), D ** -0.5, 0.09375, ((1, 8),))
    shared_up = normal_values(arg_keys[13], (D, FS), D ** -0.5, 0.09375, ((1, 8),))
    shared_down = normal_values(arg_keys[14], (FS, D), FS ** -0.5, 0.125, ((0, 8),))
    return {"query_heads": query_heads, "key_heads": key_heads, "value_heads": value_heads, "diff_lambda": diff_lambda, "sub_gain": sub_gain, "out_weight": out_weight, "routed_input": routed_input, "routes": routes, "route_weights": route_weights, "expert_gate": expert_gate, "expert_up": expert_up, "expert_down": expert_down, "shared_gate": shared_gate, "shared_up": shared_up, "shared_down": shared_down}


ROPE_BASE = 10000.0
NORM_EPS = 1e-06
MASKED = -1e+30

def rotate(values, positions):
    half_width = values.shape[-1] // 2
    inverse_freq = ROPE_BASE ** (-jnp.arange(half_width, dtype=jnp.float32) / half_width)
    angles = positions.astype(jnp.float32)[:, None] * inverse_freq[None, :]
    angles = angles.reshape((angles.shape[0],) + (1,) * (values.ndim - 2) + (half_width,))
    cosine = jnp.cos(angles)
    sine_part = jnp.sin(angles)
    lower = values[..., :half_width]
    upper = values[..., half_width:]
    return jnp.concatenate([lower * cosine - upper * sine_part, upper * cosine + lower * sine_part], axis=-1)

def split_sum(left, right, groups):
    group_width = left.shape[1] // groups

    def add_group(summed, group_index):
        left_part = lax.dynamic_slice_in_dim(left, group_index * group_width, group_width, 1)
        right_part = lax.dynamic_slice_in_dim(right, group_index * group_width, group_width, 0)
        rounded = jnp.dot(left_part, right_part, preferred_element_type=jnp.float32).astype(jnp.bfloat16)
        rounded = lax.optimization_barrier(rounded)
        return (summed + rounded.astype(jnp.float32), None)
    start_sum = jnp.zeros((left.shape[0], right.shape[1]), jnp.float32)
    summed, _ = lax.scan(add_group, start_sum, jnp.arange(groups, dtype=jnp.int32))
    return summed

def attend_head(query_head, key_head, value_head, lambda_head, sub_gain):
    seq_len = query_head.shape[0]
    query_block = 512 if seq_len % 512 == 0 else seq_len
    score_scale = query_head.shape[-1] ** (-0.5)
    key_positions = jnp.arange(seq_len, dtype=jnp.int32)

    def one_block(block_index):
        block_start = block_index * query_block
        query_rows = lax.dynamic_slice_in_dim(query_head, block_start, query_block, 0)
        query_positions = block_start + jnp.arange(query_block, dtype=jnp.int32)
        visible = key_positions[None, :] <= query_positions[:, None]
        attended = []
        for which_map in range(2):
            scores = jnp.dot(query_rows[:, which_map], key_head[:, which_map].T, preferred_element_type=jnp.float32) * score_scale
            scores = jnp.where(visible, scores, MASKED)
            maxima = lax.optimization_barrier(jnp.max(scores, axis=1, keepdims=True))
            exp_weights = jnp.where(visible, jnp.exp(scores - maxima), 0.0)
            totals = lax.optimization_barrier(jnp.sum(exp_weights, axis=1, keepdims=True))
            weighted = jnp.dot(exp_weights.astype(jnp.bfloat16), value_head, preferred_element_type=jnp.float32)
            attended.append(weighted / totals)
        mixed_heads = attended[0] - lambda_head * attended[1]
        normed = mixed_heads * lax.rsqrt(lax.optimization_barrier(jnp.mean(mixed_heads * mixed_heads, axis=1, keepdims=True)) + NORM_EPS) * sub_gain
        return normed.astype(jnp.bfloat16)
    blocks = lax.map(one_block, jnp.arange(seq_len // query_block, dtype=jnp.int32))
    return blocks.reshape(seq_len, value_head.shape[1])

def expert_apply(token_rows, gate_weight, up_weight, down_weight):
    squares = lax.optimization_barrier(jnp.sum(jnp.square(token_rows.astype(jnp.float32)), axis=1, keepdims=True))
    factor = lax.rsqrt(squares / token_rows.shape[1] + NORM_EPS)
    gate_value = jnp.dot(token_rows, gate_weight, preferred_element_type=jnp.float32) * factor
    up_value = jnp.dot(token_rows, up_weight, preferred_element_type=jnp.float32) * factor
    hidden = (jax.nn.silu(gate_value) * up_value).astype(jnp.bfloat16)
    return split_sum(hidden, down_weight, N_TP)

def slot_table(routes, block_rows, capacity, experts):
    token_count, top_count = routes.shape
    block_total = token_count // block_rows
    grouped = routes.reshape(block_total, block_rows * top_count)
    onehot = (grouped[:, :, None] == jnp.arange(experts, dtype=jnp.int32)[None, None, :]).astype(jnp.int32)
    earlier = jnp.cumsum(onehot, axis=1) - onehot
    rank_within = lax.optimization_barrier(jnp.sum(earlier * onehot, axis=2))
    block_ids = jnp.arange(block_total, dtype=jnp.int32)[:, None]
    slot_index = grouped * (block_total * capacity) + block_ids * capacity + rank_within
    return slot_index.reshape(token_count * top_count)

def reference(query_heads, key_heads, value_heads, diff_lambda, sub_gain, out_weight, routed_input, routes, route_weights, expert_gate, expert_up, expert_down, shared_gate, shared_up, shared_down):
    seq_len = query_heads.shape[0]
    positions = jnp.arange(seq_len, dtype=jnp.int32)
    query_rot = rotate(query_heads.astype(jnp.float32).reshape(seq_len, HEADS, 2, QK), positions).astype(jnp.bfloat16)
    key_rot = rotate(key_heads.astype(jnp.float32).reshape(seq_len, HEADS, 2, QK), positions).astype(jnp.bfloat16)
    value_split = value_heads.reshape(seq_len, HEADS, VD)
    per_head = lax.map(lambda head_item: attend_head(head_item[0], head_item[1], head_item[2], head_item[3], sub_gain), (jnp.transpose(query_rot, (1, 0, 2, 3)), jnp.transpose(key_rot, (1, 0, 2, 3)), jnp.transpose(value_split, (1, 0, 2)), diff_lambda))
    heads_out = jnp.transpose(per_head, (1, 0, 2)).reshape(seq_len, HEADS * VD)
    mixer_output = split_sum(heads_out, out_weight, N_TP).astype(jnp.bfloat16)
    token_count = routed_input.shape[0]
    copies = token_count * TOPK
    slot_of_copy = slot_table(routes, ROWS_B, CAP, EXPERTS)
    per_expert = N_EP * CAP
    copy_token = jnp.arange(copies, dtype=jnp.int32) // TOPK
    token_table = jnp.zeros((EXPERTS * per_expert,), jnp.int32).at[slot_of_copy].set(copy_token)
    filled = jnp.zeros((EXPERTS * per_expert,), jnp.bfloat16).at[slot_of_copy].set(jnp.ones((copies,), jnp.bfloat16))
    gathered_rows = routed_input[token_table] * filled[:, None]
    expert_rows = gathered_rows.reshape(EXPERTS, per_expert, D)
    results = lax.map(lambda expert_item: expert_apply(expert_item[0], expert_item[1], expert_item[2], expert_item[3]), (expert_rows, expert_gate, expert_up, expert_down))
    results = results.astype(jnp.bfloat16).reshape(EXPERTS * per_expert, D)
    copy_results = results[slot_of_copy].reshape(token_count, TOPK, D)
    routed = lax.optimization_barrier(jnp.sum(copy_results.astype(jnp.float32) * route_weights[:, :, None], axis=1))
    shared_result = expert_apply(routed_input, shared_gate, shared_up, shared_down)
    routed_output = (routed + shared_result).astype(jnp.bfloat16)
    return (mixer_output, routed_output)
```

```python
import functools

import jax
import jax.numpy as jnp
import numpy as np
from jax import lax
from jax.experimental import pallas as pl
from jax.experimental.pallas import tpu as pltpu
from jax.sharding import PartitionSpec as P

ROPE_BASE = 10000.0
NORM_EPS = 1e-06
MASKED = -1e30


def rotate(values, positions):
    half_width = values.shape[-1] // 2
    inverse_freq = ROPE_BASE ** (-jnp.arange(half_width, dtype=jnp.float32) / half_width)
    angles = positions.astype(jnp.float32)[:, None] * inverse_freq[None, :]
    angles = angles.reshape((angles.shape[0],) + (1,) * (values.ndim - 2) + (half_width,))
    cosine = jnp.cos(angles)
    sine_part = jnp.sin(angles)
    lower = values[..., :half_width]
    upper = values[..., half_width:]
    return jnp.concatenate(
        [lower * cosine - upper * sine_part, upper * cosine + lower * sine_part], axis=-1
    )


def mixer_terms(query_heads, key_heads, value_heads, diff_lambda, sub_gain, out_weight):
    row_count = query_heads.shape[0]
    local_heads = diff_lambda.shape[0]
    value_width = value_heads.shape[1] // local_heads
    key_width = query_heads.shape[1] // (2 * local_heads)
    score_scale = key_width ** (-0.5)
    offset = lax.axis_index("ep") * row_count
    positions = offset + jnp.arange(row_count, dtype=jnp.int32)
    last_row = offset + row_count - 1
    query_rot = rotate(
        query_heads.astype(jnp.float32).reshape(row_count, local_heads, 2, key_width), positions
    ).astype(jnp.bfloat16)
    queries = jnp.transpose(query_rot, (1, 2, 0, 3))
    key_rot = (
        rotate(
            key_heads.astype(jnp.float32).reshape(row_count, local_heads, 2, key_width), positions
        )
        .astype(jnp.bfloat16)
        .reshape(row_count, local_heads * 2 * key_width)
    )
    start_state = (
        jnp.full((local_heads, 2, row_count), MASKED, jnp.float32),
        jnp.zeros((local_heads, 2, row_count), jnp.float32),
        jnp.zeros((local_heads, 2, row_count, value_width), jnp.float32),
    )
    carried = start_state
    key_piece = lax.all_gather(key_rot, "ep", axis=0, tiled=True)
    value_piece = lax.all_gather(value_heads, "ep", axis=0, tiled=True)
    piece_rows = key_piece.shape[0]
    key_block = 512
    block_count = piece_rows // key_block
    key_blocks = key_piece.reshape(block_count, key_block, local_heads, 2, key_width)
    value_blocks = value_piece.reshape(block_count, key_block, local_heads, value_width)

    def block_step(running, block_item):
        key_rows, value_rows, block_index = block_item
        block_start = block_index * key_block

        def attend_block(partial_state):
            maxima, totals, weighted = partial_state
            key_positions = block_start + jnp.arange(key_block, dtype=jnp.int32)
            visible = key_positions[None, :] <= positions[:, None]
            scores = (
                jnp.einsum("hmqd,khmd->hmqk", queries, key_rows, preferred_element_type=jnp.float32)
                * score_scale
            )
            scores = jnp.where(visible, scores, MASKED)
            new_maxima = jnp.maximum(maxima, jnp.max(scores, axis=3))
            exp_weights = jnp.where(visible, jnp.exp(scores - new_maxima[..., None]), 0.0)
            shrink = jnp.exp(maxima - new_maxima)
            new_totals = totals * shrink + jnp.sum(exp_weights, axis=3)
            update = jnp.einsum(
                "hmqk,khw->hmqw",
                exp_weights.astype(jnp.bfloat16),
                value_rows,
                preferred_element_type=jnp.float32,
            )
            return (new_maxima, new_totals, weighted * shrink[..., None] + update)

        return (
            lax.cond(
                block_start <= last_row, attend_block, lambda partial_state: partial_state, running
            ),
            None,
        )

    carried, _ = lax.scan(
        block_step, carried, (key_blocks, value_blocks, jnp.arange(block_count, dtype=jnp.int32))
    )
    maxima, totals, weighted = carried
    attended = weighted / totals[..., None]
    mixed_heads = attended[:, 0] - diff_lambda[:, None, None] * attended[:, 1]
    normed = (
        mixed_heads
        * lax.rsqrt(jnp.mean(mixed_heads * mixed_heads, axis=2, keepdims=True) + NORM_EPS)
        * sub_gain
    )
    heads_out = jnp.transpose(normed.astype(jnp.bfloat16), (1, 0, 2)).reshape(
        row_count, local_heads * value_width
    )
    return jnp.dot(heads_out, out_weight, preferred_element_type=jnp.float32)


def expert_terms(
    routed_input, routes, expert_gate, expert_up, expert_down, shared_gate, shared_up, shared_down
):
    row_count, part_width = routed_input.shape
    top_count = routes.shape[1]
    local_experts = expert_gate.shape[0]
    groups = lax.axis_size("ep")
    experts = local_experts * groups
    capacity = 2 * row_count * top_count // experts
    copies = row_count * top_count
    flat_routes = routes.reshape(copies)
    onehot = (flat_routes[:, None] == jnp.arange(experts, dtype=jnp.int32)[None, :]).astype(
        jnp.int32
    )
    rank_within = jnp.sum((jnp.cumsum(onehot, axis=0) - onehot) * onehot, axis=1)
    slot_index = flat_routes * capacity + rank_within
    placer = (
        slot_index[:, None] == jnp.arange(experts * capacity, dtype=jnp.int32)[None, :]
    ).astype(jnp.bfloat16)
    token_slots = jnp.sum(placer.reshape(row_count, top_count, experts * capacity), axis=1)
    outgoing = jnp.dot(token_slots.T, routed_input, preferred_element_type=jnp.float32).astype(
        jnp.bfloat16
    )
    arrived = lax.all_to_all(
        outgoing.reshape(groups, local_experts * capacity, part_width),
        "ep",
        split_axis=0,
        concat_axis=0,
        tiled=True,
    )
    slot_count = groups * capacity
    slot_rows = jnp.transpose(
        arrived.reshape(groups, local_experts, capacity, part_width), (1, 0, 2, 3)
    ).reshape(local_experts, slot_count, part_width)
    slot_piece = lax.all_gather(slot_rows, "tp", axis=2, tiled=True)
    own_piece = lax.all_gather(routed_input[None], "tp", axis=2, tiled=True)
    own_rows = own_piece[0]
    gate_sum = jnp.einsum(
        "emc,ecf->emf", slot_piece, expert_gate, preferred_element_type=jnp.float32
    )
    up_sum = jnp.einsum("emc,ecf->emf", slot_piece, expert_up, preferred_element_type=jnp.float32)
    square_sum = jnp.sum(jnp.square(slot_piece.astype(jnp.float32)), axis=2)
    shared_gate_sum = jnp.dot(own_rows, shared_gate, preferred_element_type=jnp.float32)
    shared_up_sum = jnp.dot(own_rows, shared_up, preferred_element_type=jnp.float32)
    shared_square = jnp.sum(jnp.square(own_rows.astype(jnp.float32)), axis=1)
    full_width = expert_gate.shape[1]
    factor = lax.rsqrt(square_sum / full_width + NORM_EPS)[..., None]
    hidden = (jax.nn.silu(gate_sum * factor) * (up_sum * factor)).astype(jnp.bfloat16)
    shared_factor = lax.rsqrt(shared_square / full_width + NORM_EPS)[:, None]
    shared_hidden = (
        jax.nn.silu(shared_gate_sum * shared_factor) * (shared_up_sum * shared_factor)
    ).astype(jnp.bfloat16)
    shared_terms = jnp.dot(shared_hidden, shared_down, preferred_element_type=jnp.float32)
    routed_terms = jnp.einsum(
        "emf,efd->emd", hidden, expert_down, preferred_element_type=jnp.float32
    )
    routed_sum = lax.psum_scatter(
        routed_terms.astype(jnp.bfloat16), "tp", scatter_dimension=2, tiled=True
    ).astype(jnp.float32)
    return (routed_sum, shared_terms, placer)


def expert_finish(routed_sum, shared_sum, placer, route_weights):
    local_experts, slot_count, part_width = routed_sum.shape
    groups = lax.axis_size("ep")
    capacity = slot_count // groups
    leaving = jnp.transpose(
        routed_sum.astype(jnp.bfloat16).reshape(local_experts, groups, capacity, part_width),
        (1, 0, 2, 3),
    ).reshape(groups, local_experts * capacity, part_width)
    returned = lax.all_to_all(leaving, "ep", split_axis=0, concat_axis=0, tiled=True)
    copy_results = jnp.dot(
        placer,
        returned.reshape(groups * local_experts * capacity, part_width),
        preferred_element_type=jnp.float32,
    )
    row_count, top_count = route_weights.shape
    routed = jnp.sum(
        copy_results.reshape(row_count, top_count, part_width) * route_weights[:, :, None], axis=1
    )
    return (routed + shared_sum).astype(jnp.bfloat16)


def body(
    query_heads,
    key_heads,
    value_heads,
    diff_lambda,
    sub_gain,
    out_weight,
    routed_input,
    routes,
    route_weights,
    expert_gate,
    expert_up,
    expert_down,
    shared_gate,
    shared_up,
    shared_down,
):
    mixer_partial = mixer_terms(
        query_heads, key_heads, value_heads, diff_lambda, sub_gain, out_weight
    )
    routed_sum, shared_terms, placer = expert_terms(
        routed_input,
        routes,
        expert_gate,
        expert_up,
        expert_down,
        shared_gate,
        shared_up,
        shared_down,
    )
    mixer_sum, shared_sum = (
        lax.psum_scatter(
            mixer_partial.astype(jnp.bfloat16), "tp", scatter_dimension=1, tiled=True
        ).astype(jnp.float32),
        lax.psum_scatter(
            shared_terms.astype(jnp.bfloat16), "tp", scatter_dimension=1, tiled=True
        ).astype(jnp.float32),
    )
    return (
        mixer_sum.astype(jnp.bfloat16),
        expert_finish(routed_sum, shared_sum, placer, route_weights),
    )


MESH = pl.DeviceIdType.MESH
F32 = jnp.float32
BF16 = jnp.bfloat16
OWN, XB, YB, DB = 0, 1, 2, 3


def low(value):
    return value.astype(BF16)


def f32(value):
    return value.astype(F32)


def mm(left, right):
    return jnp.dot(left, right, preferred_element_type=F32)


def near_first(chips):
    rows = [sorted((s for s in range(chips) if s != z), key=lambda s: (abs(s - z), s if z < chips // 2 else -s)) for z in range(chips)]
    return [[row[j] for row in rows] for j in range(chips - 1)]


def far_first(chips):
    rows = []
    for z in range(chips):
        right = list(range(chips - 1, z, -1))
        left = list(range(0, z))
        first, second = (right, left) if z < chips // 2 else (left, right)
        row = []
        while first or second:
            if first:
                row.append(first.pop(0))
            if second:
                row.append(second.pop(0))
        rows.append(row)
    return [[row[j] for row in rows] for j in range(chips - 1)]


def layer_kernel(
    chips,
    q_ref,
    k_ref,
    v_ref,
    lam_ref,
    gain_ref,
    x_ref,
    routes_ref,
    rw_ref,
    tab_hbm,
    ow_hbm,
    gw_hbm,
    uw_hbm,
    dw_hbm,
    sg_hbm,
    su_hbm,
    sd_hbm,
    mix_ref,
    out_ref,
    xall,
    guw,
    dw,
    sgu,
    sd,
    ow,
    tab,
    acc,
    sacc,
    ssq,
    hid,
    shid,
    oacc,
    dsend,
    esend,
    lsend,
    late,
    din,
    xyin,
    zin,
    zout,
    macc,
    kv,
    qrot,
    sc_s,
    sc_p,
    sc_t,
    sc_o,
    ho,
    shtab,
    shcol,
    w_l,
    w_s,
    w_r,
    ag_s,
    ag_r,
    xy_s,
    xy_r,
    dr_s,
    dr_r,
    pt_s,
    pt_r,
    kv_s,
    kv_r,
    sh_s,
    sh_r,
    h_s,
    h_r,
    d_s,
    d_r,
    e_s,
    e_r,
    z_s,
    z_r,
):
    rows, part = x_ref.shape
    half = rows // 2
    wide = 2 * part
    hidden = gw_hbm.shape[1]
    shared = sg_hbm.shape[1]
    vwide = v_ref.shape[1]
    kwide = k_ref.shape[1]
    local_heads = lam_ref.shape[0]
    vd = vwide // local_heads
    qk = kwide // (2 * local_heads)
    e = lax.axis_index("ep")
    t = lax.axis_index("tp")
    z, c = t // 2, t % 2
    x, y = e % 2, e // 2
    pt = (e, t + 1 - 2 * c)
    xn = (e + 1 - 2 * x, t)
    yn = (e + 2 - 4 * y, t)
    zr = (e, t + 2)
    zl = (e, t - 2)
    has_r = z < chips - 1
    has_l = z > 0

    def chosen_by_z(column):
        return sum(order * (z == at).astype(jnp.int32) for at, order in enumerate(column))

    nears = [chosen_by_z(column) for column in near_first(chips)]
    fars = [chosen_by_z(column) for column in far_first(chips)] + [z]

    def remote(src, dst, send, recv, dev):
        pltpu.make_async_remote_copy(src, dst, send, recv, device_id=dev, device_id_type=MESH).start()

    def got(dst, recv):
        pltpu.make_async_remote_copy(dst, dst, recv, recv, device_id=pt, device_id_type=MESH).wait_recv()

    def sent(src, send):
        pltpu.make_async_remote_copy(src, src, send, send, device_id=pt, device_id_type=MESH).wait_send()

    def cols(index, width):
        return pl.ds(pl.multiple_of(index * width, width), width)

    loads = [
        pltpu.make_async_copy(gw_hbm, guw.at[:, pl.ds(0, hidden)], w_l.at[0]),
        pltpu.make_async_copy(uw_hbm, guw.at[:, pl.ds(hidden, hidden)], w_l.at[1]),
        pltpu.make_async_copy(sg_hbm, sgu.at[:, pl.ds(0, shared)], w_l.at[2]),
        pltpu.make_async_copy(su_hbm, sgu.at[:, pl.ds(shared, shared)], w_l.at[3]),
        pltpu.make_async_copy(tab_hbm.at[pl.ds(pl.multiple_of(e * rows, rows), rows), :], tab, w_l.at[4]),
    ]
    downs = [(ow_hbm, ow, vwide), (sd_hbm, sd, shared), (dw_hbm, dw, hidden)]
    for i, (src, dst, depth) in enumerate(downs):
        for p in range(chips):
            loads.append(
                pltpu.make_async_copy(
                    src.at[:, cols(2 * p + c, part)],
                    dst.at[cols(c, depth), pl.ds(p * part, part)],
                    w_l.at[5 + i * chips + p],
                )
            )
    loads[4].start()
    for i in list(range(4)) + list(range(5, len(loads))):
        loads[i].start()

    barrier = pltpu.get_barrier_semaphore()
    for dev in (pt, xn, yn):
        pl.semaphore_signal(barrier, inc=1, device_id=dev, device_id_type=MESH)

    @pl.when(has_r)
    def _():
        pl.semaphore_signal(barrier, inc=1, device_id=zr, device_id_type=MESH)

    @pl.when(has_l)
    def _():
        pl.semaphore_signal(barrier, inc=1, device_id=zl, device_id_type=MESH)

    pl.semaphore_wait(barrier, 3 + has_r.astype(jnp.int32) + has_l.astype(jnp.int32))

    def piece(block, s, core):
        return xall.at[block, :, cols(2 * s + core, part)]

    def z_forward(src, kind, block, s, right, left):
        @pl.when(right)
        def _():
            remote(src, piece(block, s, c), ag_s.at[kind, 0, s], ag_r.at[kind, s], zr)

        @pl.when(left)
        def _():
            remote(src, piece(block, s, c), ag_s.at[kind, 1, s], ag_r.at[kind, s], zl)

    def to_pair(src, block, s):
        remote(src, piece(block, s, c), pt_s.at[block, s], pt_r.at[block, s], pt)

    def to_xy(src, s):
        remote(src, piece(XB, s, c), xy_s.at[0, s], xy_r.at[0, s], xn)
        remote(src, piece(YB, s, c), xy_s.at[1, s], xy_r.at[1, s], yn)

    z_forward(x_ref, 0, OWN, z, has_r, has_l)
    to_xy(x_ref, z)
    to_pair(x_ref, OWN, z)
    xall[OWN, :, cols(t, part)] = x_ref[...]

    lane = lax.broadcasted_iota(jnp.int32, (rows, 128), 1)
    routes = routes_ref[...]
    weights = rw_ref[...]
    table = jnp.zeros((rows, 128), F32)
    for k in range(routes.shape[1]):
        table = table + jnp.where(routes[:, k : k + 1] == lane, weights[:, k : k + 1], 0.0)
    shtab[OWN] = table.T[:8, :]
    remote(shtab.at[OWN], shtab.at[XB], sh_s.at[0], sh_r.at[0], xn)
    remote(shtab.at[OWN], shtab.at[YB], sh_s.at[1], sh_r.at[1], yn)

    loads[4].wait()
    cosine, sine = tab[:, :128], tab[:, 128:]
    at_row = lax.broadcasted_iota(jnp.int32, (128, 128), 0)
    at_col = lax.broadcasted_iota(jnp.int32, (128, 128), 1)
    swapped = at_col + qk // 2 - qk * ((at_col // (qk // 2)) % 2)
    swap = jnp.where(at_row == swapped, 1.0, 0.0).astype(BF16)
    for i in range(kwide // 128):
        span = slice(i * 128, (i + 1) * 128)
        for src, dst in ((q_ref, qrot), (k_ref, None)):
            value = src[:, span]
            turned = low(f32(value) * cosine + mm(value, swap) * sine)
            if dst is None:
                kv[0:rows, span] = turned
            else:
                dst[:, span] = turned
    kv[0:rows, kwide:] = v_ref[...]

    def kv_rows(block, start, count):
        return kv.at[pl.ds(block * rows + start, count), :]

    remote(kv_rows(OWN, 0, rows), kv_rows(XB, 0, rows), kv_s.at[0], kv_r.at[0], xn)
    remote(kv_rows(OWN, 0, rows), kv_rows(YB, 0, rows), kv_s.at[1], kv_r.at[1], yn)

    for i, (src, dst, depth) in enumerate(downs):
        for p in range(chips):
            remote(
                src.at[:, cols(2 * p + 1 - c, part)],
                dst.at[cols(c, depth), pl.ds(p * part, part)],
                w_s.at[i, p],
                w_r.at[i, p],
                pt,
            )

    def chunk(block, s, first, weight, target, width):
        tiles = target.shape[-1] // width

        def tile(n, carry):
            span = cols(n, width)
            value = mm(xall[block, :, cols(s, wide)], weight[cols(s, wide), span])
            if not first:
                value = value + target[:, span]
            target[:, span] = value
            return carry

        lax.fori_loop(0, tiles, tile, 0)

    def squares(block, s, first):
        total = jnp.zeros((rows, 128), F32) if first else ssq[block]
        for i in range(wide // 128):
            value = f32(xall[block, :, pl.ds(pl.multiple_of(s * wide + i * 128, 128), 128)])
            total = total + value * value
        ssq[block] = total

    def expert_chunk(block, s, first):
        got(piece(block, s, 1 - c), pt_r.at[block, s])
        chunk(block, s, first, guw, acc.at[block], hidden)
        squares(block, s, first)

    def shared_chunk(s, first):
        chunk(OWN, s, first, sgu, sacc, 2 * shared)

    def activate(block, source, width, target, index):
        full = jnp.sum(ssq[block], axis=1, keepdims=True) / (chips * wide)
        factor = lax.rsqrt(full + NORM_EPS)
        gate = source[:, :width] * factor
        up = source[:, width:] * factor
        target[:, cols(c, width)] = low(gate / (1.0 + jnp.exp(-gate)) * up)
        mine = target.at[:, cols(c, width)]
        remote(mine, mine, h_s.at[index], h_r.at[index], pt)

    def own_arrival(s):
        got(piece(OWN, s, c), ag_r.at[0, s])
        src = piece(OWN, s, c)
        z_forward(src, 0, OWN, s, (s < z) & has_r, (s > z) & has_l)
        to_xy(src, s)
        to_pair(src, OWN, s)

    def side_arrival(s):
        for i, block in ((0, XB), (1, YB)):
            got(piece(block, s, c), xy_r.at[i, s])
            to_pair(piece(block, s, c), block, s)

    def far_half(s, i):
        return xall.at[DB, pl.ds(i * half, half), cols(2 * s + c, part)]

    def far_arrival(s):
        got(piece(DB, s, c), ag_r.at[1, s])
        src = piece(DB, s, c)
        z_forward(src, 1, DB, s, (s < z) & has_r, (s > z) & has_l)
        to_pair(src, DB, s)

    side_arrival(z)
    remote(xall.at[XB, pl.ds(0, half), cols(t, part)], far_half(z, 0), dr_s.at[0], dr_r.at[0], yn)
    remote(xall.at[YB, pl.ds(half, half), cols(t, part)], far_half(z, 1), dr_s.at[1], dr_r.at[1], xn)
    own_arrival(nears[0])
    loads[0].wait()
    loads[1].wait()
    expert_chunk(OWN, z, True)
    got(shtab.at[XB], sh_r.at[0])
    got(shtab.at[YB], sh_r.at[1])
    remote(shtab.at[XB], shtab.at[DB], sh_s.at[2], sh_r.at[2], yn)
    expert_chunk(OWN, nears[0], False)
    own_arrival(nears[1])
    loads[2].wait()
    loads[3].wait()
    shared_chunk(z, True)
    got(kv_rows(XB, 0, rows), kv_r.at[0])
    got(kv_rows(YB, 0, rows), kv_r.at[1])
    remote(kv_rows(XB, 0, half), kv_rows(DB, 0, half), kv_s.at[2], kv_r.at[2], yn)
    remote(kv_rows(YB, half, half), kv_rows(DB, half, half), kv_s.at[3], kv_r.at[3], xn)
    expert_chunk(OWN, nears[1], False)
    got(far_half(z, 0), dr_r.at[0])
    got(far_half(z, 1), dr_r.at[1])
    z_forward(piece(DB, z, c), 1, DB, z, has_r, has_l)
    to_pair(piece(DB, z, c), DB, z)
    own_arrival(nears[2])
    expert_chunk(XB, z, True)
    expert_chunk(YB, z, True)
    expert_chunk(OWN, nears[2], False)
    activate(OWN, acc.at[OWN], hidden, hid.at[OWN], OWN)
    expert_chunk(DB, z, True)
    got(kv_rows(DB, 0, half), kv_r.at[2])
    got(kv_rows(DB, half, half), kv_r.at[3])
    key_count = kv.shape[0]
    step_rows = 32
    ids = (e, xn[0], yn[0], xn[0] + yn[0] - e)

    def one_map(h, m):
        in_map = (lax.broadcasted_iota(jnp.int32, (rows, 128), 1) // qk) == m
        query = jnp.where(in_map, qrot[:, cols(h, 128)], jnp.zeros((rows, 128), BF16))
        sc_s[...] = lax.dot_general(
            query, kv[:, cols(h, 128)], (((1,), (1,)), ((), ())), preferred_element_type=F32
        )

        def soften(r, carry):
            at = pl.ds(pl.multiple_of(r * step_rows, step_rows), step_rows)
            key = lax.broadcasted_iota(jnp.int32, (step_rows, key_count), 1)
            which = key // rows
            group = jnp.where(
                which == 0, ids[0], jnp.where(which == 1, ids[1], jnp.where(which == 2, ids[2], ids[3]))
            )
            key_at = group * rows + key % rows
            query_at = (
                e * rows + r * step_rows + lax.broadcasted_iota(jnp.int32, (step_rows, key_count), 0)
            )
            scores = jnp.where(key_at <= query_at, sc_s[at, :] * (qk ** (-0.5)), MASKED)
            weight = jnp.exp(scores - jnp.max(scores, axis=1, keepdims=True))
            total = jnp.sum(weight, axis=1, keepdims=True)
            sc_p[at, :] = low(weight)
            sc_t[at, :] = jnp.broadcast_to(total, (step_rows, 128))
            return carry

        lax.fori_loop(0, rows // step_rows, soften, 0)
        return mm(sc_p[...], kv[:, pl.ds(pl.multiple_of(kwide + h * vd, 128), vd)]) / sc_t[...]

    def one_head(h):
        sc_o[...] = one_map(h, 0)
        mixed = sc_o[...] - lam_ref[h] * one_map(h, 1)
        scale = lax.rsqrt(jnp.mean(mixed * mixed, axis=1, keepdims=True) + NORM_EPS)
        ho[:, pl.ds(pl.multiple_of(c * vwide + h * vd, 128), vd)] = low(mixed * scale * gain_ref[...])

    for h in range(local_heads):
        one_head(h)
        if h == 0:
            for i in range(1, chips - 1):
                shared_chunk(nears[i - 1], False)
    mine = ho.at[:, cols(c, vwide)]
    remote(mine, mine, h_s.at[5], h_r.at[5], pt)
    shared_chunk(nears[chips - 2], False)
    activate(OWN, sacc, shared, shid, 4)
    for j in range(chips - 1):
        side_arrival(nears[j])
        far_arrival(nears[j])
        last = j == chips - 2
        if j == 0:
            for p in range(chips):
                loads[5 + p].wait()
                got(ow.at[cols(1 - c, vwide), pl.ds(p * part, part)], w_r.at[0, p])
            got(ho.at[:, cols(1 - c, vwide)], h_r.at[5])
            for p in range(chips):
                macc[:, pl.ds(p * part, part)] = mm(ho[...], ow[:, pl.ds(p * part, part)])
        if j == 1:
            for p in range(chips):
                loads[5 + chips + p].wait()
                loads[5 + 2 * chips + p].wait()
                got(sd.at[cols(1 - c, shared), pl.ds(p * part, part)], w_r.at[1, p])
                got(dw.at[cols(1 - c, hidden), pl.ds(p * part, part)], w_r.at[2, p])
            got(hid.at[OWN, :, cols(1 - c, hidden)], h_r.at[OWN])
            got(shid.at[:, cols(1 - c, shared)], h_r.at[4])
            got(shtab.at[DB], sh_r.at[2])
            row_id = lax.broadcasted_iota(jnp.int32, (8, rows), 0)
            for block in range(4):
                line = jnp.sum(jnp.where(row_id == e, shtab[block], 0.0), axis=0, keepdims=True)
                shcol[block] = jnp.broadcast_to(line, (128, rows)).T

            def own_down(p, carry):
                span = cols(p, part)
                oacc[:, span] = mm(hid[OWN], dw[:, span]) * shcol[OWN, :, 0:1] + mm(shid[...], sd[:, span])
                return carry

            lax.fori_loop(0, chips, own_down, 0)
        for block in (DB, XB, YB):
            expert_chunk(block, nears[j], False)
            if last:
                activate(block, acc.at[block], hidden, hid.at[block], block)

    def z_send(kind, j, p, value_of):
        upstream = ((p > z) & has_l) | ((p < z) & has_r)
        slot = zout.at[kind, j]

        @pl.when(upstream)
        def _():
            got(zin.at[kind, p], z_r.at[kind, p])
            zout[kind, j] = low(value_of() + f32(zin[kind, p]))

        @pl.when(jnp.logical_not(upstream))
        def _():
            zout[kind, j] = low(value_of())

        @pl.when(p > z)
        def _():
            remote(slot, zin.at[kind, p], z_s.at[kind, j], z_r.at[kind, p], zr)

        @pl.when((p < z) & (p != z - 1))
        def _():
            remote(slot, zin.at[kind, p], z_s.at[kind, j], z_r.at[kind, p], zl)

        @pl.when((p < z) & (p == z - 1))
        def _():
            remote(slot, zin.at[kind, chips], z_s.at[kind, j], z_r.at[kind, chips], zl)

    def z_finish(kind, value):
        target = (mix_ref, out_ref)[kind]

        @pl.when(has_l)
        def _():
            got(zin.at[kind, z], z_r.at[kind, z])

        @pl.when(has_r)
        def _():
            got(zin.at[kind, chips], z_r.at[kind, chips])

        @pl.when(has_l & has_r)
        def _():
            target[...] = low(value + f32(zin[kind, z]) + f32(zin[kind, chips]))

        @pl.when(jnp.logical_not(has_l))
        def _():
            target[...] = low(value + f32(zin[kind, chips]))

        @pl.when(jnp.logical_not(has_r))
        def _():
            target[...] = low(value + f32(zin[kind, z]))

    def mixer_send(j):
        p = fars[j]
        z_send(0, j, p, lambda: macc[:, cols(p, part)])

    edge = jnp.logical_not(has_l & has_r)

    @pl.when(edge)
    def _():
        for j in range(chips - 1):
            mixer_send(j)

    def down(block, p):
        return mm(hid[block], dw[:, cols(p, part)]) * shcol[block, :, 0:1]

    top, rest = pl.ds(0, half), pl.ds(half, half)
    got(hid.at[DB, :, cols(1 - c, hidden)], h_r.at[DB])
    for j in range(chips):
        span = cols(fars[j], part)
        dsend[:, span] = low(down(DB, fars[j]))
        remote(dsend.at[top, span], din.at[0, :, span], d_s.at[0, j], d_r.at[0, j], xn)
        remote(dsend.at[rest, span], din.at[1, :, span], d_s.at[1, j], d_r.at[1, j], yn)
    for i, block, now, later, dev in ((0, XB, 0, 1, xn), (1, YB, 1, 0, yn)):
        got(hid.at[block, :, cols(1 - c, hidden)], h_r.at[block])
        now_rows = slice(now * half, (now + 1) * half)
        late_rows = slice(later * half, (later + 1) * half)
        for j in range(chips):
            span = cols(fars[j], part)
            value = down(block, fars[j])
            esend[i, :, span] = low(value[now_rows])
            late[i, :, span] = value[late_rows]
            remote(
                esend.at[i, :, span],
                xyin.at[i, pl.ds(now * half, half), span],
                e_s.at[i, 0, j],
                e_r.at[i, 0, j],
                dev,
            )
    for j in range(chips):
        span = cols(fars[j], part)
        for i, block, now, later, dev in ((0, XB, 0, 1, xn), (1, YB, 1, 0, yn)):
            got(din.at[1 - i, :, span], d_r.at[1 - i, j])
            lsend[i, :, span] = low(late[i, :, span] + f32(din[1 - i, :, span]))
            remote(
                lsend.at[i, :, span],
                xyin.at[i, pl.ds(later * half, half), span],
                e_s.at[i, 1, j],
                e_r.at[i, 1, j],
                dev,
            )

    @pl.when(jnp.logical_not(edge))
    def _():
        for j in range(chips - 1):
            mixer_send(j)

    z_finish(0, macc[:, cols(z, part)])

    for j in range(chips):
        p = fars[j]
        span = cols(p, part)
        for i, now, later in ((0, 0, 1), (1, 1, 0)):
            got(xyin.at[i, pl.ds(now * half, half), span], e_r.at[i, 0, j])
            got(xyin.at[i, pl.ds(later * half, half), span], e_r.at[i, 1, j])

        def total():
            return oacc[:, span] + f32(xyin[0, :, span]) + f32(xyin[1, :, span])

        if j < chips - 1:
            z_send(1, j, p, total)
        else:
            z_finish(1, total())

    for kind, block in ((0, OWN), (1, DB)):
        for s in range(chips):

            @pl.when(has_r & (s <= z))
            def _():
                sent(piece(block, s, c), ag_s.at[kind, 0, s])

            @pl.when(has_l & (s >= z))
            def _():
                sent(piece(block, s, c), ag_s.at[kind, 1, s])

    for s in range(chips):
        for i in range(2):
            sent(piece(OWN, s, c), xy_s.at[i, s])
        for block in range(4):
            sent(piece(block, s, c), pt_s.at[block, s])
    for i in range(2):
        sent(far_half(z, i), dr_s.at[i])
        sent(kv_rows(OWN, 0, rows), kv_s.at[i])
        sent(kv_rows(OWN, 0, half), kv_s.at[2 + i])
    for i in range(3):
        sent(shtab.at[OWN], sh_s.at[i])
        for p in range(chips):
            src, dst, depth = downs[i]
            sent(dst.at[cols(c, depth), pl.ds(p * part, part)], w_s.at[i, p])
    for block in range(4):
        sent(hid.at[block, :, cols(c, hidden)], h_s.at[block])
    sent(shid.at[:, cols(c, shared)], h_s.at[4])
    sent(ho.at[:, cols(c, vwide)], h_s.at[5])
    for i in range(2):
        for j in range(chips):
            sent(dsend.at[top, pl.ds(j * part, part)], d_s.at[i, j])
            sent(esend.at[i, :, pl.ds(j * part, part)], e_s.at[i, 0, j])
            sent(lsend.at[i, :, pl.ds(j * part, part)], e_s.at[i, 1, j])
        for j in range(chips - 1):
            sent(zout.at[i, j], z_s.at[i, j])


def rotation_table(positions, key_width):
    half_width = key_width // 2
    freq = np.float32(ROPE_BASE) ** (-np.arange(half_width, dtype=np.float32) / np.float32(half_width))
    angles = np.arange(positions, dtype=np.float32)[:, None] * freq.astype(np.float32)[None, :]
    angles = angles.astype(np.float64)
    cosine, sine = np.cos(angles), np.sin(angles)
    copies = 128 // key_width
    cosine = np.tile(np.concatenate([cosine, cosine], axis=1), (1, copies))
    sine = np.tile(np.concatenate([-sine, sine], axis=1), (1, copies))
    return np.concatenate([cosine, sine], axis=1).astype(np.float32)


def kernel_body(
    query_heads,
    key_heads,
    value_heads,
    diff_lambda,
    sub_gain,
    out_weight,
    routed_input,
    routes,
    route_weights,
    expert_gate,
    expert_up,
    expert_down,
    shared_gate,
    shared_up,
    shared_down,
):
    rows, part = routed_input.shape
    chips = lax.axis_size("tp") // 2
    groups = lax.axis_size("ep")
    gate, up, down = expert_gate[0], expert_up[0], expert_down[0]
    width, hidden = gate.shape
    shared = shared_gate.shape[1]
    kwide, vwide = key_heads.shape[1], value_heads.shape[1]
    local_heads = diff_lambda.shape[0]
    half, mine = rows // 2, width // 2
    table = jnp.asarray(rotation_table(groups * rows, kwide // (2 * local_heads)))
    vmem = pl.BlockSpec(memory_space=pltpu.VMEM)
    smem = pl.BlockSpec(memory_space=pltpu.SMEM)
    hbm = pl.BlockSpec(memory_space=pl.ANY)
    dma = pltpu.SemaphoreType.DMA
    out = jax.ShapeDtypeStruct((rows, part), BF16)
    return pl.pallas_call(
        functools.partial(layer_kernel, chips),
        out_shape=(out, out),
        in_specs=[vmem, vmem, vmem, smem, vmem, vmem, vmem, vmem] + [hbm] * 8,
        out_specs=(vmem, vmem),
        scratch_shapes=[
            pltpu.VMEM((groups, rows, width), BF16),
            pltpu.VMEM((width, 2 * hidden), BF16),
            pltpu.VMEM((2 * hidden, mine), BF16),
            pltpu.VMEM((width, 2 * shared), BF16),
            pltpu.VMEM((2 * shared, mine), BF16),
            pltpu.VMEM((2 * vwide, mine), BF16),
            pltpu.VMEM((rows, 256), F32),
            pltpu.VMEM((groups, rows, 2 * hidden), F32),
            pltpu.VMEM((rows, 2 * shared), F32),
            pltpu.VMEM((groups, rows, 128), F32),
            pltpu.VMEM((groups, rows, 2 * hidden), BF16),
            pltpu.VMEM((rows, 2 * shared), BF16),
            pltpu.VMEM((rows, mine), F32),
            pltpu.VMEM((rows, mine), BF16),
            pltpu.VMEM((2, half, mine), BF16),
            pltpu.VMEM((2, half, mine), BF16),
            pltpu.VMEM((2, half, mine), F32),
            pltpu.VMEM((2, half, mine), BF16),
            pltpu.VMEM((2, rows, mine), BF16),
            pltpu.VMEM((2, chips + 1, rows, part), BF16),
            pltpu.VMEM((2, chips - 1, rows, part), BF16),
            pltpu.VMEM((rows, mine), F32),
            pltpu.VMEM((groups * rows, kwide + vwide), BF16),
            pltpu.VMEM((rows, kwide), BF16),
            pltpu.VMEM((rows, groups * rows), F32),
            pltpu.VMEM((rows, groups * rows), BF16),
            pltpu.VMEM((rows, 128), F32),
            pltpu.VMEM((rows, 128), F32),
            pltpu.VMEM((rows, 2 * vwide), BF16),
            pltpu.VMEM((groups, 8, rows), F32),
            pltpu.VMEM((groups, rows, 128), F32),
            dma((5 + 3 * chips,)),
            dma((3, chips)),
            dma((3, chips)),
            dma((2, 2, chips)),
            dma((2, chips)),
            dma((2, chips)),
            dma((2, chips)),
            dma((2,)),
            dma((2,)),
            dma((4, chips)),
            dma((4, chips)),
            dma((4,)),
            dma((4,)),
            dma((3,)),
            dma((3,)),
            dma((6,)),
            dma((6,)),
            dma((2, chips)),
            dma((2, chips)),
            dma((2, 2, chips)),
            dma((2, 2, chips)),
            dma((2, chips - 1)),
            dma((2, chips + 1)),
        ],
        compiler_params=pltpu.CompilerParams(
            collective_id=0, has_side_effects=True, vmem_limit_bytes=67043328
        ),
        name="layer",
    )(
        query_heads,
        key_heads,
        value_heads,
        diff_lambda,
        sub_gain[None, :],
        routed_input,
        routes,
        route_weights,
        table,
        out_weight,
        gate,
        up,
        down,
        shared_gate,
        shared_up,
        shared_down,
    )


def solution(mesh):
    dense = mesh.shape["ep"] == 4 and mesh.shape["tp"] == 8

    def chosen(*arguments):
        fits = dense and arguments[9].shape[0] == 1 and arguments[6].shape[0] % 32 == 0
        return (kernel_body if fits else body)(*arguments)

    placed = (
        P("ep", "tp"),
        P("ep", "tp"),
        P("ep", "tp"),
        P("tp"),
        P(),
        P("tp", None),
        P("ep", "tp"),
        P("ep", None),
        P("ep", None),
        P("ep", None, "tp"),
        P("ep", None, "tp"),
        P("ep", "tp", None),
        P(None, "tp"),
        P(None, "tp"),
        P("tp", None),
    )
    return jax.shard_map(
        chosen, mesh=mesh, in_specs=placed, out_specs=(P("ep", "tp"), P("ep", "tp")), check_vma=False
    )
```

```python
import functools

import jax
import jax.numpy as jnp
import numpy as np
from jax import lax
from jax.experimental import pallas as pl
from jax.experimental.pallas import tpu as pltpu
from jax.sharding import PartitionSpec as P

ROPE_BASE = 10000.0
NORM_EPS = 1e-06
MASKED = -1e30


def rotate(values, positions):
    half_width = values.shape[-1] // 2
    inverse_freq = ROPE_BASE ** (-jnp.arange(half_width, dtype=jnp.float32) / half_width)
    angles = positions.astype(jnp.float32)[:, None] * inverse_freq[None, :]
    angles = angles.reshape((angles.shape[0],) + (1,) * (values.ndim - 2) + (half_width,))
    cosine = jnp.cos(angles)
    sine_part = jnp.sin(angles)
    lower = values[..., :half_width]
    upper = values[..., half_width:]
    return jnp.concatenate(
        [lower * cosine - upper * sine_part, upper * cosine + lower * sine_part], axis=-1
    )


def mixer_terms(query_heads, key_heads, value_heads, diff_lambda, sub_gain, out_weight):
    row_count = query_heads.shape[0]
    local_heads = diff_lambda.shape[0]
    value_width = value_heads.shape[1] // local_heads
    key_width = query_heads.shape[1] // (2 * local_heads)
    score_scale = key_width ** (-0.5)
    offset = lax.axis_index("ep") * row_count
    positions = offset + jnp.arange(row_count, dtype=jnp.int32)
    last_row = offset + row_count - 1
    query_rot = rotate(
        query_heads.astype(jnp.float32).reshape(row_count, local_heads, 2, key_width), positions
    ).astype(jnp.bfloat16)
    queries = jnp.transpose(query_rot, (1, 2, 0, 3))
    key_rot = (
        rotate(
            key_heads.astype(jnp.float32).reshape(row_count, local_heads, 2, key_width), positions
        )
        .astype(jnp.bfloat16)
        .reshape(row_count, local_heads * 2 * key_width)
    )
    start_state = (
        jnp.full((local_heads, 2, row_count), MASKED, jnp.float32),
        jnp.zeros((local_heads, 2, row_count), jnp.float32),
        jnp.zeros((local_heads, 2, row_count, value_width), jnp.float32),
    )
    carried = start_state
    key_piece = lax.all_gather(key_rot, "ep", axis=0, tiled=True)
    value_piece = lax.all_gather(value_heads, "ep", axis=0, tiled=True)
    piece_rows = key_piece.shape[0]
    key_block = 512
    block_count = piece_rows // key_block
    key_blocks = key_piece.reshape(block_count, key_block, local_heads, 2, key_width)
    value_blocks = value_piece.reshape(block_count, key_block, local_heads, value_width)

    def block_step(running, block_item):
        key_rows, value_rows, block_index = block_item
        block_start = block_index * key_block

        def attend_block(partial_state):
            maxima, totals, weighted = partial_state
            key_positions = block_start + jnp.arange(key_block, dtype=jnp.int32)
            visible = key_positions[None, :] <= positions[:, None]
            scores = (
                jnp.einsum("hmqd,khmd->hmqk", queries, key_rows, preferred_element_type=jnp.float32)
                * score_scale
            )
            scores = jnp.where(visible, scores, MASKED)
            new_maxima = jnp.maximum(maxima, jnp.max(scores, axis=3))
            exp_weights = jnp.where(visible, jnp.exp(scores - new_maxima[..., None]), 0.0)
            shrink = jnp.exp(maxima - new_maxima)
            new_totals = totals * shrink + jnp.sum(exp_weights, axis=3)
            update = jnp.einsum(
                "hmqk,khw->hmqw",
                exp_weights.astype(jnp.bfloat16),
                value_rows,
                preferred_element_type=jnp.float32,
            )
            return (new_maxima, new_totals, weighted * shrink[..., None] + update)

        return (
            lax.cond(
                block_start <= last_row, attend_block, lambda partial_state: partial_state, running
            ),
            None,
        )

    carried, _ = lax.scan(
        block_step, carried, (key_blocks, value_blocks, jnp.arange(block_count, dtype=jnp.int32))
    )
    maxima, totals, weighted = carried
    attended = weighted / totals[..., None]
    mixed_heads = attended[:, 0] - diff_lambda[:, None, None] * attended[:, 1]
    normed = (
        mixed_heads
        * lax.rsqrt(jnp.mean(mixed_heads * mixed_heads, axis=2, keepdims=True) + NORM_EPS)
        * sub_gain
    )
    heads_out = jnp.transpose(normed.astype(jnp.bfloat16), (1, 0, 2)).reshape(
        row_count, local_heads * value_width
    )
    return jnp.dot(heads_out, out_weight, preferred_element_type=jnp.float32)


def expert_terms(
    routed_input, routes, expert_gate, expert_up, expert_down, shared_gate, shared_up, shared_down
):
    row_count, part_width = routed_input.shape
    top_count = routes.shape[1]
    local_experts = expert_gate.shape[0]
    groups = lax.axis_size("ep")
    experts = local_experts * groups
    capacity = 2 * row_count * top_count // experts
    copies = row_count * top_count
    flat_routes = routes.reshape(copies)
    onehot = (flat_routes[:, None] == jnp.arange(experts, dtype=jnp.int32)[None, :]).astype(
        jnp.int32
    )
    rank_within = jnp.sum((jnp.cumsum(onehot, axis=0) - onehot) * onehot, axis=1)
    slot_index = flat_routes * capacity + rank_within
    placer = (
        slot_index[:, None] == jnp.arange(experts * capacity, dtype=jnp.int32)[None, :]
    ).astype(jnp.bfloat16)
    token_slots = jnp.sum(placer.reshape(row_count, top_count, experts * capacity), axis=1)
    outgoing = jnp.dot(token_slots.T, routed_input, preferred_element_type=jnp.float32).astype(
        jnp.bfloat16
    )
    arrived = lax.all_to_all(
        outgoing.reshape(groups, local_experts * capacity, part_width),
        "ep",
        split_axis=0,
        concat_axis=0,
        tiled=True,
    )
    slot_count = groups * capacity
    slot_rows = jnp.transpose(
        arrived.reshape(groups, local_experts, capacity, part_width), (1, 0, 2, 3)
    ).reshape(local_experts, slot_count, part_width)
    slot_piece = lax.all_gather(slot_rows, "tp", axis=2, tiled=True)
    own_piece = lax.all_gather(routed_input[None], "tp", axis=2, tiled=True)
    own_rows = own_piece[0]
    gate_sum = jnp.einsum(
        "emc,ecf->emf", slot_piece, expert_gate, preferred_element_type=jnp.float32
    )
    up_sum = jnp.einsum("emc,ecf->emf", slot_piece, expert_up, preferred_element_type=jnp.float32)
    square_sum = jnp.sum(jnp.square(slot_piece.astype(jnp.float32)), axis=2)
    shared_gate_sum = jnp.dot(own_rows, shared_gate, preferred_element_type=jnp.float32)
    shared_up_sum = jnp.dot(own_rows, shared_up, preferred_element_type=jnp.float32)
    shared_square = jnp.sum(jnp.square(own_rows.astype(jnp.float32)), axis=1)
    full_width = expert_gate.shape[1]
    factor = lax.rsqrt(square_sum / full_width + NORM_EPS)[..., None]
    hidden = (jax.nn.silu(gate_sum * factor) * (up_sum * factor)).astype(jnp.bfloat16)
    shared_factor = lax.rsqrt(shared_square / full_width + NORM_EPS)[:, None]
    shared_hidden = (
        jax.nn.silu(shared_gate_sum * shared_factor) * (shared_up_sum * shared_factor)
    ).astype(jnp.bfloat16)
    shared_terms = jnp.dot(shared_hidden, shared_down, preferred_element_type=jnp.float32)
    routed_terms = jnp.einsum(
        "emf,efd->emd", hidden, expert_down, preferred_element_type=jnp.float32
    )
    routed_sum = lax.psum_scatter(
        routed_terms.astype(jnp.bfloat16), "tp", scatter_dimension=2, tiled=True
    ).astype(jnp.float32)
    return (routed_sum, shared_terms, placer)


def expert_finish(routed_sum, shared_sum, placer, route_weights):
    local_experts, slot_count, part_width = routed_sum.shape
    groups = lax.axis_size("ep")
    capacity = slot_count // groups
    leaving = jnp.transpose(
        routed_sum.astype(jnp.bfloat16).reshape(local_experts, groups, capacity, part_width),
        (1, 0, 2, 3),
    ).reshape(groups, local_experts * capacity, part_width)
    returned = lax.all_to_all(leaving, "ep", split_axis=0, concat_axis=0, tiled=True)
    copy_results = jnp.dot(
        placer,
        returned.reshape(groups * local_experts * capacity, part_width),
        preferred_element_type=jnp.float32,
    )
    row_count, top_count = route_weights.shape
    routed = jnp.sum(
        copy_results.reshape(row_count, top_count, part_width) * route_weights[:, :, None], axis=1
    )
    return (routed + shared_sum).astype(jnp.bfloat16)


def body(
    query_heads,
    key_heads,
    value_heads,
    diff_lambda,
    sub_gain,
    out_weight,
    routed_input,
    routes,
    route_weights,
    expert_gate,
    expert_up,
    expert_down,
    shared_gate,
    shared_up,
    shared_down,
):
    mixer_partial = mixer_terms(
        query_heads, key_heads, value_heads, diff_lambda, sub_gain, out_weight
    )
    routed_sum, shared_terms, placer = expert_terms(
        routed_input,
        routes,
        expert_gate,
        expert_up,
        expert_down,
        shared_gate,
        shared_up,
        shared_down,
    )
    mixer_sum, shared_sum = (
        lax.psum_scatter(
            mixer_partial.astype(jnp.bfloat16), "tp", scatter_dimension=1, tiled=True
        ).astype(jnp.float32),
        lax.psum_scatter(
            shared_terms.astype(jnp.bfloat16), "tp", scatter_dimension=1, tiled=True
        ).astype(jnp.float32),
    )
    return (
        mixer_sum.astype(jnp.bfloat16),
        expert_finish(routed_sum, shared_sum, placer, route_weights),
    )


MESH = pl.DeviceIdType.MESH
F32 = jnp.float32
BF16 = jnp.bfloat16
OWN, XB, YB, DB = 0, 1, 2, 3


def low(value):
    return value.astype(BF16)


def f32(value):
    return value.astype(F32)


def mm(left, right):
    return jnp.dot(left, right, preferred_element_type=F32)


def near_first(chips):
    rows = [sorted((s for s in range(chips) if s != z), key=lambda s: (abs(s - z), s if z < chips // 2 else -s)) for z in range(chips)]
    return [[row[j] for row in rows] for j in range(chips - 1)]


def far_first(chips):
    rows = []
    for z in range(chips):
        right = list(range(chips - 1, z, -1))
        left = list(range(0, z))
        first, second = (right, left) if z < chips // 2 else (left, right)
        row = []
        while first or second:
            if first:
                row.append(first.pop(0))
            if second:
                row.append(second.pop(0))
        rows.append(row)
    return [[row[j] for row in rows] for j in range(chips - 1)]


def layer_kernel(
    chips,
    q_ref,
    k_ref,
    v_ref,
    lam_ref,
    gain_ref,
    x_ref,
    routes_ref,
    rw_ref,
    tab_hbm,
    ow_hbm,
    gw_hbm,
    uw_hbm,
    dw_hbm,
    sg_hbm,
    su_hbm,
    sd_hbm,
    mix_ref,
    out_ref,
    xall,
    guw,
    dw,
    sgu,
    sd,
    ow,
    tab,
    acc,
    sacc,
    ssq,
    hid,
    shid,
    oacc,
    dsend,
    esend,
    lsend,
    late,
    din,
    xyin,
    zin,
    zout,
    macc,
    kv,
    qrot,
    sc_s,
    sc_p,
    sc_t,
    sc_o,
    ho,
    shtab,
    shcol,
    w_l,
    w_s,
    w_r,
    ag_s,
    ag_r,
    xy_s,
    xy_r,
    dr_s,
    dr_r,
    pt_s,
    pt_r,
    kv_s,
    kv_r,
    sh_s,
    sh_r,
    h_s,
    h_r,
    d_s,
    d_r,
    e_s,
    e_r,
    z_s,
    z_r,
):
    rows, part = x_ref.shape
    half = rows // 2
    wide = 2 * part
    hidden = gw_hbm.shape[1]
    shared = sg_hbm.shape[1]
    vwide = v_ref.shape[1]
    kwide = k_ref.shape[1]
    local_heads = lam_ref.shape[0]
    vd = vwide // local_heads
    qk = kwide // (2 * local_heads)
    e = lax.axis_index("ep")
    t = lax.axis_index("tp")
    z, c = t // 2, t % 2
    x, y = e % 2, e // 2
    pt = (e, t + 1 - 2 * c)
    xn = (e + 1 - 2 * x, t)
    yn = (e + 2 - 4 * y, t)
    zr = (e, t + 2)
    zl = (e, t - 2)
    has_r = z < chips - 1
    has_l = z > 0

    def chosen_by_z(column):
        return sum(order * (z == at).astype(jnp.int32) for at, order in enumerate(column))

    nears = [chosen_by_z(column) for column in near_first(chips)]
    fars = [chosen_by_z(column) for column in far_first(chips)] + [z]

    def remote(src, dst, send, recv, dev):
        pltpu.make_async_remote_copy(src, dst, send, recv, device_id=dev, device_id_type=MESH).start()

    def got(dst, recv):
        pltpu.make_async_remote_copy(dst, dst, recv, recv, device_id=pt, device_id_type=MESH).wait_recv()

    def sent(src, send):
        pltpu.make_async_remote_copy(src, src, send, send, device_id=pt, device_id_type=MESH).wait_send()

    def cols(index, width):
        return pl.ds(pl.multiple_of(index * width, width), width)

    loads = [
        pltpu.make_async_copy(gw_hbm, guw.at[:, pl.ds(0, hidden)], w_l.at[0]),
        pltpu.make_async_copy(uw_hbm, guw.at[:, pl.ds(hidden, hidden)], w_l.at[1]),
        pltpu.make_async_copy(sg_hbm, sgu.at[:, pl.ds(0, shared)], w_l.at[2]),
        pltpu.make_async_copy(su_hbm, sgu.at[:, pl.ds(shared, shared)], w_l.at[3]),
        pltpu.make_async_copy(tab_hbm.at[pl.ds(pl.multiple_of(e * rows, rows), rows), :], tab, w_l.at[4]),
    ]
    downs = [(ow_hbm, ow, vwide), (sd_hbm, sd, shared), (dw_hbm, dw, hidden)]
    for i, (src, dst, depth) in enumerate(downs):
        for p in range(chips):
            loads.append(
                pltpu.make_async_copy(
                    src.at[:, cols(2 * p + c, part)],
                    dst.at[cols(c, depth), pl.ds(p * part, part)],
                    w_l.at[5 + i * chips + p],
                )
            )
    loads[4].start()
    for i in list(range(4)) + list(range(5, len(loads))):
        loads[i].start()

    barrier = pltpu.get_barrier_semaphore()
    for dev in (pt, xn, yn):
        pl.semaphore_signal(barrier, inc=1, device_id=dev, device_id_type=MESH)

    @pl.when(has_r)
    def _():
        pl.semaphore_signal(barrier, inc=1, device_id=zr, device_id_type=MESH)

    @pl.when(has_l)
    def _():
        pl.semaphore_signal(barrier, inc=1, device_id=zl, device_id_type=MESH)

    pl.semaphore_wait(barrier, 3 + has_r.astype(jnp.int32) + has_l.astype(jnp.int32))

    def piece(block, s, core):
        return xall.at[block, :, cols(2 * s + core, part)]

    def halved(block, s, h):
        return xall.at[block, pl.ds(h * half, half), cols(2 * s + c, part)]

    def z_forward(src, kind, block, s, h, right, left):
        @pl.when(right)
        def _():
            remote(src, halved(block, s, h), ag_s.at[kind, 0, s, h], ag_r.at[kind, s, h], zr)

        @pl.when(left)
        def _():
            remote(src, halved(block, s, h), ag_s.at[kind, 1, s, h], ag_r.at[kind, s, h], zl)

    def to_pair(src, block, s):
        remote(src, piece(block, s, c), pt_s.at[block, s], pt_r.at[block, s], pt)

    def to_xy(s):
        remote(piece(OWN, s, c), piece(XB, s, c), xy_s.at[0, s], xy_r.at[0, s], xn)
        remote(piece(OWN, s, c), piece(YB, s, c), xy_s.at[1, s], xy_r.at[1, s], yn)

    def own_half(i, order):
        h = order if i == 0 else 1 - order
        block, dev = ((XB, xn), (YB, yn))[i]
        slot = z if order == 0 else chips
        remote(x_ref.at[pl.ds(h * half, half), :], halved(block, z, h), xy_s.at[i, slot], xy_r.at[i, slot], dev)

    for h in range(2):
        z_forward(x_ref.at[pl.ds(h * half, half), :], 0, OWN, z, h, has_r, has_l)
    own_half(0, 0)
    own_half(1, 0)
    to_pair(x_ref, OWN, z)
    xall[OWN, :, cols(t, part)] = x_ref[...]

    expert_id = lax.broadcasted_iota(jnp.int32, (8, rows), 0)
    routes = routes_ref[...]
    weights = rw_ref[...]
    table = jnp.zeros((8, rows), F32)
    for k in range(routes.shape[0]):
        table = table + jnp.where(routes[k : k + 1, :] == expert_id, weights[k : k + 1, :], 0.0)
    shtab[OWN] = table
    remote(shtab.at[OWN], shtab.at[XB], sh_s.at[0], sh_r.at[0], xn)
    remote(shtab.at[OWN], shtab.at[YB], sh_s.at[1], sh_r.at[1], yn)

    loads[4].wait()
    cosine, sine = tab[:, :128], tab[:, 128:]
    at_row = lax.broadcasted_iota(jnp.int32, (128, 128), 0)
    at_col = lax.broadcasted_iota(jnp.int32, (128, 128), 1)
    swapped = at_col + qk // 2 - qk * ((at_col // (qk // 2)) % 2)
    swap = jnp.where(at_row == swapped, 1.0, 0.0).astype(BF16)
    for i in range(kwide // 128):
        span = slice(i * 128, (i + 1) * 128)
        for src, dst in ((q_ref, qrot), (k_ref, None)):
            value = src[:, span]
            turned = low(f32(value) * cosine + mm(value, swap) * sine)
            if dst is None:
                kv[0:rows, span] = turned
            else:
                dst[:, span] = turned
    kv[0:rows, kwide:] = v_ref[...]

    def kv_rows(block, start, count):
        return kv.at[pl.ds(block * rows + start, count), :]

    remote(kv_rows(OWN, 0, rows), kv_rows(XB, 0, rows), kv_s.at[0], kv_r.at[0], xn)
    remote(kv_rows(OWN, 0, rows), kv_rows(YB, 0, rows), kv_s.at[1], kv_r.at[1], yn)

    own_half(0, 1)
    own_half(1, 1)

    def give_down(i):
        src, dst, depth = downs[i]
        for p in range(chips):
            remote(
                src.at[:, cols(2 * p + 1 - c, part)],
                dst.at[cols(c, depth), pl.ds(p * part, part)],
                w_s.at[i, p],
                w_r.at[i, p],
                pt,
            )

    def chunk(block, s, first, weight, target, width):
        tiles = target.shape[-1] // width

        def tile(n, carry):
            span = cols(n, width)
            value = mm(xall[block, :, cols(s, wide)], weight[cols(s, wide), span])
            if not first:
                value = value + target[:, span]
            target[:, span] = value
            return carry

        lax.fori_loop(0, tiles, tile, 0)

    def squares(block, s, first):
        total = jnp.zeros((rows, 128), F32) if first else ssq[block]
        for i in range(wide // 128):
            value = f32(xall[block, :, pl.ds(pl.multiple_of(s * wide + i * 128, 128), 128)])
            total = total + value * value
        ssq[block] = total

    def expert_chunk(block, s, first):
        got(piece(block, s, 1 - c), pt_r.at[block, s])
        chunk(block, s, first, guw, acc.at[block], hidden)
        squares(block, s, first)

    def shared_chunk(s, first):
        chunk(OWN, s, first, sgu, sacc, 2 * shared)

    def activate(block, source, width, target, index):
        full = jnp.sum(ssq[block], axis=1, keepdims=True) / (chips * wide)
        factor = lax.rsqrt(full + NORM_EPS)
        gate = source[:, :width] * factor
        up = source[:, width:] * factor
        target[:, cols(c, width)] = low(gate / (1.0 + jnp.exp(-gate)) * up)
        mine = target.at[:, cols(c, width)]
        remote(mine, mine, h_s.at[index], h_r.at[index], pt)

    def z_arrival(kind, s, h):
        block = (OWN, DB)[kind]
        got(halved(block, s, h), ag_r.at[kind, s, h])
        z_forward(halved(block, s, h), kind, block, s, h, (s < z) & has_r, (s > z) & has_l)
        if h == 1:
            to_pair(piece(block, s, c), block, s)

    def side_arrival(s):
        for i, block in ((0, XB), (1, YB)):
            got(piece(block, s, c), xy_r.at[i, s])
            to_pair(piece(block, s, c), block, s)

    middle = has_l & has_r

    def at_middle(work):
        @pl.when(middle)
        def _():
            work()

    def at_edge(work):
        @pl.when(jnp.logical_not(middle))
        def _():
            work()

    def arrivals(kind, *orders):
        for h in range(2):
            for j in orders:
                z_arrival(kind, nears[j], h)

    got(halved(XB, z, 0), xy_r.at[0, z])
    got(halved(YB, z, 1), xy_r.at[1, z])
    remote(halved(XB, z, 0), halved(DB, z, 0), dr_s.at[0], dr_r.at[0], yn)
    remote(halved(YB, z, 1), halved(DB, z, 1), dr_s.at[1], dr_r.at[1], xn)
    at_middle(lambda: arrivals(0, 0, 1))
    at_edge(lambda: arrivals(0, 0))
    loads[0].wait()
    loads[1].wait()
    expert_chunk(OWN, z, True)
    got(kv_rows(XB, 0, rows), kv_r.at[0])
    got(kv_rows(YB, 0, rows), kv_r.at[1])
    remote(kv_rows(XB, 0, half), kv_rows(DB, 0, half), kv_s.at[2], kv_r.at[2], yn)
    remote(kv_rows(YB, half, half), kv_rows(DB, half, half), kv_s.at[3], kv_r.at[3], xn)
    got(shtab.at[XB], sh_r.at[0])
    got(shtab.at[YB], sh_r.at[1])
    remote(shtab.at[XB], shtab.at[DB], sh_s.at[2], sh_r.at[2], yn)
    to_xy(nears[0])
    at_middle(lambda: to_xy(nears[1]))
    got(halved(XB, z, 1), xy_r.at[0, chips])
    got(halved(YB, z, 0), xy_r.at[1, chips])
    to_pair(piece(XB, z, c), XB, z)
    to_pair(piece(YB, z, c), YB, z)
    at_middle(lambda: arrivals(0, 2))
    at_edge(lambda: arrivals(0, 1))
    at_middle(lambda: to_xy(nears[2]))
    at_edge(lambda: to_xy(nears[1]))
    give_down(0)
    expert_chunk(OWN, nears[0], False)
    loads[2].wait()
    loads[3].wait()
    shared_chunk(z, True)
    got(halved(DB, z, 0), dr_r.at[0])
    got(halved(DB, z, 1), dr_r.at[1])
    for h in range(2):
        z_forward(halved(DB, z, h), 1, DB, z, h, has_r, has_l)
    to_pair(piece(DB, z, c), DB, z)

    def last_own():
        arrivals(0, 2)
        to_xy(nears[2])

    at_edge(last_own)
    give_down(1)
    give_down(2)
    expert_chunk(OWN, nears[1], False)
    got(kv_rows(DB, 0, half), kv_r.at[2])
    got(kv_rows(DB, half, half), kv_r.at[3])
    key_count = kv.shape[0]
    step_rows = 32
    ids = (e, xn[0], yn[0], xn[0] + yn[0] - e)

    def one_map(h, m):
        in_map = (lax.broadcasted_iota(jnp.int32, (rows, 128), 1) // qk) == m
        query = jnp.where(in_map, qrot[:, cols(h, 128)], jnp.zeros((rows, 128), BF16))
        sc_s[...] = lax.dot_general(
            query, kv[:, cols(h, 128)], (((1,), (1,)), ((), ())), preferred_element_type=F32
        )

        def soften(r, carry):
            at = pl.ds(pl.multiple_of(r * step_rows, step_rows), step_rows)
            key = lax.broadcasted_iota(jnp.int32, (step_rows, key_count), 1)
            which = key // rows
            group = jnp.where(
                which == 0, ids[0], jnp.where(which == 1, ids[1], jnp.where(which == 2, ids[2], ids[3]))
            )
            key_at = group * rows + key % rows
            query_at = (
                e * rows + r * step_rows + lax.broadcasted_iota(jnp.int32, (step_rows, key_count), 0)
            )
            scores = jnp.where(key_at <= query_at, sc_s[at, :] * (qk ** (-0.5)), MASKED)
            weight = jnp.exp(scores - jnp.max(scores, axis=1, keepdims=True))
            total = jnp.sum(weight, axis=1, keepdims=True)
            sc_p[at, :] = low(weight)
            sc_t[at, :] = jnp.broadcast_to(total, (step_rows, 128))
            return carry

        lax.fori_loop(0, rows // step_rows, soften, 0)
        return mm(sc_p[...], kv[:, pl.ds(pl.multiple_of(kwide + h * vd, 128), vd)]) / sc_t[...]

    for h in range(local_heads):
        sc_o[...] = one_map(h, 0)
        at_middle(lambda: [z_arrival(1, nears[j], h) for j in (0, 1)])
        mixed = sc_o[...] - lam_ref[h] * one_map(h, 1)
        scale = lax.rsqrt(jnp.mean(mixed * mixed, axis=1, keepdims=True) + NORM_EPS)
        ho[:, pl.ds(pl.multiple_of(c * vwide + h * vd, 128), vd)] = low(mixed * scale * gain_ref[...])
    mine = ho.at[:, cols(c, vwide)]
    remote(mine, mine, h_s.at[5], h_r.at[5], pt)
    at_edge(lambda: arrivals(1, 0))
    side_arrival(nears[0])
    expert_chunk(XB, z, True)
    expert_chunk(YB, z, True)
    for p in range(chips):
        loads[5 + p].wait()
        got(ow.at[cols(1 - c, vwide), pl.ds(p * part, part)], w_r.at[0, p])
    got(ho.at[:, cols(1 - c, vwide)], h_r.at[5])
    for j in range(chips):
        span = cols(fars[j], part)
        macc[:, span] = mm(ho[...], ow[:, span])
    def z_send(kind, j, p, value_of):
        upstream = ((p > z) & has_l) | ((p < z) & has_r)
        slot = zout.at[kind, j]

        @pl.when(upstream)
        def _():
            got(zin.at[kind, p], z_r.at[kind, p])
            zout[kind, j] = low(value_of() + f32(zin[kind, p]))

        @pl.when(jnp.logical_not(upstream))
        def _():
            zout[kind, j] = low(value_of())

        @pl.when(p > z)
        def _():
            remote(slot, zin.at[kind, p], z_s.at[kind, j], z_r.at[kind, p], zr)

        @pl.when((p < z) & (p != z - 1))
        def _():
            remote(slot, zin.at[kind, p], z_s.at[kind, j], z_r.at[kind, p], zl)

        @pl.when((p < z) & (p == z - 1))
        def _():
            remote(slot, zin.at[kind, chips], z_s.at[kind, j], z_r.at[kind, chips], zl)

    def z_finish(kind, value):
        target = (mix_ref, out_ref)[kind]

        @pl.when(has_l)
        def _():
            got(zin.at[kind, z], z_r.at[kind, z])

        @pl.when(has_r)
        def _():
            got(zin.at[kind, chips], z_r.at[kind, chips])

        @pl.when(has_l & has_r)
        def _():
            target[...] = low(value + f32(zin[kind, z]) + f32(zin[kind, chips]))

        @pl.when(jnp.logical_not(has_l))
        def _():
            target[...] = low(value + f32(zin[kind, chips]))

        @pl.when(jnp.logical_not(has_r))
        def _():
            target[...] = low(value + f32(zin[kind, z]))

    def mixer_send(j):
        p = fars[j]
        z_send(0, j, p, lambda: macc[:, cols(p, part)])

    at_edge(lambda: [mixer_send(j) for j in range(chips - 1)])
    at_middle(lambda: arrivals(1, 2))
    expert_chunk(DB, z, True)
    expert_chunk(OWN, nears[2], False)
    activate(OWN, acc.at[OWN], hidden, hid.at[OWN], OWN)
    for j in range(chips - 1):
        shared_chunk(nears[j], False)
    activate(OWN, sacc, shared, shid, 4)
    for block in (XB, YB, DB):
        expert_chunk(block, nears[0], False)
    at_edge(lambda: arrivals(1, 1))
    side_arrival(nears[1])
    for p in range(chips):
        loads[5 + chips + p].wait()
        loads[5 + 2 * chips + p].wait()
        got(sd.at[cols(1 - c, shared), pl.ds(p * part, part)], w_r.at[1, p])
        got(dw.at[cols(1 - c, hidden), pl.ds(p * part, part)], w_r.at[2, p])
    got(hid.at[OWN, :, cols(1 - c, hidden)], h_r.at[OWN])
    got(shid.at[:, cols(1 - c, shared)], h_r.at[4])
    got(shtab.at[DB], sh_r.at[2])
    for block in range(4):
        line = jnp.sum(jnp.where(expert_id == e, shtab[block], 0.0), axis=0, keepdims=True)
        shcol[block] = jnp.broadcast_to(line, (128, rows)).T

    def own_down(p, carry):
        span = cols(p, part)
        oacc[:, span] = mm(hid[OWN], dw[:, span]) * shcol[OWN, :, 0:1] + mm(shid[...], sd[:, span])
        return carry

    for block in (XB, YB, DB):
        expert_chunk(block, nears[1], False)
    lax.fori_loop(0, chips, own_down, 0)
    at_edge(lambda: arrivals(1, 2))
    side_arrival(nears[2])
    for block in (DB, XB, YB):
        expert_chunk(block, nears[2], False)
        activate(block, acc.at[block], hidden, hid.at[block], block)

    def down(block, p):
        return mm(hid[block], dw[:, cols(p, part)]) * shcol[block, :, 0:1]

    top, rest = pl.ds(0, half), pl.ds(half, half)
    sides = ((0, XB, 0, 1, xn), (1, YB, 1, 0, yn))

    def far_share(j):
        span = cols(fars[j], part)
        dsend[:, span] = low(down(DB, fars[j]))
        remote(dsend.at[top, span], din.at[0, :, span], d_s.at[0, j], d_r.at[0, j], xn)
        remote(dsend.at[rest, span], din.at[1, :, span], d_s.at[1, j], d_r.at[1, j], yn)

    def early_share(j):
        span = cols(fars[j], part)
        for i, block, now, later, dev in sides:
            value = down(block, fars[j])
            esend[i, :, span] = low(value[now * half : (now + 1) * half])
            late[i, :, span] = value[later * half : (later + 1) * half]
            target = xyin.at[i, pl.ds(now * half, half), span]
            remote(esend.at[i, :, span], target, e_s.at[i, 0, j], e_r.at[i, 0, j], dev)

    def late_share(j):
        span = cols(fars[j], part)
        for i, block, now, later, dev in sides:
            got(din.at[1 - i, :, span], d_r.at[1 - i, j])
            lsend[i, :, span] = low(late[i, :, span] + f32(din[1 - i, :, span]))
            target = xyin.at[i, pl.ds(later * half, half), span]
            remote(lsend.at[i, :, span], target, e_s.at[i, 1, j], e_r.at[i, 1, j], dev)

    def total_share(j):
        span = cols(fars[j], part)
        for i, block, now, later, dev in sides:
            got(xyin.at[i, pl.ds(now * half, half), span], e_r.at[i, 0, j])
            got(xyin.at[i, pl.ds(later * half, half), span], e_r.at[i, 1, j])

        def total():
            return oacc[:, span] + f32(xyin[0, :, span]) + f32(xyin[1, :, span])

        if j < chips - 1:
            z_send(1, j, fars[j], total)
        else:
            z_finish(1, total())

    got(hid.at[DB, :, cols(1 - c, hidden)], h_r.at[DB])
    far_share(0)
    got(hid.at[XB, :, cols(1 - c, hidden)], h_r.at[XB])
    got(hid.at[YB, :, cols(1 - c, hidden)], h_r.at[YB])
    early_share(0)
    far_share(1)
    at_middle(lambda: mixer_send(0))
    late_share(0)
    early_share(1)
    far_share(2)
    at_middle(lambda: mixer_send(1))
    late_share(1)
    early_share(2)
    far_share(3)
    at_middle(lambda: mixer_send(2))
    total_share(0)
    late_share(2)
    early_share(3)
    total_share(1)
    late_share(3)
    z_finish(0, macc[:, cols(z, part)])
    total_share(2)
    total_share(3)

    for kind, block in ((0, OWN), (1, DB)):
        for s in range(chips):

            @pl.when(has_r & (s <= z))
            def _():
                for h in range(2):
                    sent(halved(block, s, h), ag_s.at[kind, 0, s, h])

            @pl.when(has_l & (s >= z))
            def _():
                for h in range(2):
                    sent(halved(block, s, h), ag_s.at[kind, 1, s, h])

    for i in range(2):
        sent(halved(OWN, z, 0), xy_s.at[i, z])
        sent(halved(OWN, z, 0), xy_s.at[i, chips])
        for j in range(chips - 1):
            sent(piece(OWN, nears[j], c), xy_s.at[i, nears[j]])
    for s in range(chips):
        for block in range(4):
            sent(piece(block, s, c), pt_s.at[block, s])
    for i in range(2):
        sent(halved(DB, z, i), dr_s.at[i])
        sent(kv_rows(OWN, 0, rows), kv_s.at[i])
        sent(kv_rows(OWN, 0, half), kv_s.at[2 + i])
    for i in range(3):
        sent(shtab.at[OWN], sh_s.at[i])
        for p in range(chips):
            src, dst, depth = downs[i]
            sent(dst.at[cols(c, depth), pl.ds(p * part, part)], w_s.at[i, p])
    for block in range(4):
        sent(hid.at[block, :, cols(c, hidden)], h_s.at[block])
    sent(shid.at[:, cols(c, shared)], h_s.at[4])
    sent(ho.at[:, cols(c, vwide)], h_s.at[5])
    for i in range(2):
        for j in range(chips):
            sent(dsend.at[top, pl.ds(j * part, part)], d_s.at[i, j])
            sent(esend.at[i, :, pl.ds(j * part, part)], e_s.at[i, 0, j])
            sent(lsend.at[i, :, pl.ds(j * part, part)], e_s.at[i, 1, j])
        for j in range(chips - 1):
            sent(zout.at[i, j], z_s.at[i, j])


def rotation_table(positions, key_width):
    half_width = key_width // 2
    freq = np.float32(ROPE_BASE) ** (-np.arange(half_width, dtype=np.float32) / np.float32(half_width))
    angles = np.arange(positions, dtype=np.float32)[:, None] * freq.astype(np.float32)[None, :]
    angles = angles.astype(np.float64)
    cosine, sine = np.cos(angles), np.sin(angles)
    copies = 128 // key_width
    cosine = np.tile(np.concatenate([cosine, cosine], axis=1), (1, copies))
    sine = np.tile(np.concatenate([-sine, sine], axis=1), (1, copies))
    return np.concatenate([cosine, sine], axis=1).astype(np.float32)


def kernel_body(
    query_heads,
    key_heads,
    value_heads,
    diff_lambda,
    sub_gain,
    out_weight,
    routed_input,
    routes,
    route_weights,
    expert_gate,
    expert_up,
    expert_down,
    shared_gate,
    shared_up,
    shared_down,
):
    rows, part = routed_input.shape
    chips = lax.axis_size("tp") // 2
    groups = lax.axis_size("ep")
    gate, up, down = expert_gate[0], expert_up[0], expert_down[0]
    width, hidden = gate.shape
    shared = shared_gate.shape[1]
    kwide, vwide = key_heads.shape[1], value_heads.shape[1]
    local_heads = diff_lambda.shape[0]
    half, mine = rows // 2, width // 2
    table = jnp.asarray(rotation_table(groups * rows, kwide // (2 * local_heads)))
    vmem = pl.BlockSpec(memory_space=pltpu.VMEM)
    smem = pl.BlockSpec(memory_space=pltpu.SMEM)
    hbm = pl.BlockSpec(memory_space=pl.ANY)
    dma = pltpu.SemaphoreType.DMA
    out = jax.ShapeDtypeStruct((rows, part), BF16)
    return pl.pallas_call(
        functools.partial(layer_kernel, chips),
        out_shape=(out, out),
        in_specs=[vmem, vmem, vmem, smem, vmem, vmem, vmem, vmem] + [hbm] * 8,
        out_specs=(vmem, vmem),
        scratch_shapes=[
            pltpu.VMEM((groups, rows, width), BF16),
            pltpu.VMEM((width, 2 * hidden), BF16),
            pltpu.VMEM((2 * hidden, mine), BF16),
            pltpu.VMEM((width, 2 * shared), BF16),
            pltpu.VMEM((2 * shared, mine), BF16),
            pltpu.VMEM((2 * vwide, mine), BF16),
            pltpu.VMEM((rows, 256), F32),
            pltpu.VMEM((groups, rows, 2 * hidden), F32),
            pltpu.VMEM((rows, 2 * shared), F32),
            pltpu.VMEM((groups, rows, 128), F32),
            pltpu.VMEM((groups, rows, 2 * hidden), BF16),
            pltpu.VMEM((rows, 2 * shared), BF16),
            pltpu.VMEM((rows, mine), F32),
            pltpu.VMEM((rows, mine), BF16),
            pltpu.VMEM((2, half, mine), BF16),
            pltpu.VMEM((2, half, mine), BF16),
            pltpu.VMEM((2, half, mine), F32),
            pltpu.VMEM((2, half, mine), BF16),
            pltpu.VMEM((2, rows, mine), BF16),
            pltpu.VMEM((2, chips + 1, rows, part), BF16),
            pltpu.VMEM((2, chips - 1, rows, part), BF16),
            pltpu.VMEM((rows, mine), F32),
            pltpu.VMEM((groups * rows, kwide + vwide), BF16),
            pltpu.VMEM((rows, kwide), BF16),
            pltpu.VMEM((rows, groups * rows), F32),
            pltpu.VMEM((rows, groups * rows), BF16),
            pltpu.VMEM((rows, 128), F32),
            pltpu.VMEM((rows, 128), F32),
            pltpu.VMEM((rows, 2 * vwide), BF16),
            pltpu.VMEM((groups, 8, rows), F32),
            pltpu.VMEM((groups, rows, 128), F32),
            dma((5 + 3 * chips,)),
            dma((3, chips)),
            dma((3, chips)),
            dma((2, 2, chips, 2)),
            dma((2, chips, 2)),
            dma((2, chips + 1)),
            dma((2, chips + 1)),
            dma((2,)),
            dma((2,)),
            dma((4, chips)),
            dma((4, chips)),
            dma((4,)),
            dma((4,)),
            dma((3,)),
            dma((3,)),
            dma((6,)),
            dma((6,)),
            dma((2, chips)),
            dma((2, chips)),
            dma((2, 2, chips)),
            dma((2, 2, chips)),
            dma((2, chips - 1)),
            dma((2, chips + 1)),
        ],
        compiler_params=pltpu.CompilerParams(
            collective_id=0, has_side_effects=True, vmem_limit_bytes=67043328
        ),
        name="layer",
    )(
        query_heads,
        key_heads,
        value_heads,
        diff_lambda,
        sub_gain[None, :],
        routed_input,
        routes.T,
        route_weights.T,
        table,
        out_weight,
        gate,
        up,
        down,
        shared_gate,
        shared_up,
        shared_down,
    )


def solution(mesh):
    dense = mesh.shape["ep"] == 4 and mesh.shape["tp"] == 8

    def chosen(*arguments):
        fits = dense and arguments[9].shape[0] == 1 and arguments[6].shape[0] % 32 == 0
        return (kernel_body if fits else body)(*arguments)

    placed = (
        P("ep", "tp"),
        P("ep", "tp"),
        P("ep", "tp"),
        P("tp"),
        P(),
        P("tp", None),
        P("ep", "tp"),
        P("ep", None),
        P("ep", None),
        P("ep", None, "tp"),
        P("ep", None, "tp"),
        P("ep", "tp", None),
        P(None, "tp"),
        P(None, "tp"),
        P("tp", None),
    )
    return jax.shard_map(
        chosen, mesh=mesh, in_specs=placed, out_specs=(P("ep", "tp"), P("ep", "tp")), check_vma=False
    )
```

```python
import functools

import jax
import jax.numpy as jnp
import numpy as np
from jax import lax
from jax.experimental import pallas as pl
from jax.experimental.pallas import tpu as pltpu
from jax.sharding import PartitionSpec as P

ROPE_BASE = 10000.0
NORM_EPS = 1e-06
MASKED = -1e30


def rotate(values, positions):
    half_width = values.shape[-1] // 2
    inverse_freq = ROPE_BASE ** (-jnp.arange(half_width, dtype=jnp.float32) / half_width)
    angles = positions.astype(jnp.float32)[:, None] * inverse_freq[None, :]
    angles = angles.reshape((angles.shape[0],) + (1,) * (values.ndim - 2) + (half_width,))
    cosine = jnp.cos(angles)
    sine_part = jnp.sin(angles)
    lower = values[..., :half_width]
    upper = values[..., half_width:]
    return jnp.concatenate(
        [lower * cosine - upper * sine_part, upper * cosine + lower * sine_part], axis=-1
    )


def mixer_terms(query_heads, key_heads, value_heads, diff_lambda, sub_gain, out_weight):
    row_count = query_heads.shape[0]
    local_heads = diff_lambda.shape[0]
    value_width = value_heads.shape[1] // local_heads
    key_width = query_heads.shape[1] // (2 * local_heads)
    score_scale = key_width ** (-0.5)
    offset = lax.axis_index("ep") * row_count
    positions = offset + jnp.arange(row_count, dtype=jnp.int32)
    last_row = offset + row_count - 1
    query_rot = rotate(
        query_heads.astype(jnp.float32).reshape(row_count, local_heads, 2, key_width), positions
    ).astype(jnp.bfloat16)
    queries = jnp.transpose(query_rot, (1, 2, 0, 3))
    key_rot = (
        rotate(
            key_heads.astype(jnp.float32).reshape(row_count, local_heads, 2, key_width), positions
        )
        .astype(jnp.bfloat16)
        .reshape(row_count, local_heads * 2 * key_width)
    )
    start_state = (
        jnp.full((local_heads, 2, row_count), MASKED, jnp.float32),
        jnp.zeros((local_heads, 2, row_count), jnp.float32),
        jnp.zeros((local_heads, 2, row_count, value_width), jnp.float32),
    )
    carried = start_state
    key_piece = lax.all_gather(key_rot, "ep", axis=0, tiled=True)
    value_piece = lax.all_gather(value_heads, "ep", axis=0, tiled=True)
    piece_rows = key_piece.shape[0]
    key_block = 512
    block_count = piece_rows // key_block
    key_blocks = key_piece.reshape(block_count, key_block, local_heads, 2, key_width)
    value_blocks = value_piece.reshape(block_count, key_block, local_heads, value_width)

    def block_step(running, block_item):
        key_rows, value_rows, block_index = block_item
        block_start = block_index * key_block

        def attend_block(partial_state):
            maxima, totals, weighted = partial_state
            key_positions = block_start + jnp.arange(key_block, dtype=jnp.int32)
            visible = key_positions[None, :] <= positions[:, None]
            scores = (
                jnp.einsum("hmqd,khmd->hmqk", queries, key_rows, preferred_element_type=jnp.float32)
                * score_scale
            )
            scores = jnp.where(visible, scores, MASKED)
            new_maxima = jnp.maximum(maxima, jnp.max(scores, axis=3))
            exp_weights = jnp.where(visible, jnp.exp(scores - new_maxima[..., None]), 0.0)
            shrink = jnp.exp(maxima - new_maxima)
            new_totals = totals * shrink + jnp.sum(exp_weights, axis=3)
            update = jnp.einsum(
                "hmqk,khw->hmqw",
                exp_weights.astype(jnp.bfloat16),
                value_rows,
                preferred_element_type=jnp.float32,
            )
            return (new_maxima, new_totals, weighted * shrink[..., None] + update)

        return (
            lax.cond(
                block_start <= last_row, attend_block, lambda partial_state: partial_state, running
            ),
            None,
        )

    carried, _ = lax.scan(
        block_step, carried, (key_blocks, value_blocks, jnp.arange(block_count, dtype=jnp.int32))
    )
    maxima, totals, weighted = carried
    attended = weighted / totals[..., None]
    mixed_heads = attended[:, 0] - diff_lambda[:, None, None] * attended[:, 1]
    normed = (
        mixed_heads
        * lax.rsqrt(jnp.mean(mixed_heads * mixed_heads, axis=2, keepdims=True) + NORM_EPS)
        * sub_gain
    )
    heads_out = jnp.transpose(normed.astype(jnp.bfloat16), (1, 0, 2)).reshape(
        row_count, local_heads * value_width
    )
    return jnp.dot(heads_out, out_weight, preferred_element_type=jnp.float32)


def expert_terms(
    routed_input, routes, expert_gate, expert_up, expert_down, shared_gate, shared_up, shared_down
):
    row_count, part_width = routed_input.shape
    top_count = routes.shape[1]
    local_experts = expert_gate.shape[0]
    groups = lax.axis_size("ep")
    experts = local_experts * groups
    capacity = 2 * row_count * top_count // experts
    copies = row_count * top_count
    flat_routes = routes.reshape(copies)
    onehot = (flat_routes[:, None] == jnp.arange(experts, dtype=jnp.int32)[None, :]).astype(
        jnp.int32
    )
    rank_within = jnp.sum((jnp.cumsum(onehot, axis=0) - onehot) * onehot, axis=1)
    slot_index = flat_routes * capacity + rank_within
    placer = (
        slot_index[:, None] == jnp.arange(experts * capacity, dtype=jnp.int32)[None, :]
    ).astype(jnp.bfloat16)
    token_slots = jnp.sum(placer.reshape(row_count, top_count, experts * capacity), axis=1)
    outgoing = jnp.dot(token_slots.T, routed_input, preferred_element_type=jnp.float32).astype(
        jnp.bfloat16
    )
    arrived = lax.all_to_all(
        outgoing.reshape(groups, local_experts * capacity, part_width),
        "ep",
        split_axis=0,
        concat_axis=0,
        tiled=True,
    )
    slot_count = groups * capacity
    slot_rows = jnp.transpose(
        arrived.reshape(groups, local_experts, capacity, part_width), (1, 0, 2, 3)
    ).reshape(local_experts, slot_count, part_width)
    slot_piece = lax.all_gather(slot_rows, "tp", axis=2, tiled=True)
    own_piece = lax.all_gather(routed_input[None], "tp", axis=2, tiled=True)
    own_rows = own_piece[0]
    gate_sum = jnp.einsum(
        "emc,ecf->emf", slot_piece, expert_gate, preferred_element_type=jnp.float32
    )
    up_sum = jnp.einsum("emc,ecf->emf", slot_piece, expert_up, preferred_element_type=jnp.float32)
    square_sum = jnp.sum(jnp.square(slot_piece.astype(jnp.float32)), axis=2)
    shared_gate_sum = jnp.dot(own_rows, shared_gate, preferred_element_type=jnp.float32)
    shared_up_sum = jnp.dot(own_rows, shared_up, preferred_element_type=jnp.float32)
    shared_square = jnp.sum(jnp.square(own_rows.astype(jnp.float32)), axis=1)
    full_width = expert_gate.shape[1]
    factor = lax.rsqrt(square_sum / full_width + NORM_EPS)[..., None]
    hidden = (jax.nn.silu(gate_sum * factor) * (up_sum * factor)).astype(jnp.bfloat16)
    shared_factor = lax.rsqrt(shared_square / full_width + NORM_EPS)[:, None]
    shared_hidden = (
        jax.nn.silu(shared_gate_sum * shared_factor) * (shared_up_sum * shared_factor)
    ).astype(jnp.bfloat16)
    shared_terms = jnp.dot(shared_hidden, shared_down, preferred_element_type=jnp.float32)
    routed_terms = jnp.einsum(
        "emf,efd->emd", hidden, expert_down, preferred_element_type=jnp.float32
    )
    routed_sum = lax.psum_scatter(
        routed_terms.astype(jnp.bfloat16), "tp", scatter_dimension=2, tiled=True
    ).astype(jnp.float32)
    return (routed_sum, shared_terms, placer)


def expert_finish(routed_sum, shared_sum, placer, route_weights):
    local_experts, slot_count, part_width = routed_sum.shape
    groups = lax.axis_size("ep")
    capacity = slot_count // groups
    leaving = jnp.transpose(
        routed_sum.astype(jnp.bfloat16).reshape(local_experts, groups, capacity, part_width),
        (1, 0, 2, 3),
    ).reshape(groups, local_experts * capacity, part_width)
    returned = lax.all_to_all(leaving, "ep", split_axis=0, concat_axis=0, tiled=True)
    copy_results = jnp.dot(
        placer,
        returned.reshape(groups * local_experts * capacity, part_width),
        preferred_element_type=jnp.float32,
    )
    row_count, top_count = route_weights.shape
    routed = jnp.sum(
        copy_results.reshape(row_count, top_count, part_width) * route_weights[:, :, None], axis=1
    )
    return (routed + shared_sum).astype(jnp.bfloat16)


def body(
    query_heads,
    key_heads,
    value_heads,
    diff_lambda,
    sub_gain,
    out_weight,
    routed_input,
    routes,
    route_weights,
    expert_gate,
    expert_up,
    expert_down,
    shared_gate,
    shared_up,
    shared_down,
):
    mixer_partial = mixer_terms(
        query_heads, key_heads, value_heads, diff_lambda, sub_gain, out_weight
    )
    routed_sum, shared_terms, placer = expert_terms(
        routed_input,
        routes,
        expert_gate,
        expert_up,
        expert_down,
        shared_gate,
        shared_up,
        shared_down,
    )
    mixer_sum, shared_sum = (
        lax.psum_scatter(
            mixer_partial.astype(jnp.bfloat16), "tp", scatter_dimension=1, tiled=True
        ).astype(jnp.float32),
        lax.psum_scatter(
            shared_terms.astype(jnp.bfloat16), "tp", scatter_dimension=1, tiled=True
        ).astype(jnp.float32),
    )
    return (
        mixer_sum.astype(jnp.bfloat16),
        expert_finish(routed_sum, shared_sum, placer, route_weights),
    )


MESH = pl.DeviceIdType.MESH
F32 = jnp.float32
BF16 = jnp.bfloat16
OWN, XB, YB, DB = 0, 1, 2, 3


def low(value):
    return value.astype(BF16)


def f32(value):
    return value.astype(F32)


def mm(left, right):
    return jnp.dot(left, right, preferred_element_type=F32)


def near_first(chips):
    rows = [sorted((s for s in range(chips) if s != z), key=lambda s: (abs(s - z), s if z < chips // 2 else -s)) for z in range(chips)]
    return [[row[j] for row in rows] for j in range(chips - 1)]


def far_first(chips):
    rows = []
    for z in range(chips):
        right = list(range(chips - 1, z, -1))
        left = list(range(0, z))
        first, second = (right, left) if z < chips // 2 else (left, right)
        row = []
        while first or second:
            if first:
                row.append(first.pop(0))
            if second:
                row.append(second.pop(0))
        rows.append(row)
    return [[row[j] for row in rows] for j in range(chips - 1)]


def layer_kernel(
    chips,
    q_ref,
    k_ref,
    v_ref,
    lam_ref,
    gain_ref,
    x_ref,
    routes_ref,
    rw_ref,
    tab_hbm,
    ow_hbm,
    gw_hbm,
    uw_hbm,
    dw_hbm,
    sg_hbm,
    su_hbm,
    sd_hbm,
    mix_ref,
    out_ref,
    xall,
    guw,
    dw,
    sgu,
    sd,
    ow,
    tab,
    acc,
    sacc,
    ssq,
    hid,
    shid,
    oacc,
    dsend,
    esend,
    lsend,
    late,
    din,
    xyin,
    zin,
    zout,
    macc,
    kv,
    qrot,
    sc_s,
    sc_p,
    sc_m,
    sc_t,
    sc_o,
    sc_a,
    ho,
    shtab,
    shcol,
    w_l,
    w_s,
    w_r,
    ag_s,
    ag_r,
    xy_s,
    xy_r,
    dr_s,
    dr_r,
    pt_s,
    pt_r,
    kv_s,
    kv_r,
    sh_s,
    sh_r,
    h_s,
    h_r,
    d_s,
    d_r,
    e_s,
    e_r,
    z_s,
    z_r,
):
    rows, part = x_ref.shape
    half = rows // 2
    wide = 2 * part
    hidden = gw_hbm.shape[1]
    shared = sg_hbm.shape[1]
    vwide = v_ref.shape[1]
    kwide = k_ref.shape[1]
    local_heads = lam_ref.shape[0]
    vd = vwide // local_heads
    qk = kwide // (2 * local_heads)
    e = lax.axis_index("ep")
    t = lax.axis_index("tp")
    z, c = t // 2, t % 2
    x, y = e % 2, e // 2
    pt = (e, t + 1 - 2 * c)
    xn = (e + 1 - 2 * x, t)
    yn = (e + 2 - 4 * y, t)
    zr = (e, t + 2)
    zl = (e, t - 2)
    has_r = z < chips - 1
    has_l = z > 0

    def chosen_by_z(column):
        return sum(order * (z == at).astype(jnp.int32) for at, order in enumerate(column))

    nears = [chosen_by_z(column) for column in near_first(chips)]
    fars = [chosen_by_z(column) for column in far_first(chips)] + [z]

    def remote(src, dst, send, recv, dev):
        pltpu.make_async_remote_copy(src, dst, send, recv, device_id=dev, device_id_type=MESH).start()

    def got(dst, recv):
        pltpu.make_async_remote_copy(dst, dst, recv, recv, device_id=pt, device_id_type=MESH).wait_recv()

    def sent(src, send):
        pltpu.make_async_remote_copy(src, src, send, send, device_id=pt, device_id_type=MESH).wait_send()

    def cols(index, width):
        return pl.ds(pl.multiple_of(index * width, width), width)

    barrier = pltpu.get_barrier_semaphore()
    for dev in (pt, xn, yn):
        pl.semaphore_signal(barrier, inc=1, device_id=dev, device_id_type=MESH)

    @pl.when(has_r)
    def _():
        pl.semaphore_signal(barrier, inc=1, device_id=zr, device_id_type=MESH)

    @pl.when(has_l)
    def _():
        pl.semaphore_signal(barrier, inc=1, device_id=zl, device_id_type=MESH)

    loads = [
        pltpu.make_async_copy(gw_hbm, guw.at[:, pl.ds(0, hidden)], w_l.at[0]),
        pltpu.make_async_copy(uw_hbm, guw.at[:, pl.ds(hidden, hidden)], w_l.at[1]),
        pltpu.make_async_copy(sg_hbm, sgu.at[:, pl.ds(0, shared)], w_l.at[2]),
        pltpu.make_async_copy(su_hbm, sgu.at[:, pl.ds(shared, shared)], w_l.at[3]),
        pltpu.make_async_copy(tab_hbm.at[pl.ds(pl.multiple_of(e * rows, rows), rows), :], tab, w_l.at[4]),
    ]
    downs = [(ow_hbm, ow, vwide), (sd_hbm, sd, shared), (dw_hbm, dw, hidden)]
    for i, (src, dst, depth) in enumerate(downs):
        for p in range(chips):
            loads.append(
                pltpu.make_async_copy(
                    src.at[:, cols(2 * p + c, part)],
                    dst.at[cols(c, depth), pl.ds(p * part, part)],
                    w_l.at[5 + i * chips + p],
                )
            )
    loads[4].start()
    for i in list(range(4)) + list(range(5, len(loads))):
        loads[i].start()


    def piece(block, s, core):
        return xall.at[pl.ds(block * rows, rows), cols(2 * s + core, part)]

    def halved(block, s, h):
        return xall.at[pl.ds(block * rows + h * half, half), cols(2 * s + c, part)]

    def z_forward(src, kind, block, s, h, right, left):
        @pl.when(right)
        def _():
            remote(src, halved(block, s, h), ag_s.at[kind, 0, s, h], ag_r.at[kind, s, h], zr)

        @pl.when(left)
        def _():
            remote(src, halved(block, s, h), ag_s.at[kind, 1, s, h], ag_r.at[kind, s, h], zl)

    def to_pair(src, block, s):
        remote(src, piece(block, s, c), pt_s.at[block, s], pt_r.at[block, s], pt)

    def to_xy(s):
        remote(piece(OWN, s, c), piece(XB, s, c), xy_s.at[0, s], xy_r.at[0, s], xn)
        remote(piece(OWN, s, c), piece(YB, s, c), xy_s.at[1, s], xy_r.at[1, s], yn)

    def own_half(i, order):
        h = order if i == 0 else 1 - order
        block, dev = ((XB, xn), (YB, yn))[i]
        slot = z if order == 0 else chips
        remote(x_ref.at[pl.ds(h * half, half), :], halved(block, z, h), xy_s.at[i, slot], xy_r.at[i, slot], dev)

    loads[4].wait()
    cosine, sine = tab[:, :128], tab[:, 128:]
    at_row = lax.broadcasted_iota(jnp.int32, (128, 128), 0)
    at_col = lax.broadcasted_iota(jnp.int32, (128, 128), 1)
    swapped = at_col + qk // 2 - qk * ((at_col // (qk // 2)) % 2)
    swap = jnp.where(at_row == swapped, 1.0, 0.0).astype(BF16)
    for i in range(kwide // 128):
        span = slice(i * 128, (i + 1) * 128)
        for src, dst in ((q_ref, qrot), (k_ref, None)):
            value = src[:, span]
            turned = low(f32(value) * cosine + mm(value, swap) * sine)
            if dst is None:
                kv[0:rows, span] = turned
            else:
                turned = turned * jnp.asarray(qk ** (-0.5), BF16)
                for m in range(2):
                    in_map = (lax.broadcasted_iota(jnp.int32, (rows, 128), 1) // qk) == m
                    dst[2 * i + m] = jnp.where(in_map, turned, jnp.zeros((rows, 128), BF16))
    kv[0:rows, kwide:] = v_ref[...]

    pl.semaphore_wait(barrier, 3 + has_r.astype(jnp.int32) + has_l.astype(jnp.int32))

    for h in range(2):
        z_forward(x_ref.at[pl.ds(h * half, half), :], 0, OWN, z, h, has_r, has_l)
    own_half(0, 0)
    own_half(1, 0)
    to_pair(x_ref, OWN, z)
    xall[0:rows, cols(t, part)] = x_ref[...]

    expert_id = lax.broadcasted_iota(jnp.int32, (8, rows), 0)
    routes = routes_ref[...]
    weights = rw_ref[...]
    table = jnp.zeros((8, rows), F32)
    for k in range(routes.shape[0]):
        table = table + jnp.where(routes[k : k + 1, :] == expert_id, weights[k : k + 1, :], 0.0)
    shtab[OWN] = table
    remote(shtab.at[OWN], shtab.at[XB], sh_s.at[0], sh_r.at[0], xn)
    remote(shtab.at[OWN], shtab.at[YB], sh_s.at[1], sh_r.at[1], yn)

    def kv_rows(block, start, count):
        return kv.at[pl.ds(block * rows + start, count), :]

    remote(kv_rows(OWN, 0, rows), kv_rows(XB, 0, rows), kv_s.at[0], kv_r.at[0], xn)
    remote(kv_rows(OWN, 0, rows), kv_rows(YB, 0, rows), kv_s.at[1], kv_r.at[1], yn)

    own_half(0, 1)
    own_half(1, 1)

    def give_down(i):
        src, dst, depth = downs[i]
        for p in range(chips):
            remote(
                src.at[:, cols(2 * p + 1 - c, part)],
                dst.at[cols(c, depth), pl.ds(p * part, part)],
                w_s.at[i, p],
                w_r.at[i, p],
                pt,
            )

    def chunk(block, count, at, depth, first, weight, target, base, width):
        tiles = target.shape[-1] // width
        left_rows, target_rows = pl.ds(block * rows, count * rows), pl.ds(base * rows, count * rows)

        def tile(n, carry):
            span = cols(n, width)
            value = mm(xall[left_rows, cols(at, depth)], weight[cols(at, depth), span])
            if not first:
                value = value + target[target_rows, span]
            target[target_rows, span] = value
            return carry

        lax.fori_loop(0, tiles, tile, 0)

    def squares(block, count, at, depth, first):
        span = pl.ds(block * rows, count * rows)
        total = jnp.zeros((count * rows, 128), F32) if first else ssq[span, :]
        for i in range(depth // 128):
            value = f32(xall[span, pl.ds(pl.multiple_of(at * depth + i * 128, 128), 128)])
            total = total + value * value
        ssq[span, :] = total

    def expert_chunk(block, s, first, count=1):
        for b in range(block, block + count):
            got(piece(b, s, 1 - c), pt_r.at[b, s])
        chunk(block, count, s, wide, first, guw, acc, block, hidden)
        squares(block, count, s, wide, first)

    def expert_half(block, s, core, count=1):
        if core is not c:
            for b in range(block, block + count):
                got(piece(b, s, 1 - c), pt_r.at[b, s])
        chunk(block, count, 2 * s + core, part, False, guw, acc, block, hidden)
        squares(block, count, 2 * s + core, part, False)

    def shared_chunk(s, first):
        chunk(OWN, 1, s, wide, first, sgu, sacc, 0, 2 * shared)

    def activate(block, source, width, target, index):
        full = jnp.sum(ssq[pl.ds(block * rows, rows), :], axis=1, keepdims=True) / (chips * wide)
        factor = lax.rsqrt(full + NORM_EPS)
        gate = source[:, :width] * factor
        up = source[:, width:] * factor
        target[:, cols(c, width)] = low(gate / (1.0 + jnp.exp(-gate)) * up)
        mine = target.at[:, cols(c, width)]
        remote(mine, mine, h_s.at[index], h_r.at[index], pt)

    def z_arrival(kind, s, h):
        block = (OWN, DB)[kind]
        got(halved(block, s, h), ag_r.at[kind, s, h])
        z_forward(halved(block, s, h), kind, block, s, h, (s < z) & has_r, (s > z) & has_l)
        if h == 1:
            to_pair(piece(block, s, c), block, s)

    def side_arrival(s):
        for i, block in ((0, XB), (1, YB)):
            got(piece(block, s, c), xy_r.at[i, s])
            to_pair(piece(block, s, c), block, s)

    middle = has_l & has_r

    def at_middle(work):
        @pl.when(middle)
        def _():
            work()

    def at_edge(work):
        @pl.when(jnp.logical_not(middle))
        def _():
            work()

    def arrivals(kind, *orders):
        for h in range(2):
            for j in orders:
                z_arrival(kind, nears[j], h)

    def value_cols(h):
        return pl.ds(kwide + h * vd, vd)

    step_rows = 64
    ids = (e, xn[0], yn[0], xn[0] + yn[0] - e)
    bias = [jnp.where(ids[b] < e, 0.0, MASKED) for b in range(4)]

    def attend_first(i):
        count = 3 * rows
        sc_s[...] = lax.dot_general(
            qrot[i], kv[0:count, cols(i // 2, 128)], (((1,), (1,)), ((), ())), preferred_element_type=F32
        )

        for r in range(0, rows, step_rows):
            at = slice(r, r + step_rows)
            key = lax.broadcasted_iota(jnp.int32, (step_rows, rows), 1)
            row = r + lax.broadcasted_iota(jnp.int32, (step_rows, rows), 0)
            scores = [
                jnp.where(key <= row, sc_s[at, 0:rows], MASKED),
                sc_s[at, rows : 2 * rows] + bias[XB],
                sc_s[at, 2 * rows :] + bias[YB],
            ]
            most = jnp.maximum(jnp.maximum(scores[0], scores[1]), scores[2])
            most = jnp.max(most, axis=1, keepdims=True)
            weight = [jnp.exp(score - most) for score in scores]
            total = jnp.sum(weight[0] + weight[1] + weight[2], axis=1, keepdims=True)
            for b in range(3):
                sc_p[at, b * rows : (b + 1) * rows] = low(weight[b])
            sc_m[i, at, :] = jnp.broadcast_to(most, (step_rows, 128))
            sc_t[i, at, :] = jnp.broadcast_to(total, (step_rows, 128))

        sc_o[i] = mm(sc_p[...], kv[0:count, value_cols(i // 2)])

    def attend_last(i):
        count = 3 * rows
        sc_s[:, 0:rows] = lax.dot_general(
            qrot[i], kv[count:, cols(i // 2, 128)], (((1,), (1,)), ((), ())), preferred_element_type=F32
        )

        for r in range(0, rows, step_rows):
            at = slice(r, r + step_rows)
            scores = sc_s[at, 0:rows] + bias[DB]
            before = sc_m[i, at, :]
            most = jnp.maximum(before, jnp.max(scores, axis=1, keepdims=True))
            weight = jnp.exp(scores - most[:, 0:1])
            shrink = jnp.exp(before - most)
            sc_p[at, 0:rows] = low(weight)
            sc_a[at, :] = shrink
            sc_t[i, at, :] = sc_t[i, at, :] * shrink + jnp.sum(weight, axis=1, keepdims=True)

        return (sc_o[i] * sc_a[...] + mm(sc_p[:, 0:rows], kv[count:, value_cols(i // 2)])) / sc_t[i]

    def finish_head(h):
        sc_o[2 * h] = attend_last(2 * h)
        mixed = sc_o[2 * h] - lam_ref[h] * attend_last(2 * h + 1)
        scale = lax.rsqrt(jnp.mean(mixed * mixed, axis=1, keepdims=True) + NORM_EPS)
        ho[:, pl.ds(pl.multiple_of(c * vwide + h * vd, 128), vd)] = low(mixed * scale * gain_ref[...])

    loads[0].wait()
    loads[1].wait()
    expert_chunk(OWN, z, True)
    at_middle(lambda: [z_arrival(0, nears[j], 0) for j in (0, 1)])
    loads[2].wait()
    loads[3].wait()
    shared_chunk(z, True)
    got(halved(XB, z, 0), xy_r.at[0, z])
    got(halved(YB, z, 1), xy_r.at[1, z])
    remote(halved(XB, z, 0), halved(DB, z, 0), dr_s.at[0], dr_r.at[0], yn)
    remote(halved(YB, z, 1), halved(DB, z, 1), dr_s.at[1], dr_r.at[1], xn)
    at_middle(lambda: [z_arrival(0, nears[j], 1) for j in (0, 1)])
    at_edge(lambda: arrivals(0, 0))
    at_middle(lambda: z_arrival(0, nears[2], 0))
    expert_chunk(OWN, nears[0], False)
    shared_chunk(nears[0], False)
    got(kv_rows(XB, 0, rows), kv_r.at[0])
    got(kv_rows(YB, 0, rows), kv_r.at[1])
    remote(kv_rows(XB, 0, half), kv_rows(DB, 0, half), kv_s.at[2], kv_r.at[2], yn)
    remote(kv_rows(YB, half, half), kv_rows(DB, half, half), kv_s.at[3], kv_r.at[3], xn)
    got(shtab.at[XB], sh_r.at[0])
    got(shtab.at[YB], sh_r.at[1])
    remote(shtab.at[XB], shtab.at[DB], sh_s.at[2], sh_r.at[2], yn)
    to_xy(nears[0])
    at_middle(lambda: to_xy(nears[1]))
    at_middle(lambda: z_arrival(0, nears[2], 1))
    at_middle(lambda: to_xy(nears[2]))
    attend_first(0)
    attend_first(1)
    got(halved(XB, z, 1), xy_r.at[0, chips])
    got(halved(YB, z, 0), xy_r.at[1, chips])
    to_pair(piece(XB, z, c), XB, z)
    to_pair(piece(YB, z, c), YB, z)
    at_edge(lambda: arrivals(0, 1))
    at_edge(lambda: to_xy(nears[1]))
    got(halved(DB, z, 0), dr_r.at[0])
    got(halved(DB, z, 1), dr_r.at[1])
    for h in range(2):
        z_forward(halved(DB, z, h), 1, DB, z, h, has_r, has_l)
    to_pair(piece(DB, z, c), DB, z)
    give_down(0)
    attend_first(2)
    attend_first(3)
    expert_chunk(OWN, nears[1], False)
    shared_chunk(nears[1], False)

    def last_own():
        arrivals(0, 2)
        to_xy(nears[2])

    at_edge(last_own)
    give_down(1)
    give_down(2)
    expert_chunk(XB, z, True, 2)
    at_middle(lambda: [z_arrival(1, nears[j], 0) for j in (0, 1)])
    got(kv_rows(DB, 0, half), kv_r.at[2])
    got(kv_rows(DB, half, half), kv_r.at[3])
    finish_head(0)
    finish_head(1)
    mine = ho.at[:, cols(c, vwide)]
    remote(mine, mine, h_s.at[5], h_r.at[5], pt)
    at_middle(lambda: [z_arrival(1, nears[j], 1) for j in (0, 1)])
    expert_chunk(DB, z, True)
    expert_chunk(OWN, nears[2], False)
    activate(OWN, acc.at[pl.ds(OWN * rows, rows), :], hidden, hid.at[OWN], OWN)
    shared_chunk(nears[2], False)
    activate(OWN, sacc, shared, shid, 4)
    at_edge(lambda: arrivals(1, 0))
    side_arrival(nears[0])
    for p in range(chips):
        loads[5 + p].wait()
        got(ow.at[cols(1 - c, vwide), pl.ds(p * part, part)], w_r.at[0, p])
    got(ho.at[:, cols(1 - c, vwide)], h_r.at[5])
    for j in range(chips):
        span = cols(fars[j], part)
        macc[:, span] = mm(ho[...], ow[:, span])

    def z_send(kind, j, p, value_of):
        upstream = ((p > z) & has_l) | ((p < z) & has_r)
        slot = zout.at[kind, j]

        @pl.when(upstream)
        def _():
            got(zin.at[kind, p], z_r.at[kind, p])
            zout[kind, j] = low(value_of() + f32(zin[kind, p]))

        @pl.when(jnp.logical_not(upstream))
        def _():
            zout[kind, j] = low(value_of())

        @pl.when(p > z)
        def _():
            remote(slot, zin.at[kind, p], z_s.at[kind, j], z_r.at[kind, p], zr)

        @pl.when((p < z) & (p != z - 1))
        def _():
            remote(slot, zin.at[kind, p], z_s.at[kind, j], z_r.at[kind, p], zl)

        @pl.when((p < z) & (p == z - 1))
        def _():
            remote(slot, zin.at[kind, chips], z_s.at[kind, j], z_r.at[kind, chips], zl)

    def z_finish(kind, value):
        target = (mix_ref, out_ref)[kind]

        @pl.when(has_l)
        def _():
            got(zin.at[kind, z], z_r.at[kind, z])

        @pl.when(has_r)
        def _():
            got(zin.at[kind, chips], z_r.at[kind, chips])

        @pl.when(has_l & has_r)
        def _():
            target[...] = low(value + f32(zin[kind, z]) + f32(zin[kind, chips]))

        @pl.when(jnp.logical_not(has_l))
        def _():
            target[...] = low(value + f32(zin[kind, chips]))

        @pl.when(jnp.logical_not(has_r))
        def _():
            target[...] = low(value + f32(zin[kind, z]))

    def mixer_send(j):
        p = fars[j]
        z_send(0, j, p, lambda: macc[:, cols(p, part)])

    at_edge(lambda: [mixer_send(j) for j in range(chips - 1)])
    at_middle(lambda: z_arrival(1, nears[2], 0))
    for p in range(chips):
        loads[5 + chips + p].wait()
        loads[5 + 2 * chips + p].wait()
        got(sd.at[cols(1 - c, shared), pl.ds(p * part, part)], w_r.at[1, p])
        got(dw.at[cols(1 - c, hidden), pl.ds(p * part, part)], w_r.at[2, p])
    got(hid.at[OWN, :, cols(1 - c, hidden)], h_r.at[OWN])
    got(shid.at[:, cols(1 - c, shared)], h_r.at[4])
    got(shtab.at[DB], sh_r.at[2])
    for block in range(4):
        line = jnp.sum(jnp.where(expert_id == e, shtab[block], 0.0), axis=0, keepdims=True)
        shcol[block] = jnp.broadcast_to(line, (128, rows)).T

    def own_down(p, carry):
        span = cols(p, part)
        oacc[:, span] = mm(hid[OWN], dw[:, span]) * shcol[OWN, :, 0:1] + mm(shid[...], sd[:, span])
        return carry

    lax.fori_loop(0, chips, own_down, 0)
    at_middle(lambda: z_arrival(1, nears[2], 1))
    at_edge(lambda: arrivals(1, 1))
    side_arrival(nears[1])
    expert_chunk(XB, nears[0], False, 3)
    expert_chunk(XB, nears[1], False, 3)
    at_edge(lambda: arrivals(1, 2))
    side_arrival(nears[2])
    expert_half(DB, nears[2], c)
    expert_half(XB, nears[2], c, 2)
    expert_half(DB, nears[2], 1 - c)
    activate(DB, acc.at[pl.ds(DB * rows, rows), :], hidden, hid.at[DB], DB)
    expert_half(XB, nears[2], 1 - c, 2)

    def down(block, p):
        return mm(hid[block], dw[:, cols(p, part)]) * shcol[block, :, 0:1]

    top, rest = pl.ds(0, half), pl.ds(half, half)
    sides = ((0, XB, 0, 1, xn), (1, YB, 1, 0, yn))

    def far_share(j):
        span = cols(fars[j], part)
        dsend[:, span] = low(down(DB, fars[j]))
        remote(dsend.at[top, span], din.at[0, :, span], d_s.at[0, j], d_r.at[0, j], xn)
        remote(dsend.at[rest, span], din.at[1, :, span], d_s.at[1, j], d_r.at[1, j], yn)

    def early_share(j):
        span = cols(fars[j], part)
        for i, block, now, later, dev in sides:
            value = down(block, fars[j])
            esend[i, :, span] = low(value[now * half : (now + 1) * half])
            late[i, :, span] = value[later * half : (later + 1) * half]
            target = xyin.at[i, pl.ds(now * half, half), span]
            remote(esend.at[i, :, span], target, e_s.at[i, 0, j], e_r.at[i, 0, j], dev)

    def late_share(j):
        span = cols(fars[j], part)
        for i, block, now, later, dev in sides:
            got(din.at[1 - i, :, span], d_r.at[1 - i, j])
            lsend[i, :, span] = low(late[i, :, span] + f32(din[1 - i, :, span]))
            target = xyin.at[i, pl.ds(later * half, half), span]
            remote(lsend.at[i, :, span], target, e_s.at[i, 1, j], e_r.at[i, 1, j], dev)

    def total_share(j):
        span = cols(fars[j], part)
        for i, block, now, later, dev in sides:
            got(xyin.at[i, pl.ds(now * half, half), span], e_r.at[i, 0, j])
            got(xyin.at[i, pl.ds(later * half, half), span], e_r.at[i, 1, j])

        def total():
            return oacc[:, span] + f32(xyin[0, :, span]) + f32(xyin[1, :, span])

        if j < chips - 1:
            z_send(1, j, fars[j], total)
        else:
            z_finish(1, total())

    got(hid.at[DB, :, cols(1 - c, hidden)], h_r.at[DB])
    far_share(0)
    activate(XB, acc.at[pl.ds(XB * rows, rows), :], hidden, hid.at[XB], XB)
    activate(YB, acc.at[pl.ds(YB * rows, rows), :], hidden, hid.at[YB], YB)
    got(hid.at[XB, :, cols(1 - c, hidden)], h_r.at[XB])
    got(hid.at[YB, :, cols(1 - c, hidden)], h_r.at[YB])
    early_share(0)
    far_share(1)
    at_middle(lambda: mixer_send(0))
    late_share(0)
    early_share(1)
    far_share(2)
    at_middle(lambda: mixer_send(1))
    late_share(1)
    early_share(2)
    far_share(3)
    at_middle(lambda: mixer_send(2))
    total_share(0)
    late_share(2)
    early_share(3)
    total_share(1)
    late_share(3)
    z_finish(0, macc[:, cols(z, part)])
    total_share(2)
    total_share(3)

    for kind, block in ((0, OWN), (1, DB)):
        for s in range(chips):

            @pl.when(has_r & (s <= z))
            def _():
                for h in range(2):
                    sent(halved(block, s, h), ag_s.at[kind, 0, s, h])

            @pl.when(has_l & (s >= z))
            def _():
                for h in range(2):
                    sent(halved(block, s, h), ag_s.at[kind, 1, s, h])

    for i in range(2):
        sent(halved(OWN, z, 0), xy_s.at[i, z])
        sent(halved(OWN, z, 0), xy_s.at[i, chips])
        for j in range(chips - 1):
            sent(piece(OWN, nears[j], c), xy_s.at[i, nears[j]])
    for s in range(chips):
        for block in range(4):
            sent(piece(block, s, c), pt_s.at[block, s])
    for i in range(2):
        sent(halved(DB, z, i), dr_s.at[i])
        sent(kv_rows(OWN, 0, rows), kv_s.at[i])
        sent(kv_rows(OWN, 0, half), kv_s.at[2 + i])
    for i in range(3):
        sent(shtab.at[OWN], sh_s.at[i])
        for p in range(chips):
            src, dst, depth = downs[i]
            sent(dst.at[cols(c, depth), pl.ds(p * part, part)], w_s.at[i, p])
    for block in range(4):
        sent(hid.at[block, :, cols(c, hidden)], h_s.at[block])
    sent(shid.at[:, cols(c, shared)], h_s.at[4])
    sent(ho.at[:, cols(c, vwide)], h_s.at[5])
    for i in range(2):
        for j in range(chips):
            sent(dsend.at[top, pl.ds(j * part, part)], d_s.at[i, j])
            sent(esend.at[i, :, pl.ds(j * part, part)], e_s.at[i, 0, j])
            sent(lsend.at[i, :, pl.ds(j * part, part)], e_s.at[i, 1, j])
        for j in range(chips - 1):
            sent(zout.at[i, j], z_s.at[i, j])


def emit_kernel(mixed_ref, routed_ref, mix_hbm, out_hbm, sems):
    first = pltpu.make_async_copy(mixed_ref, mix_hbm, sems.at[0])
    second = pltpu.make_async_copy(routed_ref, out_hbm, sems.at[1])
    first.start()
    second.start()
    first.wait()
    second.wait()


def rotation_table(positions, key_width):
    half_width = key_width // 2
    freq = np.float32(ROPE_BASE) ** (-np.arange(half_width, dtype=np.float32) / np.float32(half_width))
    angles = np.arange(positions, dtype=np.float32)[:, None] * freq.astype(np.float32)[None, :]
    angles = angles.astype(np.float64)
    cosine, sine = np.cos(angles), np.sin(angles)
    copies = 128 // key_width
    cosine = np.tile(np.concatenate([cosine, cosine], axis=1), (1, copies))
    sine = np.tile(np.concatenate([-sine, sine], axis=1), (1, copies))
    return np.concatenate([cosine, sine], axis=1).astype(np.float32)


def kernel_body(
    query_heads,
    key_heads,
    value_heads,
    diff_lambda,
    sub_gain,
    out_weight,
    routed_input,
    routes,
    route_weights,
    expert_gate,
    expert_up,
    expert_down,
    shared_gate,
    shared_up,
    shared_down,
):
    rows, part = routed_input.shape
    chips = lax.axis_size("tp") // 2
    groups = lax.axis_size("ep")
    gate, up, down = expert_gate[0], expert_up[0], expert_down[0]
    width, hidden = gate.shape
    shared = shared_gate.shape[1]
    kwide, vwide = key_heads.shape[1], value_heads.shape[1]
    local_heads = diff_lambda.shape[0]
    half, mine = rows // 2, width // 2
    table = jnp.asarray(rotation_table(groups * rows, kwide // (2 * local_heads)))
    vmem = pl.BlockSpec(memory_space=pltpu.VMEM)
    smem = pl.BlockSpec(memory_space=pltpu.SMEM)
    hbm = pl.BlockSpec(memory_space=pl.ANY)
    dma = pltpu.SemaphoreType.DMA
    out = jax.ShapeDtypeStruct((rows, part), BF16)
    mixed, routed = pl.pallas_call(
        functools.partial(layer_kernel, chips),
        out_shape=(out, out),
        in_specs=[vmem, vmem, vmem, smem, vmem, vmem, vmem, vmem] + [hbm] * 8,
        out_specs=(vmem, vmem),
        scratch_shapes=[
            pltpu.VMEM((groups * rows, width), BF16),
            pltpu.VMEM((width, 2 * hidden), BF16),
            pltpu.VMEM((2 * hidden, mine), BF16),
            pltpu.VMEM((width, 2 * shared), BF16),
            pltpu.VMEM((2 * shared, mine), BF16),
            pltpu.VMEM((2 * vwide, mine), BF16),
            pltpu.VMEM((rows, 256), F32),
            pltpu.VMEM((groups * rows, 2 * hidden), F32),
            pltpu.VMEM((rows, 2 * shared), F32),
            pltpu.VMEM((groups * rows, 128), F32),
            pltpu.VMEM((groups, rows, 2 * hidden), BF16),
            pltpu.VMEM((rows, 2 * shared), BF16),
            pltpu.VMEM((rows, mine), F32),
            pltpu.VMEM((rows, mine), BF16),
            pltpu.VMEM((2, half, mine), BF16),
            pltpu.VMEM((2, half, mine), BF16),
            pltpu.VMEM((2, half, mine), F32),
            pltpu.VMEM((2, half, mine), BF16),
            pltpu.VMEM((2, rows, mine), BF16),
            pltpu.VMEM((2, chips + 1, rows, part), BF16),
            pltpu.VMEM((2, chips - 1, rows, part), BF16),
            pltpu.VMEM((rows, mine), F32),
            pltpu.VMEM((groups * rows, kwide + vwide), BF16),
            pltpu.VMEM((2 * local_heads, rows, 128), BF16),
            pltpu.VMEM((rows, 3 * rows), F32),
            pltpu.VMEM((rows, 3 * rows), BF16),
            pltpu.VMEM((2 * local_heads, rows, 128), F32),
            pltpu.VMEM((2 * local_heads, rows, 128), F32),
            pltpu.VMEM((2 * local_heads, rows, 128), F32),
            pltpu.VMEM((rows, 128), F32),
            pltpu.VMEM((rows, 2 * vwide), BF16),
            pltpu.VMEM((groups, 8, rows), F32),
            pltpu.VMEM((groups, rows, 128), F32),
            dma((5 + 3 * chips,)),
            dma((3, chips)),
            dma((3, chips)),
            dma((2, 2, chips, 2)),
            dma((2, chips, 2)),
            dma((2, chips + 1)),
            dma((2, chips + 1)),
            dma((2,)),
            dma((2,)),
            dma((4, chips)),
            dma((4, chips)),
            dma((4,)),
            dma((4,)),
            dma((3,)),
            dma((3,)),
            dma((6,)),
            dma((6,)),
            dma((2, chips)),
            dma((2, chips)),
            dma((2, 2, chips)),
            dma((2, 2, chips)),
            dma((2, chips - 1)),
            dma((2, chips + 1)),
        ],
        compiler_params=pltpu.CompilerParams(
            collective_id=0, has_side_effects=True, vmem_limit_bytes=67043328
        ),
        name="layer",
    )(
        query_heads,
        key_heads,
        value_heads,
        diff_lambda,
        sub_gain[None, :],
        routed_input,
        routes.T,
        route_weights.T,
        table,
        out_weight,
        gate,
        up,
        down,
        shared_gate,
        shared_up,
        shared_down,
    )
    return pl.pallas_call(
        emit_kernel,
        out_shape=(out, out),
        in_specs=[vmem, vmem],
        out_specs=(hbm, hbm),
        scratch_shapes=[dma((2,))],
        name="emit",
    )(mixed, routed)


def solution(mesh):
    dense = mesh.shape["ep"] == 4 and mesh.shape["tp"] == 8

    def chosen(*arguments):
        fits = dense and arguments[9].shape[0] == 1 and arguments[6].shape[0] % 32 == 0
        return (kernel_body if fits else body)(*arguments)

    placed = (
        P("ep", "tp"),
        P("ep", "tp"),
        P("ep", "tp"),
        P("tp"),
        P(),
        P("tp", None),
        P("ep", "tp"),
        P("ep", None),
        P("ep", None),
        P("ep", None, "tp"),
        P("ep", None, "tp"),
        P("ep", "tp", None),
        P(None, "tp"),
        P(None, "tp"),
        P("tp", None),
    )
    return jax.shard_map(
        chosen, mesh=mesh, in_specs=placed, out_specs=(P("ep", "tp"), P("ep", "tp")), check_vma=False
    )
```

```python
import functools

import jax
import jax.numpy as jnp
import numpy as np
from jax import lax
from jax.experimental import pallas as pl
from jax.experimental.pallas import tpu as pltpu
from jax.sharding import PartitionSpec as P

ROPE_BASE = 10000.0
NORM_EPS = 1e-06
MASKED = -1e30


def rotate(values, positions):
    half_width = values.shape[-1] // 2
    inverse_freq = ROPE_BASE ** (-jnp.arange(half_width, dtype=jnp.float32) / half_width)
    angles = positions.astype(jnp.float32)[:, None] * inverse_freq[None, :]
    angles = angles.reshape((angles.shape[0],) + (1,) * (values.ndim - 2) + (half_width,))
    cosine = jnp.cos(angles)
    sine_part = jnp.sin(angles)
    lower = values[..., :half_width]
    upper = values[..., half_width:]
    return jnp.concatenate(
        [lower * cosine - upper * sine_part, upper * cosine + lower * sine_part], axis=-1
    )


def mixer_terms(query_heads, key_heads, value_heads, diff_lambda, sub_gain, out_weight):
    row_count = query_heads.shape[0]
    local_heads = diff_lambda.shape[0]
    value_width = value_heads.shape[1] // local_heads
    key_width = query_heads.shape[1] // (2 * local_heads)
    score_scale = key_width ** (-0.5)
    offset = lax.axis_index("ep") * row_count
    positions = offset + jnp.arange(row_count, dtype=jnp.int32)
    last_row = offset + row_count - 1
    query_rot = rotate(
        query_heads.astype(jnp.float32).reshape(row_count, local_heads, 2, key_width), positions
    ).astype(jnp.bfloat16)
    queries = jnp.transpose(query_rot, (1, 2, 0, 3))
    key_rot = (
        rotate(
            key_heads.astype(jnp.float32).reshape(row_count, local_heads, 2, key_width), positions
        )
        .astype(jnp.bfloat16)
        .reshape(row_count, local_heads * 2 * key_width)
    )
    start_state = (
        jnp.full((local_heads, 2, row_count), MASKED, jnp.float32),
        jnp.zeros((local_heads, 2, row_count), jnp.float32),
        jnp.zeros((local_heads, 2, row_count, value_width), jnp.float32),
    )
    carried = start_state
    key_piece = lax.all_gather(key_rot, "ep", axis=0, tiled=True)
    value_piece = lax.all_gather(value_heads, "ep", axis=0, tiled=True)
    piece_rows = key_piece.shape[0]
    key_block = 512
    block_count = piece_rows // key_block
    key_blocks = key_piece.reshape(block_count, key_block, local_heads, 2, key_width)
    value_blocks = value_piece.reshape(block_count, key_block, local_heads, value_width)

    def block_step(running, block_item):
        key_rows, value_rows, block_index = block_item
        block_start = block_index * key_block

        def attend_block(partial_state):
            maxima, totals, weighted = partial_state
            key_positions = block_start + jnp.arange(key_block, dtype=jnp.int32)
            visible = key_positions[None, :] <= positions[:, None]
            scores = (
                jnp.einsum("hmqd,khmd->hmqk", queries, key_rows, preferred_element_type=jnp.float32)
                * score_scale
            )
            scores = jnp.where(visible, scores, MASKED)
            new_maxima = jnp.maximum(maxima, jnp.max(scores, axis=3))
            exp_weights = jnp.where(visible, jnp.exp(scores - new_maxima[..., None]), 0.0)
            shrink = jnp.exp(maxima - new_maxima)
            new_totals = totals * shrink + jnp.sum(exp_weights, axis=3)
            update = jnp.einsum(
                "hmqk,khw->hmqw",
                exp_weights.astype(jnp.bfloat16),
                value_rows,
                preferred_element_type=jnp.float32,
            )
            return (new_maxima, new_totals, weighted * shrink[..., None] + update)

        return (
            lax.cond(
                block_start <= last_row, attend_block, lambda partial_state: partial_state, running
            ),
            None,
        )

    carried, _ = lax.scan(
        block_step, carried, (key_blocks, value_blocks, jnp.arange(block_count, dtype=jnp.int32))
    )
    maxima, totals, weighted = carried
    attended = weighted / totals[..., None]
    mixed_heads = attended[:, 0] - diff_lambda[:, None, None] * attended[:, 1]
    normed = (
        mixed_heads
        * lax.rsqrt(jnp.mean(mixed_heads * mixed_heads, axis=2, keepdims=True) + NORM_EPS)
        * sub_gain
    )
    heads_out = jnp.transpose(normed.astype(jnp.bfloat16), (1, 0, 2)).reshape(
        row_count, local_heads * value_width
    )
    return jnp.dot(heads_out, out_weight, preferred_element_type=jnp.float32)


def expert_terms(
    routed_input, routes, expert_gate, expert_up, expert_down, shared_gate, shared_up, shared_down
):
    row_count, part_width = routed_input.shape
    top_count = routes.shape[1]
    local_experts = expert_gate.shape[0]
    groups = lax.axis_size("ep")
    experts = local_experts * groups
    capacity = 2 * row_count * top_count // experts
    copies = row_count * top_count
    flat_routes = routes.reshape(copies)
    onehot = (flat_routes[:, None] == jnp.arange(experts, dtype=jnp.int32)[None, :]).astype(
        jnp.int32
    )
    rank_within = jnp.sum((jnp.cumsum(onehot, axis=0) - onehot) * onehot, axis=1)
    slot_index = flat_routes * capacity + rank_within
    placer = (
        slot_index[:, None] == jnp.arange(experts * capacity, dtype=jnp.int32)[None, :]
    ).astype(jnp.bfloat16)
    token_slots = jnp.sum(placer.reshape(row_count, top_count, experts * capacity), axis=1)
    outgoing = jnp.dot(token_slots.T, routed_input, preferred_element_type=jnp.float32).astype(
        jnp.bfloat16
    )
    arrived = lax.all_to_all(
        outgoing.reshape(groups, local_experts * capacity, part_width),
        "ep",
        split_axis=0,
        concat_axis=0,
        tiled=True,
    )
    slot_count = groups * capacity
    slot_rows = jnp.transpose(
        arrived.reshape(groups, local_experts, capacity, part_width), (1, 0, 2, 3)
    ).reshape(local_experts, slot_count, part_width)
    slot_piece = lax.all_gather(slot_rows, "tp", axis=2, tiled=True)
    own_piece = lax.all_gather(routed_input[None], "tp", axis=2, tiled=True)
    own_rows = own_piece[0]
    gate_sum = jnp.einsum(
        "emc,ecf->emf", slot_piece, expert_gate, preferred_element_type=jnp.float32
    )
    up_sum = jnp.einsum("emc,ecf->emf", slot_piece, expert_up, preferred_element_type=jnp.float32)
    square_sum = jnp.sum(jnp.square(slot_piece.astype(jnp.float32)), axis=2)
    shared_gate_sum = jnp.dot(own_rows, shared_gate, preferred_element_type=jnp.float32)
    shared_up_sum = jnp.dot(own_rows, shared_up, preferred_element_type=jnp.float32)
    shared_square = jnp.sum(jnp.square(own_rows.astype(jnp.float32)), axis=1)
    full_width = expert_gate.shape[1]
    factor = lax.rsqrt(square_sum / full_width + NORM_EPS)[..., None]
    hidden = (jax.nn.silu(gate_sum * factor) * (up_sum * factor)).astype(jnp.bfloat16)
    shared_factor = lax.rsqrt(shared_square / full_width + NORM_EPS)[:, None]
    shared_hidden = (
        jax.nn.silu(shared_gate_sum * shared_factor) * (shared_up_sum * shared_factor)
    ).astype(jnp.bfloat16)
    shared_terms = jnp.dot(shared_hidden, shared_down, preferred_element_type=jnp.float32)
    routed_terms = jnp.einsum(
        "emf,efd->emd", hidden, expert_down, preferred_element_type=jnp.float32
    )
    routed_sum = lax.psum_scatter(
        routed_terms.astype(jnp.bfloat16), "tp", scatter_dimension=2, tiled=True
    ).astype(jnp.float32)
    return (routed_sum, shared_terms, placer)


def expert_finish(routed_sum, shared_sum, placer, route_weights):
    local_experts, slot_count, part_width = routed_sum.shape
    groups = lax.axis_size("ep")
    capacity = slot_count // groups
    leaving = jnp.transpose(
        routed_sum.astype(jnp.bfloat16).reshape(local_experts, groups, capacity, part_width),
        (1, 0, 2, 3),
    ).reshape(groups, local_experts * capacity, part_width)
    returned = lax.all_to_all(leaving, "ep", split_axis=0, concat_axis=0, tiled=True)
    copy_results = jnp.dot(
        placer,
        returned.reshape(groups * local_experts * capacity, part_width),
        preferred_element_type=jnp.float32,
    )
    row_count, top_count = route_weights.shape
    routed = jnp.sum(
        copy_results.reshape(row_count, top_count, part_width) * route_weights[:, :, None], axis=1
    )
    return (routed + shared_sum).astype(jnp.bfloat16)


def body(
    query_heads,
    key_heads,
    value_heads,
    diff_lambda,
    sub_gain,
    out_weight,
    routed_input,
    routes,
    route_weights,
    expert_gate,
    expert_up,
    expert_down,
    shared_gate,
    shared_up,
    shared_down,
):
    mixer_partial = mixer_terms(
        query_heads, key_heads, value_heads, diff_lambda, sub_gain, out_weight
    )
    routed_sum, shared_terms, placer = expert_terms(
        routed_input,
        routes,
        expert_gate,
        expert_up,
        expert_down,
        shared_gate,
        shared_up,
        shared_down,
    )
    mixer_sum, shared_sum = (
        lax.psum_scatter(
            mixer_partial.astype(jnp.bfloat16), "tp", scatter_dimension=1, tiled=True
        ).astype(jnp.float32),
        lax.psum_scatter(
            shared_terms.astype(jnp.bfloat16), "tp", scatter_dimension=1, tiled=True
        ).astype(jnp.float32),
    )
    return (
        mixer_sum.astype(jnp.bfloat16),
        expert_finish(routed_sum, shared_sum, placer, route_weights),
    )


MESH = pl.DeviceIdType.MESH
F32 = jnp.float32
BF16 = jnp.bfloat16
OWN, XB, YB, DB = 0, 1, 2, 3


def low(value):
    return value.astype(BF16)


def f32(value):
    return value.astype(F32)


def mm(left, right):
    return jnp.dot(left, right, preferred_element_type=F32)


def near_first(chips):
    rows = [sorted((s for s in range(chips) if s != z), key=lambda s: (abs(s - z), s if z < chips // 2 else -s)) for z in range(chips)]
    return [[row[j] for row in rows] for j in range(chips - 1)]


def far_first(chips):
    rows = []
    for z in range(chips):
        right = list(range(chips - 1, z, -1))
        left = list(range(0, z))
        first, second = (right, left) if z < chips // 2 else (left, right)
        row = []
        while first or second:
            if first:
                row.append(first.pop(0))
            if second:
                row.append(second.pop(0))
        rows.append(row)
    return [[row[j] for row in rows] for j in range(chips - 1)]


def layer_kernel(
    chips,
    lam_ref,
    q_hbm,
    k_hbm,
    v_hbm,
    gain_hbm,
    x_hbm,
    routes_hbm,
    rw_hbm,
    tab_hbm,
    ow_hbm,
    gw_hbm,
    uw_hbm,
    dw_hbm,
    sg_hbm,
    su_hbm,
    sd_hbm,
    mix_hbm,
    out_hbm,
    mix_ref,
    out_ref,
    xall,
    guw,
    dw,
    sgu,
    sd,
    ow,
    tab,
    q_ref,
    k_ref,
    gain_ref,
    routes_ref,
    rw_ref,
    acc,
    sacc,
    ssq,
    hid,
    shid,
    oacc,
    dsend,
    esend,
    lsend,
    late,
    din,
    xyin,
    zin,
    zout,
    macc,
    kv,
    qrot,
    sc_s,
    sc_p,
    sc_m,
    sc_t,
    sc_o,
    sc_a,
    ho,
    shtab,
    shcol,
    w_l,
    w_s,
    w_r,
    ag_s,
    ag_r,
    xy_s,
    xy_r,
    dr_s,
    dr_r,
    pt_s,
    pt_r,
    kv_s,
    kv_r,
    sh_s,
    sh_r,
    h_s,
    h_r,
    d_s,
    d_r,
    e_s,
    e_r,
    z_s,
    z_r,
    in_l,
):
    rows, part = x_hbm.shape
    half = rows // 2
    wide = 2 * part
    hidden = gw_hbm.shape[1]
    shared = sg_hbm.shape[1]
    vwide = v_hbm.shape[1]
    kwide = k_hbm.shape[1]
    local_heads = lam_ref.shape[0]
    vd = vwide // local_heads
    qk = kwide // (2 * local_heads)
    e = lax.axis_index("ep")
    t = lax.axis_index("tp")
    z, c = t // 2, t % 2
    x, y = e % 2, e // 2
    pt = (e, t + 1 - 2 * c)
    xn = (e + 1 - 2 * x, t)
    yn = (e + 2 - 4 * y, t)
    zr = (e, t + 2)
    zl = (e, t - 2)
    has_r = z < chips - 1
    has_l = z > 0

    def chosen_by_z(column):
        return sum(order * (z == at).astype(jnp.int32) for at, order in enumerate(column))

    nears = [chosen_by_z(column) for column in near_first(chips)]
    fars = [chosen_by_z(column) for column in far_first(chips)] + [z]

    def remote(src, dst, send, recv, dev):
        pltpu.make_async_remote_copy(src, dst, send, recv, device_id=dev, device_id_type=MESH).start()

    def got(dst, recv):
        pltpu.make_async_remote_copy(dst, dst, recv, recv, device_id=pt, device_id_type=MESH).wait_recv()

    def sent(src, send):
        pltpu.make_async_remote_copy(src, src, send, send, device_id=pt, device_id_type=MESH).wait_send()

    def cols(index, width):
        return pl.ds(pl.multiple_of(index * width, width), width)

    barrier = pltpu.get_barrier_semaphore()
    for dev in (pt, xn, yn):
        pl.semaphore_signal(barrier, inc=1, device_id=dev, device_id_type=MESH)

    @pl.when(has_r)
    def _():
        pl.semaphore_signal(barrier, inc=1, device_id=zr, device_id_type=MESH)

    @pl.when(has_l)
    def _():
        pl.semaphore_signal(barrier, inc=1, device_id=zl, device_id_type=MESH)

    loads = [
        pltpu.make_async_copy(gw_hbm, guw.at[:, pl.ds(0, hidden)], w_l.at[0]),
        pltpu.make_async_copy(uw_hbm, guw.at[:, pl.ds(hidden, hidden)], w_l.at[1]),
        pltpu.make_async_copy(sg_hbm, sgu.at[:, pl.ds(0, shared)], w_l.at[2]),
        pltpu.make_async_copy(su_hbm, sgu.at[:, pl.ds(shared, shared)], w_l.at[3]),
        pltpu.make_async_copy(tab_hbm.at[pl.ds(pl.multiple_of(e * rows, rows), rows), :], tab, w_l.at[4]),
    ]
    downs = [(ow_hbm, ow, vwide), (sd_hbm, sd, shared), (dw_hbm, dw, hidden)]
    for i, (src, dst, depth) in enumerate(downs):
        for p in range(chips):
            loads.append(
                pltpu.make_async_copy(
                    src.at[:, cols(2 * p + c, part)],
                    dst.at[cols(c, depth), pl.ds(p * part, part)],
                    w_l.at[5 + i * chips + p],
                )
            )
    own_rows = pl.ds(0, rows)
    inputs = [
        pltpu.make_async_copy(x_hbm, xall.at[own_rows, cols(t, part)], in_l.at[0]),
        pltpu.make_async_copy(q_hbm, q_ref, in_l.at[1]),
        pltpu.make_async_copy(k_hbm, k_ref, in_l.at[2]),
        pltpu.make_async_copy(v_hbm, kv.at[own_rows, pl.ds(kwide, vwide)], in_l.at[3]),
        pltpu.make_async_copy(routes_hbm, routes_ref, in_l.at[4]),
        pltpu.make_async_copy(rw_hbm, rw_ref, in_l.at[5]),
        pltpu.make_async_copy(gain_hbm, gain_ref, in_l.at[6]),
    ]
    inputs[0].start()
    inputs[1].start()
    inputs[2].start()
    loads[4].start()
    for copy in inputs[3:]:
        copy.start()


    def piece(block, s, core):
        return xall.at[pl.ds(block * rows, rows), cols(2 * s + core, part)]

    def base(block, h):
        return block * rows + (h if block in (OWN, DB) else 1 - h) * half

    def halved(block, s, h, core=None):
        return xall.at[pl.ds(base(block, h), half), cols(2 * s + (c if core is None else core), part)]

    def z_forward(src, kind, block, s, h, right, left):
        @pl.when(right)
        def _():
            remote(src, halved(block, s, h), ag_s.at[kind, 0, s, h], ag_r.at[kind, s, h], zr)

        @pl.when(left)
        def _():
            remote(src, halved(block, s, h), ag_s.at[kind, 1, s, h], ag_r.at[kind, s, h], zl)

    def to_pair(src, block, s):
        remote(src, piece(block, s, c), pt_s.at[block, s, 0], pt_r.at[block, s, 0], pt)

    def half_of(i, order):
        return order if i == 0 else 1 - order

    def to_side(i, order, s, src):
        block, dev = ((XB, xn), (YB, yn))[i]
        target = halved(block, s, half_of(i, order))
        remote(src, target, xy_s.at[i, s, order], xy_r.at[i, s, order], dev)

    def own_half(i, order):
        to_side(i, order, z, halved(OWN, z, half_of(i, order)))

    def to_xy(s):
        for order in range(2):
            for i in range(2):
                to_side(i, order, s, halved(OWN, s, half_of(i, order)))

    def side_half(i, order, s, core=None):
        return halved((XB, YB)[i], s, half_of(i, order), core)

    def side_arrival(s, order):
        for i, block in ((0, XB), (1, YB)):
            mine = side_half(i, order, s)
            got(mine, xy_r.at[i, s, order])
            remote(mine, mine, pt_s.at[block, s, order], pt_r.at[block, s, order], pt)

    def paired(block, s):
        got(piece(block, s, 1 - c), pt_r.at[block, s, 0])

    def paired_half(i, order, s):
        got(side_half(i, order, s, 1 - c), pt_r.at[(XB, YB)[i], s, order])

    inputs[0].wait()
    loads[0].start()
    loads[1].start()
    pl.semaphore_wait(barrier, 3 + has_r.astype(jnp.int32) + has_l.astype(jnp.int32))

    for h in range(2):
        z_forward(halved(OWN, z, h), 0, OWN, z, h, has_r, has_l)
    own_half(0, 0)
    own_half(1, 0)
    to_pair(piece(OWN, z, c), OWN, z)

    expert_id = lax.broadcasted_iota(jnp.int32, (8, rows), 0)
    inputs[4].wait()
    inputs[5].wait()
    routes = routes_ref[...]
    weights = rw_ref[...]
    table = jnp.zeros((8, rows), F32)
    for k in range(routes.shape[0]):
        table = table + jnp.where(routes[k : k + 1, :] == expert_id, weights[k : k + 1, :], 0.0)
    shtab[OWN] = table
    remote(shtab.at[OWN], shtab.at[XB], sh_s.at[0], sh_r.at[0], xn)
    remote(shtab.at[OWN], shtab.at[YB], sh_s.at[1], sh_r.at[1], yn)

    for copy in inputs[1:4]:
        copy.wait()
    loads[4].wait()
    cosine, sine = tab[:, :128], tab[:, 128:]
    at_row = lax.broadcasted_iota(jnp.int32, (128, 128), 0)
    at_col = lax.broadcasted_iota(jnp.int32, (128, 128), 1)
    swapped = at_col + qk // 2 - qk * ((at_col // (qk // 2)) % 2)
    swap = jnp.where(at_row == swapped, 1.0, 0.0).astype(BF16)
    for i in range(kwide // 128):
        span = slice(i * 128, (i + 1) * 128)
        for src, dst in ((q_ref, qrot), (k_ref, None)):
            value = src[:, span]
            turned = low(f32(value) * cosine + mm(value, swap) * sine)
            if dst is None:
                kv[0:rows, span] = turned
            else:
                turned = turned * jnp.asarray(qk ** (-0.5), BF16)
                for m in range(2):
                    in_map = (lax.broadcasted_iota(jnp.int32, (rows, 128), 1) // qk) == m
                    dst[2 * i + m] = jnp.where(in_map, turned, jnp.zeros((rows, 128), BF16))

    def kv_rows(block, start, count):
        return kv.at[pl.ds(block * rows + start, count), :]

    remote(kv_rows(OWN, 0, rows), kv_rows(XB, 0, rows), kv_s.at[0], kv_r.at[0], xn)
    remote(kv_rows(OWN, 0, rows), kv_rows(YB, 0, rows), kv_s.at[1], kv_r.at[1], yn)

    own_half(0, 1)
    own_half(1, 1)
    for i in list(range(2, 4)) + list(range(5, len(loads))):
        loads[i].start()

    def give_down(i):
        src, dst, depth = downs[i]
        for p in range(chips):
            remote(
                src.at[:, cols(2 * p + 1 - c, part)],
                dst.at[cols(c, depth), pl.ds(p * part, part)],
                w_s.at[i, p],
                w_r.at[i, p],
                pt,
            )

    def chunk(start, count, at, depth, first, weight, target, width):
        tiles = target.shape[-1] // width
        span_rows = pl.ds(start, count)

        def tile(n, carry):
            span = cols(n, width)
            value = mm(xall[span_rows, cols(at, depth)], weight[cols(at, depth), span])
            if not first:
                value = value + target[span_rows, span]
            target[span_rows, span] = value
            return carry

        lax.fori_loop(0, tiles, tile, 0)

    def squares(start, count, at, depth, first):
        span = pl.ds(start, count)
        total = jnp.zeros((count, 128), F32) if first else ssq[span, :]
        for i in range(depth // 128):
            value = f32(xall[span, pl.ds(pl.multiple_of(at * depth + i * 128, 128), 128)])
            total = total + value * value
        ssq[span, :] = total

    def expert_rows(start, count, at, depth, first=False):
        chunk(start, count, at, depth, first, guw, acc, hidden)
        squares(start, count, at, depth, first)

    def expert_chunk(block, s, first, count=1):
        for b in range(block, block + count):
            if b in (OWN, DB):
                paired(b, s)
            else:
                for order in range(2):
                    paired_half(b - XB, order, s)
        expert_rows(block * rows, count * rows, s, wide, first)

    def shared_chunk(s, first):
        chunk(0, rows, s, wide, first, sgu, sacc, 2 * shared)

    def activate(start, count, source, width, target, target_start, index):
        full = jnp.sum(ssq[pl.ds(start, count), :], axis=1, keepdims=True) / (chips * wide)
        factor = lax.rsqrt(full + NORM_EPS)
        span = pl.ds(target_start, count)
        gate = source[span, :width] * factor
        up = source[span, width:] * factor
        target[span, cols(c, width)] = low(gate / (1.0 + jnp.exp(-gate)) * up)
        mine = target.at[span, cols(c, width)]
        remote(mine, mine, h_s.at[index], h_r.at[index], pt)

    def expert_activate(start, count, index):
        activate(start, count, acc, hidden, hid, start, index)

    def expert_hidden(start, count, index):
        got(hid.at[pl.ds(start, count), cols(1 - c, hidden)], h_r.at[index])

    def z_arrival(kind, s, h):
        block = (OWN, DB)[kind]
        got(halved(block, s, h), ag_r.at[kind, s, h])
        z_forward(halved(block, s, h), kind, block, s, h, (s < z) & has_r, (s > z) & has_l)
        if h == 1:
            to_pair(piece(block, s, c), block, s)

    middle = has_l & has_r

    def at_middle(work):
        @pl.when(middle)
        def _():
            work()

    def at_edge(work):
        @pl.when(jnp.logical_not(middle))
        def _():
            work()

    def arrivals(kind, *orders):
        for h in range(2):
            for j in orders:
                z_arrival(kind, nears[j], h)

    def value_cols(h):
        return pl.ds(kwide + h * vd, vd)

    step_rows = 64
    ids = (e, xn[0], yn[0], xn[0] + yn[0] - e)
    bias = [jnp.where(ids[b] < e, 0.0, MASKED) for b in range(4)]

    inputs[6].wait()

    def attend_first(i):
        count = 3 * rows
        sc_s[...] = lax.dot_general(
            qrot[i], kv[0:count, cols(i // 2, 128)], (((1,), (1,)), ((), ())), preferred_element_type=F32
        )

        for r in range(0, rows, step_rows):
            at = slice(r, r + step_rows)
            key = lax.broadcasted_iota(jnp.int32, (step_rows, rows), 1)
            row = r + lax.broadcasted_iota(jnp.int32, (step_rows, rows), 0)
            scores = [
                jnp.where(key <= row, sc_s[at, 0:rows], MASKED),
                sc_s[at, rows : 2 * rows] + bias[XB],
                sc_s[at, 2 * rows :] + bias[YB],
            ]
            most = jnp.maximum(jnp.maximum(scores[0], scores[1]), scores[2])
            most = jnp.max(most, axis=1, keepdims=True)
            weight = [jnp.exp(score - most) for score in scores]
            total = jnp.sum(weight[0] + weight[1] + weight[2], axis=1, keepdims=True)
            for b in range(3):
                sc_p[at, b * rows : (b + 1) * rows] = low(weight[b])
            sc_m[i, at, :] = jnp.broadcast_to(most, (step_rows, 128))
            sc_t[i, at, :] = jnp.broadcast_to(total, (step_rows, 128))

        sc_o[i] = mm(sc_p[...], kv[0:count, value_cols(i // 2)])

    def attend_last(i):
        count = 3 * rows
        sc_s[:, 0:rows] = lax.dot_general(
            qrot[i], kv[count:, cols(i // 2, 128)], (((1,), (1,)), ((), ())), preferred_element_type=F32
        )

        for r in range(0, rows, step_rows):
            at = slice(r, r + step_rows)
            scores = sc_s[at, 0:rows] + bias[DB]
            before = sc_m[i, at, :]
            most = jnp.maximum(before, jnp.max(scores, axis=1, keepdims=True))
            weight = jnp.exp(scores - most[:, 0:1])
            shrink = jnp.exp(before - most)
            sc_p[at, 0:rows] = low(weight)
            sc_a[at, :] = shrink
            sc_t[i, at, :] = sc_t[i, at, :] * shrink + jnp.sum(weight, axis=1, keepdims=True)

        return (sc_o[i] * sc_a[...] + mm(sc_p[:, 0:rows], kv[count:, value_cols(i // 2)])) / sc_t[i]

    def finish_head(h):
        sc_o[2 * h] = attend_last(2 * h)
        mixed = sc_o[2 * h] - lam_ref[h] * attend_last(2 * h + 1)
        scale = lax.rsqrt(jnp.mean(mixed * mixed, axis=1, keepdims=True) + NORM_EPS)
        ho[:, pl.ds(pl.multiple_of(c * vwide + h * vd, 128), vd)] = low(mixed * scale * gain_ref[...])

    loads[0].wait()
    loads[1].wait()
    expert_chunk(OWN, z, True)
    at_middle(lambda: [z_arrival(0, nears[j], 0) for j in (0, 1)])
    loads[2].wait()
    loads[3].wait()
    shared_chunk(z, True)
    side_arrival(z, 0)
    remote(halved(XB, z, 0), halved(DB, z, 0), dr_s.at[0], dr_r.at[0], yn)
    remote(halved(YB, z, 1), halved(DB, z, 1), dr_s.at[1], dr_r.at[1], xn)
    at_middle(lambda: [z_arrival(0, nears[j], 1) for j in (0, 1)])
    at_edge(lambda: arrivals(0, 0))
    at_middle(lambda: z_arrival(0, nears[2], 0))
    expert_chunk(OWN, nears[0], False)
    shared_chunk(nears[0], False)
    got(kv_rows(XB, 0, rows), kv_r.at[0])
    got(kv_rows(YB, 0, rows), kv_r.at[1])
    remote(kv_rows(XB, 0, half), kv_rows(DB, 0, half), kv_s.at[2], kv_r.at[2], yn)
    remote(kv_rows(YB, half, half), kv_rows(DB, half, half), kv_s.at[3], kv_r.at[3], xn)
    got(shtab.at[XB], sh_r.at[0])
    got(shtab.at[YB], sh_r.at[1])
    remote(shtab.at[XB], shtab.at[DB], sh_s.at[2], sh_r.at[2], yn)
    to_xy(nears[0])
    at_middle(lambda: to_xy(nears[1]))
    at_middle(lambda: z_arrival(0, nears[2], 1))
    at_middle(lambda: to_xy(nears[2]))
    attend_first(0)
    attend_first(1)
    side_arrival(z, 1)
    at_edge(lambda: arrivals(0, 1))
    at_edge(lambda: to_xy(nears[1]))
    got(halved(DB, z, 0), dr_r.at[0])
    got(halved(DB, z, 1), dr_r.at[1])
    for h in range(2):
        z_forward(halved(DB, z, h), 1, DB, z, h, has_r, has_l)
    to_pair(piece(DB, z, c), DB, z)
    give_down(0)
    attend_first(2)
    attend_first(3)
    expert_chunk(OWN, nears[1], False)
    shared_chunk(nears[1], False)

    def last_own():
        arrivals(0, 2)
        to_xy(nears[2])

    at_edge(last_own)
    give_down(1)
    give_down(2)
    expert_chunk(XB, z, True, 2)
    at_middle(lambda: [z_arrival(1, nears[j], 0) for j in (0, 1)])
    got(kv_rows(DB, 0, half), kv_r.at[2])
    got(kv_rows(DB, half, half), kv_r.at[3])
    finish_head(0)
    finish_head(1)
    mine = ho.at[:, cols(c, vwide)]
    remote(mine, mine, h_s.at[6], h_r.at[6], pt)
    at_middle(lambda: [z_arrival(1, nears[j], 1) for j in (0, 1)])
    expert_chunk(DB, z, True)
    expert_chunk(OWN, nears[2], False)
    expert_activate(0, rows, 0)
    shared_chunk(nears[2], False)
    activate(0, rows, sacc, shared, shid, 0, 5)
    at_edge(lambda: arrivals(1, 0))
    side_arrival(nears[0], 0)
    side_arrival(nears[0], 1)
    for p in range(chips):
        loads[5 + p].wait()
        got(ow.at[cols(1 - c, vwide), pl.ds(p * part, part)], w_r.at[0, p])
    got(ho.at[:, cols(1 - c, vwide)], h_r.at[6])
    for j in range(chips):
        span = cols(fars[j], part)
        macc[:, span] = mm(ho[...], ow[:, span])

    def z_send(kind, j, p, h, value_of):
        upstream = ((p > z) & has_l) | ((p < z) & has_r)
        at = pl.ds(h * half, half)
        slot = zout.at[kind, j, at]

        @pl.when(upstream)
        def _():
            got(zin.at[kind, p, at], z_r.at[kind, p, h])
            zout[kind, j, at] = low(value_of(at) + f32(zin[kind, p, at]))

        @pl.when(jnp.logical_not(upstream))
        def _():
            zout[kind, j, at] = low(value_of(at))

        @pl.when(p > z)
        def _():
            remote(slot, zin.at[kind, p, at], z_s.at[kind, j, h], z_r.at[kind, p, h], zr)

        @pl.when((p < z) & (p != z - 1))
        def _():
            remote(slot, zin.at[kind, p, at], z_s.at[kind, j, h], z_r.at[kind, p, h], zl)

        @pl.when((p < z) & (p == z - 1))
        def _():
            remote(slot, zin.at[kind, chips, at], z_s.at[kind, j, h], z_r.at[kind, chips, h], zl)

    def z_finish(kind, value_of):
        target = (mix_ref, out_ref)[kind]
        for h in range(2):
            at = pl.ds(h * half, half)

            @pl.when(has_l)
            def _():
                got(zin.at[kind, z, at], z_r.at[kind, z, h])

            @pl.when(has_r)
            def _():
                got(zin.at[kind, chips, at], z_r.at[kind, chips, h])

            @pl.when(has_l & has_r)
            def _():
                target[at] = low(value_of(at) + f32(zin[kind, z, at]) + f32(zin[kind, chips, at]))

            @pl.when(jnp.logical_not(has_l))
            def _():
                target[at] = low(value_of(at) + f32(zin[kind, chips, at]))

            @pl.when(jnp.logical_not(has_r))
            def _():
                target[at] = low(value_of(at) + f32(zin[kind, z, at]))

    def mixer_send(j):
        p = fars[j]
        for h in range(2):
            z_send(0, j, p, h, lambda at: macc[at, cols(p, part)])

    at_edge(lambda: [mixer_send(j) for j in range(chips - 1)])
    at_middle(lambda: z_arrival(1, nears[2], 0))
    for p in range(chips):
        loads[5 + chips + p].wait()
        loads[5 + 2 * chips + p].wait()
        got(sd.at[cols(1 - c, shared), pl.ds(p * part, part)], w_r.at[1, p])
        got(dw.at[cols(1 - c, hidden), pl.ds(p * part, part)], w_r.at[2, p])
    got(shtab.at[DB], sh_r.at[2])
    for block in range(4):
        line = jnp.sum(jnp.where(expert_id == e, shtab[block], 0.0), axis=0, keepdims=True)
        column = jnp.broadcast_to(line, (128, rows)).T
        for h in range(2):
            shcol[pl.ds(base(block, h), half), :] = column[h * half : (h + 1) * half]
    expert_chunk(XB, nears[0], False, 3)
    at_middle(lambda: z_arrival(1, nears[2], 1))
    at_edge(lambda: arrivals(1, 1))
    side_arrival(nears[1], 0)
    side_arrival(nears[1], 1)
    EARLY, X_LATE, Y_LATE, FAR = rows + half, rows, 2 * rows + half, 3 * rows
    expert_rows(XB * rows, 3 * rows, 2 * nears[1] + c, part)
    paired(DB, nears[1])
    for i in range(2):
        for order in range(2):
            paired_half(i, order, nears[1])
    expert_rows(XB * rows, 3 * rows, 2 * nears[1] + 1 - c, part)
    side_arrival(nears[2], 0)
    expert_rows(EARLY, rows, 2 * nears[2] + c, part)
    paired_half(0, 0, nears[2])
    paired_half(1, 0, nears[2])
    expert_rows(EARLY, rows, 2 * nears[2] + 1 - c, part)
    expert_activate(EARLY, rows, 1)
    at_edge(lambda: arrivals(1, 2))
    side_arrival(nears[2], 1)

    def down(start, count, p):
        span = pl.ds(start, count)
        return mm(hid[span, :], dw[:, cols(p, part)]) * shcol[span, 0:1]

    def own_down(p, carry):
        span = cols(p, part)
        oacc[:, span] = down(0, rows, p) + mm(shid[...], sd[:, span])
        return carry

    top, rest = pl.ds(0, half), pl.ds(half, half)
    sides = ((0, X_LATE, 0, 1, xn), (1, Y_LATE, 1, 0, yn))

    def far_share(j):
        span = cols(fars[j], part)
        dsend[:, span] = low(down(FAR, rows, fars[j]))
        remote(dsend.at[top, span], din.at[0, :, span], d_s.at[0, j], d_r.at[0, j], xn)
        remote(dsend.at[rest, span], din.at[1, :, span], d_s.at[1, j], d_r.at[1, j], yn)

    def early_share(j):
        span = cols(fars[j], part)
        value = low(down(EARLY, rows, fars[j]))
        for i, start, now, later, dev in sides:
            esend[i, :, span] = value[i * half : (i + 1) * half]
            target = xyin.at[i, pl.ds(now * half, half), span]
            remote(esend.at[i, :, span], target, e_s.at[i, 0, j], e_r.at[i, 0, j], dev)

    def late_share(j):
        span = cols(fars[j], part)
        for i, start, now, later, dev in sides:
            late[i] = down(start, half, fars[j])
        for i, start, now, later, dev in sides:
            got(din.at[1 - i, :, span], d_r.at[1 - i, j])
            lsend[i, :, span] = low(late[i] + f32(din[1 - i, :, span]))
            target = xyin.at[i, pl.ds(later * half, half), span]
            remote(lsend.at[i, :, span], target, e_s.at[i, 1, j], e_r.at[i, 1, j], dev)

    def total(j):
        span = cols(fars[j], part)
        return lambda at: oacc[at, span] + f32(xyin[0, at, span]) + f32(xyin[1, at, span])

    def total_ready(j):
        span = cols(fars[j], part)
        for i, start, now, later, dev in sides:
            got(xyin.at[i, pl.ds(now * half, half), span], e_r.at[i, 0, j])
            got(xyin.at[i, pl.ds(later * half, half), span], e_r.at[i, 1, j])

    def total_half(j, h):
        z_send(1, j, fars[j], h, total(j))

    def total_share(j):
        total_ready(j)
        total_half(j, 0)
        total_half(j, 1)

    expert_rows(Y_LATE, half + rows, 2 * nears[2] + c, part)
    expert_hidden(EARLY, rows, 1)
    early_share(0)
    early_share(1)
    paired(DB, nears[2])
    paired_half(1, 1, nears[2])
    expert_rows(Y_LATE, half + rows, 2 * nears[2] + 1 - c, part)
    expert_activate(FAR, rows, 2)
    expert_activate(Y_LATE, half, 4)
    expert_rows(X_LATE, half, 2 * nears[2] + c, part)
    paired_half(0, 1, nears[2])
    expert_rows(X_LATE, half, 2 * nears[2] + 1 - c, part)
    expert_activate(X_LATE, half, 3)
    expert_hidden(FAR, rows, 2)
    far_share(0)
    far_share(1)
    at_middle(lambda: mixer_send(0))
    expert_hidden(0, rows, 0)
    got(shid.at[:, cols(1 - c, shared)], h_r.at[5])
    lax.fori_loop(0, chips, own_down, 0)
    expert_hidden(X_LATE, half, 3)
    expert_hidden(Y_LATE, half, 4)
    late_share(0)
    at_middle(lambda: mixer_send(1))
    far_share(2)
    late_share(1)
    early_share(2)
    at_middle(lambda: mixer_send(2))
    at_edge(lambda: total_share(0))
    late_share(2)
    far_share(3)
    at_middle(lambda: total_share(0))
    at_edge(lambda: total_share(1))
    early_share(3)
    at_edge(lambda: total_share(2))

    def middle_first():
        total_ready(1)
        total_half(1, 0)
        total_ready(2)
        total_half(2, 0)

    def middle_second():
        total_half(1, 1)
        total_half(2, 1)

    at_middle(middle_first)
    late_share(3)
    at_middle(middle_second)
    z_finish(0, lambda at: macc[at, cols(z, part)])
    mix_out = pltpu.make_async_copy(mix_ref, mix_hbm, in_l.at[7])
    mix_out.start()
    total_ready(3)
    z_finish(1, total(3))
    routed_out = pltpu.make_async_copy(out_ref, out_hbm, in_l.at[8])
    routed_out.start()

    for kind, block in ((0, OWN), (1, DB)):
        for s in range(chips):

            @pl.when(has_r & (s <= z))
            def _():
                for h in range(2):
                    sent(halved(block, s, h), ag_s.at[kind, 0, s, h])

            @pl.when(has_l & (s >= z))
            def _():
                for h in range(2):
                    sent(halved(block, s, h), ag_s.at[kind, 1, s, h])

    for s in range(chips):
        for i in range(2):
            for order in range(2):
                sent(halved(OWN, s, 0), xy_s.at[i, s, order])
                sent(halved(OWN, s, 0), pt_s.at[(XB, YB)[i], s, order])
        for block in (OWN, DB):
            sent(piece(block, s, c), pt_s.at[block, s, 0])
    for i in range(2):
        sent(halved(DB, z, i), dr_s.at[i])
        sent(kv_rows(OWN, 0, rows), kv_s.at[i])
        sent(kv_rows(OWN, 0, half), kv_s.at[2 + i])
    for i in range(3):
        sent(shtab.at[OWN], sh_s.at[i])
        for p in range(chips):
            src, dst, depth = downs[i]
            sent(dst.at[cols(c, depth), pl.ds(p * part, part)], w_s.at[i, p])
    for count, index in ((rows, 0), (rows, 1), (rows, 2), (half, 3), (half, 4)):
        sent(hid.at[pl.ds(0, count), cols(c, hidden)], h_s.at[index])
    sent(shid.at[:, cols(c, shared)], h_s.at[5])
    sent(ho.at[:, cols(c, vwide)], h_s.at[6])
    for i in range(2):
        for j in range(chips):
            sent(dsend.at[top, pl.ds(j * part, part)], d_s.at[i, j])
            sent(esend.at[i, :, pl.ds(j * part, part)], e_s.at[i, 0, j])
            sent(lsend.at[i, :, pl.ds(j * part, part)], e_s.at[i, 1, j])
        for j in range(chips - 1):
            for h in range(2):
                sent(zout.at[i, j, pl.ds(0, half)], z_s.at[i, j, h])
    mix_out.wait()
    routed_out.wait()


def emit_kernel(mixed_hbm, routed_hbm, mix_hbm, out_hbm, mixed, routed, sems):
    pairs = ((mixed_hbm, mixed, mix_hbm), (routed_hbm, routed, out_hbm))
    loads = [pltpu.make_async_copy(src, held, sems.at[i]) for i, (src, held, _) in enumerate(pairs)]
    stores = [pltpu.make_async_copy(held, dst, sems.at[2 + i]) for i, (_, held, dst) in enumerate(pairs)]
    for load in loads:
        load.start()
    for load, store in zip(loads, stores):
        load.wait()
        store.start()
    for store in stores:
        store.wait()


def rotation_table(positions, key_width):
    half_width = key_width // 2
    freq = np.float32(ROPE_BASE) ** (-np.arange(half_width, dtype=np.float32) / np.float32(half_width))
    angles = np.arange(positions, dtype=np.float32)[:, None] * freq.astype(np.float32)[None, :]
    angles = angles.astype(np.float64)
    cosine, sine = np.cos(angles), np.sin(angles)
    copies = 128 // key_width
    cosine = np.tile(np.concatenate([cosine, cosine], axis=1), (1, copies))
    sine = np.tile(np.concatenate([-sine, sine], axis=1), (1, copies))
    return np.concatenate([cosine, sine], axis=1).astype(np.float32)


def kernel_body(
    query_heads,
    key_heads,
    value_heads,
    diff_lambda,
    sub_gain,
    out_weight,
    routed_input,
    routes,
    route_weights,
    expert_gate,
    expert_up,
    expert_down,
    shared_gate,
    shared_up,
    shared_down,
):
    rows, part = routed_input.shape
    chips = lax.axis_size("tp") // 2
    groups = lax.axis_size("ep")
    gate, up, down = expert_gate[0], expert_up[0], expert_down[0]
    width, hidden = gate.shape
    shared = shared_gate.shape[1]
    kwide, vwide = key_heads.shape[1], value_heads.shape[1]
    local_heads = diff_lambda.shape[0]
    half, mine = rows // 2, width // 2
    table = jnp.asarray(rotation_table(groups * rows, kwide // (2 * local_heads)))
    smem = pl.BlockSpec(memory_space=pltpu.SMEM)
    hbm = pl.BlockSpec(memory_space=pl.ANY)
    dma = pltpu.SemaphoreType.DMA
    out = jax.ShapeDtypeStruct((rows, part), BF16)
    mixed, routed = pl.pallas_call(
        functools.partial(layer_kernel, chips),
        out_shape=(out, out),
        in_specs=[smem] + [hbm] * 15,
        out_specs=(hbm, hbm),
        scratch_shapes=[
            pltpu.VMEM((rows, part), BF16),
            pltpu.VMEM((rows, part), BF16),
            pltpu.VMEM((groups * rows, width), BF16),
            pltpu.VMEM((width, 2 * hidden), BF16),
            pltpu.VMEM((2 * hidden, mine), BF16),
            pltpu.VMEM((width, 2 * shared), BF16),
            pltpu.VMEM((2 * shared, mine), BF16),
            pltpu.VMEM((2 * vwide, mine), BF16),
            pltpu.VMEM((rows, 256), F32),
            pltpu.VMEM(query_heads.shape, BF16),
            pltpu.VMEM(key_heads.shape, BF16),
            pltpu.VMEM((1, sub_gain.shape[0]), F32),
            pltpu.VMEM(routes.shape[::-1], routes.dtype),
            pltpu.VMEM(routes.shape[::-1], F32),
            pltpu.VMEM((groups * rows, 2 * hidden), F32),
            pltpu.VMEM((rows, 2 * shared), F32),
            pltpu.VMEM((groups * rows, 128), F32),
            pltpu.VMEM((groups * rows, 2 * hidden), BF16),
            pltpu.VMEM((rows, 2 * shared), BF16),
            pltpu.VMEM((rows, mine), F32),
            pltpu.VMEM((rows, mine), BF16),
            pltpu.VMEM((2, half, mine), BF16),
            pltpu.VMEM((2, half, mine), BF16),
            pltpu.VMEM((2, half, part), F32),
            pltpu.VMEM((2, half, mine), BF16),
            pltpu.VMEM((2, rows, mine), BF16),
            pltpu.VMEM((2, chips + 1, rows, part), BF16),
            pltpu.VMEM((2, chips - 1, rows, part), BF16),
            pltpu.VMEM((rows, mine), F32),
            pltpu.VMEM((groups * rows, kwide + vwide), BF16),
            pltpu.VMEM((2 * local_heads, rows, 128), BF16),
            pltpu.VMEM((rows, 3 * rows), F32),
            pltpu.VMEM((rows, 3 * rows), BF16),
            pltpu.VMEM((2 * local_heads, rows, 128), F32),
            pltpu.VMEM((2 * local_heads, rows, 128), F32),
            pltpu.VMEM((2 * local_heads, rows, 128), F32),
            pltpu.VMEM((rows, 128), F32),
            pltpu.VMEM((rows, 2 * vwide), BF16),
            pltpu.VMEM((groups, 8, rows), F32),
            pltpu.VMEM((groups * rows, 128), F32),
            dma((5 + 3 * chips,)),
            dma((3, chips)),
            dma((3, chips)),
            dma((2, 2, chips, 2)),
            dma((2, chips, 2)),
            dma((2, chips, 2)),
            dma((2, chips, 2)),
            dma((2,)),
            dma((2,)),
            dma((4, chips, 2)),
            dma((4, chips, 2)),
            dma((4,)),
            dma((4,)),
            dma((3,)),
            dma((3,)),
            dma((7,)),
            dma((7,)),
            dma((2, chips)),
            dma((2, chips)),
            dma((2, 2, chips)),
            dma((2, 2, chips)),
            dma((2, chips - 1, 2)),
            dma((2, chips + 1, 2)),
            dma((9,)),
        ],
        compiler_params=pltpu.CompilerParams(
            collective_id=0, has_side_effects=True, vmem_limit_bytes=67043328
        ),
        name="layer",
    )(
        diff_lambda,
        query_heads,
        key_heads,
        value_heads,
        sub_gain[None, :],
        routed_input,
        routes.T,
        route_weights.T,
        table,
        out_weight,
        gate,
        up,
        down,
        shared_gate,
        shared_up,
        shared_down,
    )
    return pl.pallas_call(
        emit_kernel,
        out_shape=(out, out),
        in_specs=[hbm, hbm],
        out_specs=(hbm, hbm),
        scratch_shapes=[pltpu.VMEM((rows, part), BF16), pltpu.VMEM((rows, part), BF16), dma((4,))],
        name="emit",
    )(mixed, routed)


def solution(mesh):
    dense = mesh.shape["ep"] == 4 and mesh.shape["tp"] == 8

    def chosen(*arguments):
        fits = dense and arguments[9].shape[0] == 1 and arguments[6].shape[0] % 32 == 0
        return (kernel_body if fits else body)(*arguments)

    placed = (
        P("ep", "tp"),
        P("ep", "tp"),
        P("ep", "tp"),
        P("tp"),
        P(),
        P("tp", None),
        P("ep", "tp"),
        P("ep", None),
        P("ep", None),
        P("ep", None, "tp"),
        P("ep", None, "tp"),
        P("ep", "tp", None),
        P(None, "tp"),
        P(None, "tp"),
        P("tp", None),
    )
    return jax.shard_map(
        chosen, mesh=mesh, in_specs=placed, out_specs=(P("ep", "tp"), P("ep", "tp")), check_vma=False
    )
```

```python
import functools

import jax
import jax.numpy as jnp
import numpy as np
from jax import lax
from jax.experimental import pallas as pl
from jax.experimental.pallas import tpu as pltpu
from jax.sharding import PartitionSpec as P

ROPE_BASE = 10000.0
NORM_EPS = 1e-06
MASKED = -1e30


def rotate(values, positions):
    half_width = values.shape[-1] // 2
    inverse_freq = ROPE_BASE ** (-jnp.arange(half_width, dtype=jnp.float32) / half_width)
    angles = positions.astype(jnp.float32)[:, None] * inverse_freq[None, :]
    angles = angles.reshape((angles.shape[0],) + (1,) * (values.ndim - 2) + (half_width,))
    cosine = jnp.cos(angles)
    sine_part = jnp.sin(angles)
    lower = values[..., :half_width]
    upper = values[..., half_width:]
    return jnp.concatenate(
        [lower * cosine - upper * sine_part, upper * cosine + lower * sine_part], axis=-1
    )


def mixer_terms(query_heads, key_heads, value_heads, diff_lambda, sub_gain, out_weight):
    row_count = query_heads.shape[0]
    local_heads = diff_lambda.shape[0]
    value_width = value_heads.shape[1] // local_heads
    key_width = query_heads.shape[1] // (2 * local_heads)
    score_scale = key_width ** (-0.5)
    offset = lax.axis_index("ep") * row_count
    positions = offset + jnp.arange(row_count, dtype=jnp.int32)
    last_row = offset + row_count - 1
    query_rot = rotate(
        query_heads.astype(jnp.float32).reshape(row_count, local_heads, 2, key_width), positions
    ).astype(jnp.bfloat16)
    queries = jnp.transpose(query_rot, (1, 2, 0, 3))
    key_rot = (
        rotate(
            key_heads.astype(jnp.float32).reshape(row_count, local_heads, 2, key_width), positions
        )
        .astype(jnp.bfloat16)
        .reshape(row_count, local_heads * 2 * key_width)
    )
    start_state = (
        jnp.full((local_heads, 2, row_count), MASKED, jnp.float32),
        jnp.zeros((local_heads, 2, row_count), jnp.float32),
        jnp.zeros((local_heads, 2, row_count, value_width), jnp.float32),
    )
    carried = start_state
    key_piece = lax.all_gather(key_rot, "ep", axis=0, tiled=True)
    value_piece = lax.all_gather(value_heads, "ep", axis=0, tiled=True)
    piece_rows = key_piece.shape[0]
    key_block = 512
    block_count = piece_rows // key_block
    key_blocks = key_piece.reshape(block_count, key_block, local_heads, 2, key_width)
    value_blocks = value_piece.reshape(block_count, key_block, local_heads, value_width)

    def block_step(running, block_item):
        key_rows, value_rows, block_index = block_item
        block_start = block_index * key_block

        def attend_block(partial_state):
            maxima, totals, weighted = partial_state
            key_positions = block_start + jnp.arange(key_block, dtype=jnp.int32)
            visible = key_positions[None, :] <= positions[:, None]
            scores = (
                jnp.einsum("hmqd,khmd->hmqk", queries, key_rows, preferred_element_type=jnp.float32)
                * score_scale
            )
            scores = jnp.where(visible, scores, MASKED)
            new_maxima = jnp.maximum(maxima, jnp.max(scores, axis=3))
            exp_weights = jnp.where(visible, jnp.exp(scores - new_maxima[..., None]), 0.0)
            shrink = jnp.exp(maxima - new_maxima)
            new_totals = totals * shrink + jnp.sum(exp_weights, axis=3)
            update = jnp.einsum(
                "hmqk,khw->hmqw",
                exp_weights.astype(jnp.bfloat16),
                value_rows,
                preferred_element_type=jnp.float32,
            )
            return (new_maxima, new_totals, weighted * shrink[..., None] + update)

        return (
            lax.cond(
                block_start <= last_row, attend_block, lambda partial_state: partial_state, running
            ),
            None,
        )

    carried, _ = lax.scan(
        block_step, carried, (key_blocks, value_blocks, jnp.arange(block_count, dtype=jnp.int32))
    )
    maxima, totals, weighted = carried
    attended = weighted / totals[..., None]
    mixed_heads = attended[:, 0] - diff_lambda[:, None, None] * attended[:, 1]
    normed = (
        mixed_heads
        * lax.rsqrt(jnp.mean(mixed_heads * mixed_heads, axis=2, keepdims=True) + NORM_EPS)
        * sub_gain
    )
    heads_out = jnp.transpose(normed.astype(jnp.bfloat16), (1, 0, 2)).reshape(
        row_count, local_heads * value_width
    )
    return jnp.dot(heads_out, out_weight, preferred_element_type=jnp.float32)


def expert_terms(
    routed_input, routes, expert_gate, expert_up, expert_down, shared_gate, shared_up, shared_down
):
    row_count, part_width = routed_input.shape
    top_count = routes.shape[1]
    local_experts = expert_gate.shape[0]
    groups = lax.axis_size("ep")
    experts = local_experts * groups
    capacity = 2 * row_count * top_count // experts
    copies = row_count * top_count
    flat_routes = routes.reshape(copies)
    onehot = (flat_routes[:, None] == jnp.arange(experts, dtype=jnp.int32)[None, :]).astype(
        jnp.int32
    )
    rank_within = jnp.sum((jnp.cumsum(onehot, axis=0) - onehot) * onehot, axis=1)
    slot_index = flat_routes * capacity + rank_within
    placer = (
        slot_index[:, None] == jnp.arange(experts * capacity, dtype=jnp.int32)[None, :]
    ).astype(jnp.bfloat16)
    token_slots = jnp.sum(placer.reshape(row_count, top_count, experts * capacity), axis=1)
    outgoing = jnp.dot(token_slots.T, routed_input, preferred_element_type=jnp.float32).astype(
        jnp.bfloat16
    )
    arrived = lax.all_to_all(
        outgoing.reshape(groups, local_experts * capacity, part_width),
        "ep",
        split_axis=0,
        concat_axis=0,
        tiled=True,
    )
    slot_count = groups * capacity
    slot_rows = jnp.transpose(
        arrived.reshape(groups, local_experts, capacity, part_width), (1, 0, 2, 3)
    ).reshape(local_experts, slot_count, part_width)
    slot_piece = lax.all_gather(slot_rows, "tp", axis=2, tiled=True)
    own_piece = lax.all_gather(routed_input[None], "tp", axis=2, tiled=True)
    own_rows = own_piece[0]
    gate_sum = jnp.einsum(
        "emc,ecf->emf", slot_piece, expert_gate, preferred_element_type=jnp.float32
    )
    up_sum = jnp.einsum("emc,ecf->emf", slot_piece, expert_up, preferred_element_type=jnp.float32)
    square_sum = jnp.sum(jnp.square(slot_piece.astype(jnp.float32)), axis=2)
    shared_gate_sum = jnp.dot(own_rows, shared_gate, preferred_element_type=jnp.float32)
    shared_up_sum = jnp.dot(own_rows, shared_up, preferred_element_type=jnp.float32)
    shared_square = jnp.sum(jnp.square(own_rows.astype(jnp.float32)), axis=1)
    full_width = expert_gate.shape[1]
    factor = lax.rsqrt(square_sum / full_width + NORM_EPS)[..., None]
    hidden = (jax.nn.silu(gate_sum * factor) * (up_sum * factor)).astype(jnp.bfloat16)
    shared_factor = lax.rsqrt(shared_square / full_width + NORM_EPS)[:, None]
    shared_hidden = (
        jax.nn.silu(shared_gate_sum * shared_factor) * (shared_up_sum * shared_factor)
    ).astype(jnp.bfloat16)
    shared_terms = jnp.dot(shared_hidden, shared_down, preferred_element_type=jnp.float32)
    routed_terms = jnp.einsum(
        "emf,efd->emd", hidden, expert_down, preferred_element_type=jnp.float32
    )
    routed_sum = lax.psum_scatter(
        routed_terms.astype(jnp.bfloat16), "tp", scatter_dimension=2, tiled=True
    ).astype(jnp.float32)
    return (routed_sum, shared_terms, placer)


def expert_finish(routed_sum, shared_sum, placer, route_weights):
    local_experts, slot_count, part_width = routed_sum.shape
    groups = lax.axis_size("ep")
    capacity = slot_count // groups
    leaving = jnp.transpose(
        routed_sum.astype(jnp.bfloat16).reshape(local_experts, groups, capacity, part_width),
        (1, 0, 2, 3),
    ).reshape(groups, local_experts * capacity, part_width)
    returned = lax.all_to_all(leaving, "ep", split_axis=0, concat_axis=0, tiled=True)
    copy_results = jnp.dot(
        placer,
        returned.reshape(groups * local_experts * capacity, part_width),
        preferred_element_type=jnp.float32,
    )
    row_count, top_count = route_weights.shape
    routed = jnp.sum(
        copy_results.reshape(row_count, top_count, part_width) * route_weights[:, :, None], axis=1
    )
    return (routed + shared_sum).astype(jnp.bfloat16)


def body(
    query_heads,
    key_heads,
    value_heads,
    diff_lambda,
    sub_gain,
    out_weight,
    routed_input,
    routes,
    route_weights,
    expert_gate,
    expert_up,
    expert_down,
    shared_gate,
    shared_up,
    shared_down,
):
    mixer_partial = mixer_terms(
        query_heads, key_heads, value_heads, diff_lambda, sub_gain, out_weight
    )
    routed_sum, shared_terms, placer = expert_terms(
        routed_input,
        routes,
        expert_gate,
        expert_up,
        expert_down,
        shared_gate,
        shared_up,
        shared_down,
    )
    mixer_sum, shared_sum = (
        lax.psum_scatter(
            mixer_partial.astype(jnp.bfloat16), "tp", scatter_dimension=1, tiled=True
        ).astype(jnp.float32),
        lax.psum_scatter(
            shared_terms.astype(jnp.bfloat16), "tp", scatter_dimension=1, tiled=True
        ).astype(jnp.float32),
    )
    return (
        mixer_sum.astype(jnp.bfloat16),
        expert_finish(routed_sum, shared_sum, placer, route_weights),
    )


MESH = pl.DeviceIdType.MESH
F32 = jnp.float32
BF16 = jnp.bfloat16
OWN, XB, YB, DB = 0, 1, 2, 3


def low(value):
    return value.astype(BF16)


def f32(value):
    return value.astype(F32)


def mm(left, right):
    return jnp.dot(left, right, preferred_element_type=F32)


def near_first(chips):
    rows = [sorted((s for s in range(chips) if s != z), key=lambda s: (abs(s - z), s if z < chips // 2 else -s)) for z in range(chips)]
    return [[row[j] for row in rows] for j in range(chips - 1)]


def far_first(chips):
    rows = []
    for z in range(chips):
        right = list(range(chips - 1, z, -1))
        left = list(range(0, z))
        first, second = (right, left) if z < chips // 2 else (left, right)
        row = []
        while first or second:
            if first:
                row.append(first.pop(0))
            if second:
                row.append(second.pop(0))
        rows.append(row)
    return [[row[j] for row in rows] for j in range(chips - 1)]


def layer_kernel(
    chips,
    lam_ref,
    q_hbm,
    k_hbm,
    v_hbm,
    gain_hbm,
    x_hbm,
    routes_hbm,
    rw_hbm,
    tab_hbm,
    ow_hbm,
    gw_hbm,
    uw_hbm,
    dw_hbm,
    sg_hbm,
    su_hbm,
    sd_hbm,
    mix_hbm,
    out_hbm,
    mix_ref,
    out_ref,
    xall,
    guw,
    dw,
    sgu,
    sd,
    ow,
    tab,
    q_ref,
    k_ref,
    gain_ref,
    routes_ref,
    rw_ref,
    acc,
    sacc,
    ssq,
    hid,
    shid,
    oacc,
    dsend,
    esend,
    lsend,
    late,
    din,
    xyin,
    zin,
    zout,
    macc,
    kv,
    qrot,
    sc_s,
    sc_p,
    sc_m,
    sc_t,
    sc_o,
    sc_a,
    ho,
    shtab,
    shcol,
    w_l,
    w_s,
    w_r,
    ag_s,
    ag_r,
    xy_s,
    xy_r,
    dr_s,
    dr_r,
    pt_s,
    pt_r,
    kv_s,
    kv_r,
    sh_s,
    sh_r,
    h_s,
    h_r,
    d_s,
    d_r,
    e_s,
    e_r,
    z_s,
    z_r,
    in_l,
):
    rows, part = x_hbm.shape
    half = rows // 2
    wide = 2 * part
    hidden = gw_hbm.shape[1]
    shared = sg_hbm.shape[1]
    vwide = v_hbm.shape[1]
    kwide = k_hbm.shape[1]
    local_heads = lam_ref.shape[0]
    vd = vwide // local_heads
    qk = kwide // (2 * local_heads)
    e = lax.axis_index("ep")
    t = lax.axis_index("tp")
    z, c = t // 2, t % 2
    x, y = e % 2, e // 2
    pt = (e, t + 1 - 2 * c)
    xn = (e + 1 - 2 * x, t)
    yn = (e + 2 - 4 * y, t)
    zr = (e, t + 2)
    zl = (e, t - 2)
    has_r = z < chips - 1
    has_l = z > 0

    def chosen_by_z(column):
        return sum(order * (z == at).astype(jnp.int32) for at, order in enumerate(column))

    nears = [chosen_by_z(column) for column in near_first(chips)]
    fars = [chosen_by_z(column) for column in far_first(chips)] + [z]

    def remote(src, dst, send, recv, dev):
        pltpu.make_async_remote_copy(src, dst, send, recv, device_id=dev, device_id_type=MESH).start()

    def got(dst, recv):
        pltpu.make_async_remote_copy(dst, dst, recv, recv, device_id=pt, device_id_type=MESH).wait_recv()

    def sent(src, send):
        pltpu.make_async_remote_copy(src, src, send, send, device_id=pt, device_id_type=MESH).wait_send()

    def cols(index, width):
        return pl.ds(pl.multiple_of(index * width, width), width)

    barrier = pltpu.get_barrier_semaphore()
    for dev in (pt, xn, yn):
        pl.semaphore_signal(barrier, inc=1, device_id=dev, device_id_type=MESH)

    @pl.when(has_r)
    def _():
        pl.semaphore_signal(barrier, inc=1, device_id=zr, device_id_type=MESH)

    @pl.when(has_l)
    def _():
        pl.semaphore_signal(barrier, inc=1, device_id=zl, device_id_type=MESH)

    loads = [
        pltpu.make_async_copy(gw_hbm, guw.at[:, pl.ds(0, hidden)], w_l.at[0]),
        pltpu.make_async_copy(uw_hbm, guw.at[:, pl.ds(hidden, hidden)], w_l.at[1]),
        pltpu.make_async_copy(sg_hbm, sgu.at[:, pl.ds(0, shared)], w_l.at[2]),
        pltpu.make_async_copy(su_hbm, sgu.at[:, pl.ds(shared, shared)], w_l.at[3]),
        pltpu.make_async_copy(tab_hbm.at[pl.ds(pl.multiple_of(e * rows, rows), rows), :], tab, w_l.at[4]),
    ]
    downs = [(ow_hbm, ow, vwide), (sd_hbm, sd, shared), (dw_hbm, dw, hidden)]
    for i, (src, dst, depth) in enumerate(downs):
        for p in range(chips):
            loads.append(
                pltpu.make_async_copy(
                    src.at[:, cols(2 * p + c, part)],
                    dst.at[cols(c, depth), pl.ds(p * part, part)],
                    w_l.at[5 + i],
                )
            )
    own_rows = pl.ds(0, rows)
    inputs = [
        pltpu.make_async_copy(x_hbm, xall.at[own_rows, cols(t, part)], in_l.at[0]),
        pltpu.make_async_copy(q_hbm, q_ref, in_l.at[1]),
        pltpu.make_async_copy(k_hbm, k_ref, in_l.at[2]),
        pltpu.make_async_copy(v_hbm, kv.at[own_rows, pl.ds(kwide, vwide)], in_l.at[3]),
        pltpu.make_async_copy(routes_hbm, routes_ref, in_l.at[4]),
        pltpu.make_async_copy(rw_hbm, rw_ref, in_l.at[5]),
        pltpu.make_async_copy(gain_hbm, gain_ref, in_l.at[6]),
    ]
    inputs[0].start()
    inputs[1].start()
    inputs[2].start()
    loads[4].start()
    for copy in inputs[3:]:
        copy.start()


    def piece(block, s, core):
        return xall.at[pl.ds(block * rows, rows), cols(2 * s + core, part)]

    def base(block, h):
        if block in (OWN, DB):
            return block * rows + h * half
        early = h == (0 if block == XB else 1)
        return (rows if early else 2 * rows) + (0 if block == XB else half)

    def halved(block, s, h, core=None):
        return xall.at[pl.ds(base(block, h), half), cols(2 * s + (c if core is None else core), part)]

    def z_forward(src, kind, block, s, h, right, left, slot=None):
        @pl.when(right)
        def _():
            remote(src, halved(block, s, h), ag_s.at[kind, s, h], ag_r.at[kind, s, h], zr)

        @pl.when(left)
        def _():
            remote(src, halved(block, s, h), ag_s.at[kind, s if slot is None else slot, h], ag_r.at[kind, s, h], zl)

    def to_pair(src, block, s):
        remote(src, piece(block, s, c), pt_s.at[0], pt_r.at[block, s], pt)

    def half_of(i, order):
        return order if i == 0 else 1 - order

    def to_side(i, order, s, src):
        block, dev = ((XB, xn), (YB, yn))[i]
        target = halved(block, s, half_of(i, order))
        remote(src, target, xy_s.at[i], xy_r.at[order, s], dev)

    def own_half(i, order):
        to_side(i, order, z, halved(OWN, z, half_of(i, order)))

    def to_xy(s, order):
        for i in range(2):
            to_side(i, order, s, halved(OWN, s, half_of(i, order)))

    def side_rows(order, s, core):
        return xall.at[pl.ds((1 + order) * rows, rows), cols(2 * s + core, part)]

    def side_arrival(s, order):
        mine = side_rows(order, s, c)
        got(mine, xy_r.at[order, s])
        remote(mine, mine, pt_s.at[0], pt_r.at[1 + order, s], pt)

    def paired(block, s):
        got(piece(block, s, 1 - c), pt_r.at[block, s])

    def paired_sides(order, s):
        got(side_rows(order, s, 1 - c), pt_r.at[1 + order, s])

    inputs[0].wait()
    loads[0].start()
    loads[1].start()
    pl.semaphore_wait(barrier, 3 + has_r.astype(jnp.int32) + has_l.astype(jnp.int32))

    for h in range(2):
        z_forward(halved(OWN, z, h), 0, OWN, z, h, has_r, has_l, chips)
    own_half(0, 0)
    own_half(1, 0)
    to_pair(piece(OWN, z, c), OWN, z)

    expert_id = lax.broadcasted_iota(jnp.int32, (8, rows), 0)
    inputs[4].wait()
    inputs[5].wait()
    routes = routes_ref[...]
    weights = rw_ref[...]
    table = jnp.zeros((8, rows), F32)
    for k in range(routes.shape[0]):
        table = table + jnp.where(routes[k : k + 1, :] == expert_id, weights[k : k + 1, :], 0.0)
    shtab[OWN] = table
    remote(shtab.at[OWN], shtab.at[XB], sh_s.at[0], sh_r.at[0], xn)
    remote(shtab.at[OWN], shtab.at[YB], sh_s.at[0], sh_r.at[0], yn)

    for copy in inputs[1:4]:
        copy.wait()
    loads[4].wait()
    cosine, sine = tab[:, :128], tab[:, 128:]
    at_row = lax.broadcasted_iota(jnp.int32, (128, 128), 0)
    at_col = lax.broadcasted_iota(jnp.int32, (128, 128), 1)
    swapped = at_col + qk // 2 - qk * ((at_col // (qk // 2)) % 2)
    swap = jnp.where(at_row == swapped, 1.0, 0.0).astype(BF16)
    for i in range(kwide // 128):
        span = slice(i * 128, (i + 1) * 128)
        for src, dst in ((q_ref, qrot), (k_ref, None)):
            value = src[:, span]
            turned = low(f32(value) * cosine + mm(value, swap) * sine)
            if dst is None:
                kv[0:rows, span] = turned
            else:
                turned = turned * jnp.asarray(qk ** (-0.5), BF16)
                for m in range(2):
                    in_map = (lax.broadcasted_iota(jnp.int32, (rows, 128), 1) // qk) == m
                    dst[2 * i + m] = jnp.where(in_map, turned, jnp.zeros((rows, 128), BF16))

    def kv_rows(block, start, count):
        return kv.at[pl.ds(block * rows + start, count), :]

    remote(kv_rows(OWN, 0, rows), kv_rows(XB, 0, rows), kv_s.at[0], kv_r.at[0], xn)
    remote(kv_rows(OWN, 0, rows), kv_rows(YB, 0, rows), kv_s.at[0], kv_r.at[0], yn)

    own_half(0, 1)
    own_half(1, 1)
    for i in list(range(2, 4)) + list(range(5, len(loads))):
        loads[i].start()

    def give_down(i):
        src, dst, depth = downs[i]
        for p in range(chips):
            remote(
                src.at[:, cols(2 * p + 1 - c, part)],
                dst.at[cols(c, depth), pl.ds(p * part, part)],
                w_s.at[i],
                w_r.at[i],
                pt,
            )

    def down_ready(i):
        src, dst, depth = downs[i]
        mine = dst.at[cols(c, depth), :]
        pltpu.make_async_copy(mine, mine, w_l.at[5 + i]).wait()
        got(dst.at[cols(1 - c, depth), :], w_r.at[i])

    def chunk(start, count, at, depth, first, weight, target, width):
        tiles = target.shape[-1] // width
        span_rows = pl.ds(start, count)

        def tile(n, carry):
            span = cols(n, width)
            value = mm(xall[span_rows, cols(at, depth)], weight[cols(at, depth), span])
            if not first:
                value = value + target[span_rows, span]
            target[span_rows, span] = value
            return carry

        lax.fori_loop(0, tiles, tile, 0)

    def squares(start, count, at, depth, first):
        span = pl.ds(start, count)
        total = jnp.zeros((count, 128), F32) if first else ssq[span, :]
        for i in range(depth // 128):
            value = f32(xall[span, pl.ds(pl.multiple_of(at * depth + i * 128, 128), 128)])
            total = total + value * value
        ssq[span, :] = total

    def expert_rows(start, count, at, depth, first=False):
        chunk(start, count, at, depth, first, guw, acc, hidden)
        squares(start, count, at, depth, first)

    def expert_chunk(block, s, first, count=1):
        for b in range(block, block + count):
            if b in (OWN, DB):
                paired(b, s)
            else:
                paired_sides(b - XB, s)
        expert_rows(block * rows, count * rows, s, wide, first)

    def shared_chunk(s, first):
        chunk(0, rows, s, wide, first, sgu, sacc, 2 * shared)

    def activate(start, count, source, width, target, target_start, index):
        full = jnp.sum(ssq[pl.ds(start, count), :], axis=1, keepdims=True) / (chips * wide)
        factor = lax.rsqrt(full + NORM_EPS)
        span = pl.ds(target_start, count)
        gate = source[span, :width] * factor
        up = source[span, width:] * factor
        target[span, cols(c, width)] = low(gate / (1.0 + jnp.exp(-gate)) * up)
        mine = target.at[span, cols(c, width)]
        remote(mine, mine, h_s.at[0 if index < 4 else 1], h_r.at[index], pt)

    def expert_activate(start, count, index):
        activate(start, count, acc, hidden, hid, start, index)

    def expert_hidden(start, count, index):
        got(hid.at[pl.ds(start, count), cols(1 - c, hidden)], h_r.at[index])

    def z_arrival(kind, s, h):
        block = (OWN, DB)[kind]
        got(halved(block, s, h), ag_r.at[kind, s, h])
        z_forward(halved(block, s, h), kind, block, s, h, (s < z) & has_r, (s > z) & has_l)
        if h == 1:
            to_pair(piece(block, s, c), block, s)

    middle = has_l & has_r

    def at_middle(work):
        @pl.when(middle)
        def _():
            work()

    def at_edge(work):
        @pl.when(jnp.logical_not(middle))
        def _():
            work()

    def arrivals(kind, *orders):
        for h in range(2):
            for j in orders:
                z_arrival(kind, nears[j], h)

    def value_cols(h):
        return pl.ds(kwide + h * vd, vd)

    step_rows = 64
    ids = (e, xn[0], yn[0], xn[0] + yn[0] - e)
    bias = [jnp.where(ids[b] < e, 0.0, MASKED) for b in range(4)]

    inputs[6].wait()

    def attend_first(i):
        count = 3 * rows
        sc_s[...] = lax.dot_general(
            qrot[i], kv[0:count, cols(i // 2, 128)], (((1,), (1,)), ((), ())), preferred_element_type=F32
        )

        for r in range(0, rows, step_rows):
            at = slice(r, r + step_rows)
            key = lax.broadcasted_iota(jnp.int32, (step_rows, rows), 1)
            row = r + lax.broadcasted_iota(jnp.int32, (step_rows, rows), 0)
            scores = [
                jnp.where(key <= row, sc_s[at, 0:rows], MASKED),
                sc_s[at, rows : 2 * rows] + bias[XB],
                sc_s[at, 2 * rows :] + bias[YB],
            ]
            most = jnp.maximum(jnp.maximum(scores[0], scores[1]), scores[2])
            most = jnp.max(most, axis=1, keepdims=True)
            weight = [jnp.exp(score - most) for score in scores]
            total = jnp.sum(weight[0] + weight[1] + weight[2], axis=1, keepdims=True)
            for b in range(3):
                sc_p[at, b * rows : (b + 1) * rows] = low(weight[b])
            sc_m[i, at, :] = jnp.broadcast_to(most, (step_rows, 128))
            sc_t[i, at, :] = jnp.broadcast_to(total, (step_rows, 128))

        sc_o[i] = mm(sc_p[...], kv[0:count, value_cols(i // 2)])

    def attend_last(i):
        count = 3 * rows
        sc_s[:, 0:rows] = lax.dot_general(
            qrot[i], kv[count:, cols(i // 2, 128)], (((1,), (1,)), ((), ())), preferred_element_type=F32
        )

        for r in range(0, rows, step_rows):
            at = slice(r, r + step_rows)
            scores = sc_s[at, 0:rows] + bias[DB]
            before = sc_m[i, at, :]
            most = jnp.maximum(before, jnp.max(scores, axis=1, keepdims=True))
            weight = jnp.exp(scores - most[:, 0:1])
            shrink = jnp.exp(before - most)
            sc_p[at, 0:rows] = low(weight)
            sc_a[at, :] = shrink
            sc_t[i, at, :] = sc_t[i, at, :] * shrink + jnp.sum(weight, axis=1, keepdims=True)

        return (sc_o[i] * sc_a[...] + mm(sc_p[:, 0:rows], kv[count:, value_cols(i // 2)])) / sc_t[i]

    def finish_head(h):
        sc_o[2 * h] = attend_last(2 * h)
        mixed = sc_o[2 * h] - lam_ref[h] * attend_last(2 * h + 1)
        scale = lax.rsqrt(jnp.mean(mixed * mixed, axis=1, keepdims=True) + NORM_EPS)
        ho[:, pl.ds(pl.multiple_of(c * vwide + h * vd, 128), vd)] = low(mixed * scale * gain_ref[...])

    loads[0].wait()
    loads[1].wait()
    expert_chunk(OWN, z, True)
    at_middle(lambda: [z_arrival(0, nears[j], 0) for j in (0, 1)])
    loads[2].wait()
    loads[3].wait()
    shared_chunk(z, True)
    side_arrival(z, 0)
    remote(halved(XB, z, 0), halved(DB, z, 0), dr_s.at[0], dr_r.at[0], yn)
    remote(halved(YB, z, 1), halved(DB, z, 1), dr_s.at[0], dr_r.at[0], xn)
    at_middle(lambda: [z_arrival(0, nears[j], 1) for j in (0, 1)])
    at_edge(lambda: arrivals(0, 0))
    at_middle(lambda: z_arrival(0, nears[2], 0))
    expert_chunk(OWN, nears[0], False)
    shared_chunk(nears[0], False)
    got(kv_rows(XB, 0, 2 * rows), kv_r.at[0])
    remote(kv_rows(XB, 0, half), kv_rows(DB, 0, half), kv_s.at[0], kv_r.at[1], yn)
    remote(kv_rows(YB, half, half), kv_rows(DB, half, half), kv_s.at[0], kv_r.at[1], xn)
    got(shtab.at[pl.ds(XB, 2)], sh_r.at[0])
    remote(shtab.at[XB], shtab.at[DB], sh_s.at[0], sh_r.at[1], yn)
    to_xy(nears[0], 0)
    at_middle(lambda: to_xy(nears[1], 0))
    at_middle(lambda: z_arrival(0, nears[2], 1))
    at_middle(lambda: to_xy(nears[2], 0))
    attend_first(0)
    attend_first(1)
    side_arrival(z, 1)
    at_edge(lambda: arrivals(0, 1))
    at_edge(lambda: to_xy(nears[1], 0))
    got(piece(DB, z, c), dr_r.at[0])
    for h in range(2):
        z_forward(halved(DB, z, h), 1, DB, z, h, has_r, has_l, chips)
    to_pair(piece(DB, z, c), DB, z)
    give_down(0)
    attend_first(2)
    attend_first(3)
    expert_chunk(OWN, nears[1], False)
    shared_chunk(nears[1], False)

    def last_own():
        arrivals(0, 2)
        to_xy(nears[2], 0)

    at_edge(last_own)
    for j in range(chips - 1):
        to_xy(nears[j], 1)
    give_down(1)
    give_down(2)
    expert_chunk(XB, z, True, 2)
    at_middle(lambda: [z_arrival(1, nears[j], 0) for j in (0, 1)])
    got(kv_rows(DB, 0, rows), kv_r.at[1])
    finish_head(0)
    finish_head(1)
    mine = ho.at[:, cols(c, vwide)]
    remote(mine, mine, h_s.at[2], h_r.at[5], pt)
    at_middle(lambda: [z_arrival(1, nears[j], 1) for j in (0, 1)])
    side_arrival(nears[0], 0)
    expert_chunk(DB, z, True)
    expert_chunk(OWN, nears[2], False)
    expert_activate(0, rows, 0)
    shared_chunk(nears[2], False)
    activate(0, rows, sacc, shared, shid, 0, 4)
    at_edge(lambda: arrivals(1, 0))
    side_arrival(nears[1], 0)
    down_ready(0)
    got(ho.at[:, cols(1 - c, vwide)], h_r.at[5])
    for j in range(chips):
        span = cols(fars[j], part)
        macc[:, span] = mm(ho[...], ow[:, span])

    def z_send(kind, j, p, h, value_of):
        upstream = ((p > z) & has_l) | ((p < z) & has_r)
        at = pl.ds(h * half, half)
        slot = zout.at[kind, j, at]

        @pl.when(upstream)
        def _():
            got(zin.at[kind, p, at], z_r.at[kind, p, h])
            zout[kind, j, at] = low(value_of(at) + f32(zin[kind, p, at]))

        @pl.when(jnp.logical_not(upstream))
        def _():
            zout[kind, j, at] = low(value_of(at))

        @pl.when(p > z)
        def _():
            remote(slot, zin.at[kind, p, at], z_s.at[kind], z_r.at[kind, p, h], zr)

        @pl.when((p < z) & (p != z - 1))
        def _():
            remote(slot, zin.at[kind, p, at], z_s.at[kind], z_r.at[kind, p, h], zl)

        @pl.when((p < z) & (p == z - 1))
        def _():
            remote(slot, zin.at[kind, chips, at], z_s.at[kind], z_r.at[kind, chips, h], zl)

    def z_finish(kind, value_of):
        target = (mix_ref, out_ref)[kind]
        for h in range(2):
            at = pl.ds(h * half, half)

            @pl.when(has_l)
            def _():
                got(zin.at[kind, z, at], z_r.at[kind, z, h])

            @pl.when(has_r)
            def _():
                got(zin.at[kind, chips, at], z_r.at[kind, chips, h])

            @pl.when(has_l & has_r)
            def _():
                target[at] = low(value_of(at) + f32(zin[kind, z, at]) + f32(zin[kind, chips, at]))

            @pl.when(jnp.logical_not(has_l))
            def _():
                target[at] = low(value_of(at) + f32(zin[kind, chips, at]))

            @pl.when(jnp.logical_not(has_r))
            def _():
                target[at] = low(value_of(at) + f32(zin[kind, z, at]))

    def mixer_send(j):
        p = fars[j]
        for h in range(2):
            z_send(0, j, p, h, lambda at: macc[at, cols(p, part)])

    at_edge(lambda: [mixer_send(j) for j in range(chips - 1)])
    at_middle(lambda: z_arrival(1, nears[2], 0))
    down_ready(1)
    down_ready(2)
    got(shtab.at[DB], sh_r.at[1])
    for block in range(4):
        line = jnp.sum(jnp.where(expert_id == e, shtab[block], 0.0), axis=0, keepdims=True)
        column = jnp.broadcast_to(line, (128, rows)).T
        for h in range(2):
            shcol[pl.ds(base(block, h), half), :] = column[h * half : (h + 1) * half]
    EARLY, LATE, FAR = rows, 2 * rows, 3 * rows

    paired_sides(0, nears[0])
    expert_rows(EARLY, rows, nears[0], wide)
    side_arrival(nears[2], 0)
    paired_sides(0, nears[1])
    expert_rows(EARLY, rows, nears[1], wide)
    at_middle(lambda: z_arrival(1, nears[2], 1))
    at_edge(lambda: arrivals(1, 1))
    expert_rows(EARLY, rows, 2 * nears[2] + c, part)
    paired_sides(0, nears[2])
    expert_rows(EARLY, rows, 2 * nears[2] + 1 - c, part)
    expert_activate(EARLY, rows, 1)
    side_arrival(nears[0], 1)
    paired(DB, nears[0])
    expert_rows(FAR, rows, nears[0], wide)

    def down(start, count, p):
        span = pl.ds(start, count)
        return mm(hid[span, :], dw[:, cols(p, part)]) * shcol[span, 0:1]

    def own_down(p, carry):
        span = cols(p, part)
        oacc[:, span] = down(0, rows, p) + mm(shid[...], sd[:, span])
        return carry

    top, rest = pl.ds(0, half), pl.ds(half, half)
    sides = ((0, XB, 0, 1, xn), (1, YB, 1, 0, yn))

    def far_share(j):
        span = cols(fars[j], part)
        dsend[:, span] = low(down(FAR, rows, fars[j]))
        remote(dsend.at[top, span], din.at[0, :, span], d_s.at[0], d_r.at[j], xn)
        remote(dsend.at[rest, span], din.at[1, :, span], d_s.at[1], d_r.at[j], yn)

    def early_share(j):
        span = cols(fars[j], part)
        value = low(down(EARLY, rows, fars[j]))
        for i, start, now, later, dev in sides:
            esend[i, :, span] = value[i * half : (i + 1) * half]
            target = xyin.at[i, pl.ds(now * half, half), span]
            remote(esend.at[i, :, span], target, e_s.at[i, 0], e_r.at[j], dev)

    def late_share(j):
        span = cols(fars[j], part)
        value = down(LATE, rows, fars[j])
        for i in range(2):
            late[i] = value[i * half : (i + 1) * half]
        got(din.at[:, :, span], d_r.at[j])
        for i, start, now, later, dev in sides:
            lsend[i, :, span] = low(late[i] + f32(din[1 - i, :, span]))
            target = xyin.at[i, pl.ds(later * half, half), span]
            remote(lsend.at[i, :, span], target, e_s.at[i, 1], e_r.at[j], dev)

    def total(j):
        span = cols(fars[j], part)
        return lambda at: oacc[at, span] + f32(xyin[0, at, span]) + f32(xyin[1, at, span])

    def total_ready(j):
        span = cols(fars[j], part)
        got(xyin.at[:, :, span], e_r.at[j])

    def total_half(j, h):
        z_send(1, j, fars[j], h, total(j))

    def total_share(j):
        total_ready(j)
        total_half(j, 0)
        total_half(j, 1)

    expert_hidden(EARLY, rows, 1)
    early_share(0)
    early_share(1)
    expert_rows(FAR, rows, 2 * nears[1] + c, part)
    paired(DB, nears[1])
    expert_rows(FAR, rows, 2 * nears[1] + 1 - c, part)
    at_edge(lambda: arrivals(1, 2))
    expert_rows(FAR, rows, 2 * nears[2] + c, part)
    side_arrival(nears[1], 1)
    paired_sides(1, nears[0])
    expert_rows(LATE, rows, nears[0], wide)
    side_arrival(nears[2], 1)
    paired(DB, nears[2])
    expert_rows(FAR, rows, 2 * nears[2] + 1 - c, part)
    expert_activate(FAR, rows, 2)
    paired_sides(1, nears[1])
    expert_rows(LATE, rows, nears[1], wide)
    expert_hidden(FAR, rows, 2)
    far_share(0)
    far_share(1)
    expert_rows(LATE, rows, 2 * nears[2] + c, part)
    paired_sides(1, nears[2])
    expert_rows(LATE, rows, 2 * nears[2] + 1 - c, part)
    expert_activate(LATE, rows, 3)
    at_middle(lambda: mixer_send(0))
    expert_hidden(0, rows, 0)
    got(shid.at[:, cols(1 - c, shared)], h_r.at[4])
    lax.fori_loop(0, chips, own_down, 0)
    expert_hidden(LATE, rows, 3)
    late_share(0)
    far_share(2)
    at_middle(lambda: mixer_send(1))
    late_share(1)
    early_share(2)
    at_middle(lambda: mixer_send(2))
    at_edge(lambda: total_share(0))
    late_share(2)
    far_share(3)
    at_middle(lambda: total_share(0))
    at_edge(lambda: total_share(1))
    early_share(3)
    at_edge(lambda: total_share(2))

    def middle_first():
        total_ready(1)
        total_half(1, 0)
        total_ready(2)
        total_half(2, 0)

    def middle_second():
        total_half(1, 1)
        total_half(2, 1)

    at_middle(middle_first)
    late_share(3)
    at_middle(middle_second)
    z_finish(0, lambda at: macc[at, cols(z, part)])
    mix_out = pltpu.make_async_copy(mix_ref, mix_hbm, in_l.at[7])
    mix_out.start()
    total_ready(3)
    z_finish(1, total(3))
    routed_out = pltpu.make_async_copy(out_ref, out_hbm, in_l.at[8])
    routed_out.start()

    for kind in range(2):
        for s in range(chips):

            @pl.when((has_r & (s <= z)) | (has_l & (s > z)))
            def _():
                for h in range(2):
                    sent(halved(OWN, s, h), ag_s.at[kind, s, h])

        @pl.when(has_l)
        def _():
            for h in range(2):
                sent(halved(OWN, z, h), ag_s.at[kind, chips, h])

    for i in range(2):
        sent(dsend, xy_s.at[i])
        sent(dsend.at[top], d_s.at[i])
        sent(esend.at[i], e_s.at[i, 0])
        sent(lsend.at[i], e_s.at[i, 1])
        sent(zout.at[i], z_s.at[i])
    for i in range(3):
        src, dst, depth = downs[i]
        sent(dst.at[cols(c, depth), :], w_s.at[i])
    sent(xall.at[pl.ds(0, 2 * rows), :], pt_s.at[0])
    sent(piece(DB, z, c), dr_s.at[0])
    sent(kv_rows(OWN, 0, 3 * rows), kv_s.at[0])
    sent(shtab.at[pl.ds(OWN, 3)], sh_s.at[0])
    sent(hid.at[:, cols(c, hidden)], h_s.at[0])
    sent(shid.at[:, cols(c, shared)], h_s.at[1])
    sent(ho.at[:, cols(c, vwide)], h_s.at[2])
    mix_out.wait()
    routed_out.wait()


def emit_kernel(mixed_hbm, routed_hbm, mix_hbm, out_hbm, mixed, routed, sems):
    pairs = ((mixed_hbm, mixed, mix_hbm), (routed_hbm, routed, out_hbm))
    loads = [pltpu.make_async_copy(src, held, sems.at[i]) for i, (src, held, _) in enumerate(pairs)]
    stores = [pltpu.make_async_copy(held, dst, sems.at[2 + i]) for i, (_, held, dst) in enumerate(pairs)]
    for load in loads:
        load.start()
    for load, store in zip(loads, stores):
        load.wait()
        store.start()
    for store in stores:
        store.wait()


def rotation_table(positions, key_width):
    half_width = key_width // 2
    freq = np.float32(ROPE_BASE) ** (-np.arange(half_width, dtype=np.float32) / np.float32(half_width))
    angles = np.arange(positions, dtype=np.float32)[:, None] * freq.astype(np.float32)[None, :]
    angles = angles.astype(np.float64)
    cosine, sine = np.cos(angles), np.sin(angles)
    copies = 128 // key_width
    cosine = np.tile(np.concatenate([cosine, cosine], axis=1), (1, copies))
    sine = np.tile(np.concatenate([-sine, sine], axis=1), (1, copies))
    return np.concatenate([cosine, sine], axis=1).astype(np.float32)


def kernel_body(
    query_heads,
    key_heads,
    value_heads,
    diff_lambda,
    sub_gain,
    out_weight,
    routed_input,
    routes,
    route_weights,
    expert_gate,
    expert_up,
    expert_down,
    shared_gate,
    shared_up,
    shared_down,
):
    rows, part = routed_input.shape
    chips = lax.axis_size("tp") // 2
    groups = lax.axis_size("ep")
    gate, up, down = expert_gate[0], expert_up[0], expert_down[0]
    width, hidden = gate.shape
    shared = shared_gate.shape[1]
    kwide, vwide = key_heads.shape[1], value_heads.shape[1]
    local_heads = diff_lambda.shape[0]
    half, mine = rows // 2, width // 2
    table = jnp.asarray(rotation_table(groups * rows, kwide // (2 * local_heads)))
    smem = pl.BlockSpec(memory_space=pltpu.SMEM)
    hbm = pl.BlockSpec(memory_space=pl.ANY)
    dma = pltpu.SemaphoreType.DMA
    out = jax.ShapeDtypeStruct((rows, part), BF16)
    mixed, routed = pl.pallas_call(
        functools.partial(layer_kernel, chips),
        out_shape=(out, out),
        in_specs=[smem] + [hbm] * 15,
        out_specs=(hbm, hbm),
        scratch_shapes=[
            pltpu.VMEM((rows, part), BF16),
            pltpu.VMEM((rows, part), BF16),
            pltpu.VMEM((groups * rows, width), BF16),
            pltpu.VMEM((width, 2 * hidden), BF16),
            pltpu.VMEM((2 * hidden, mine), BF16),
            pltpu.VMEM((width, 2 * shared), BF16),
            pltpu.VMEM((2 * shared, mine), BF16),
            pltpu.VMEM((2 * vwide, mine), BF16),
            pltpu.VMEM((rows, 256), F32),
            pltpu.VMEM(query_heads.shape, BF16),
            pltpu.VMEM(key_heads.shape, BF16),
            pltpu.VMEM((1, sub_gain.shape[0]), F32),
            pltpu.VMEM(routes.shape[::-1], routes.dtype),
            pltpu.VMEM(routes.shape[::-1], F32),
            pltpu.VMEM((groups * rows, 2 * hidden), F32),
            pltpu.VMEM((rows, 2 * shared), F32),
            pltpu.VMEM((groups * rows, 128), F32),
            pltpu.VMEM((groups * rows, 2 * hidden), BF16),
            pltpu.VMEM((rows, 2 * shared), BF16),
            pltpu.VMEM((rows, mine), F32),
            pltpu.VMEM((rows, mine), BF16),
            pltpu.VMEM((2, half, mine), BF16),
            pltpu.VMEM((2, half, mine), BF16),
            pltpu.VMEM((2, half, part), F32),
            pltpu.VMEM((2, half, mine), BF16),
            pltpu.VMEM((2, rows, mine), BF16),
            pltpu.VMEM((2, chips + 1, rows, part), BF16),
            pltpu.VMEM((2, chips - 1, rows, part), BF16),
            pltpu.VMEM((rows, mine), F32),
            pltpu.VMEM((groups * rows, kwide + vwide), BF16),
            pltpu.VMEM((2 * local_heads, rows, 128), BF16),
            pltpu.VMEM((rows, 3 * rows), F32),
            pltpu.VMEM((rows, 3 * rows), BF16),
            pltpu.VMEM((2 * local_heads, rows, 128), F32),
            pltpu.VMEM((2 * local_heads, rows, 128), F32),
            pltpu.VMEM((2 * local_heads, rows, 128), F32),
            pltpu.VMEM((rows, 128), F32),
            pltpu.VMEM((rows, 2 * vwide), BF16),
            pltpu.VMEM((groups, 8, rows), F32),
            pltpu.VMEM((groups * rows, 128), F32),
            dma((8,)),
            dma((3,)),
            dma((3,)),
            dma((2, chips + 1, 2)),
            dma((2, chips, 2)),
            dma((2,)),
            dma((2, chips)),
            dma((1,)),
            dma((1,)),
            dma((1,)),
            dma((4, chips)),
            dma((1,)),
            dma((2,)),
            dma((1,)),
            dma((2,)),
            dma((3,)),
            dma((6,)),
            dma((2,)),
            dma((chips,)),
            dma((2, 2)),
            dma((chips,)),
            dma((2,)),
            dma((2, chips + 1, 2)),
            dma((9,)),
        ],
        compiler_params=pltpu.CompilerParams(
            collective_id=0, has_side_effects=True, vmem_limit_bytes=67043328
        ),
        name="layer",
    )(
        diff_lambda,
        query_heads,
        key_heads,
        value_heads,
        sub_gain[None, :],
        routed_input,
        routes.T,
        route_weights.T,
        table,
        out_weight,
        gate,
        up,
        down,
        shared_gate,
        shared_up,
        shared_down,
    )
    return pl.pallas_call(
        emit_kernel,
        out_shape=(out, out),
        in_specs=[hbm, hbm],
        out_specs=(hbm, hbm),
        scratch_shapes=[pltpu.VMEM((rows, part), BF16), pltpu.VMEM((rows, part), BF16), dma((4,))],
        name="emit",
    )(mixed, routed)


def solution(mesh):
    dense = mesh.shape["ep"] == 4 and mesh.shape["tp"] == 8

    def chosen(*arguments):
        fits = dense and arguments[9].shape[0] == 1 and arguments[6].shape[0] % 32 == 0
        return (kernel_body if fits else body)(*arguments)

    placed = (
        P("ep", "tp"),
        P("ep", "tp"),
        P("ep", "tp"),
        P("tp"),
        P(),
        P("tp", None),
        P("ep", "tp"),
        P("ep", None),
        P("ep", None),
        P("ep", None, "tp"),
        P("ep", None, "tp"),
        P("ep", "tp", None),
        P(None, "tp"),
        P(None, "tp"),
        P("tp", None),
    )
    return jax.shard_map(
        chosen, mesh=mesh, in_specs=placed, out_specs=(P("ep", "tp"), P("ep", "tp")), check_vma=False
    )
```

```python
import functools

import jax
import jax.numpy as jnp
import numpy as np
from jax import lax
from jax.experimental import pallas as pl
from jax.experimental.pallas import tpu as pltpu
from jax.sharding import PartitionSpec as P

ROPE_BASE = 10000.0
NORM_EPS = 1e-06
MASKED = -1e30


def rotate(values, positions):
    half_width = values.shape[-1] // 2
    inverse_freq = ROPE_BASE ** (-jnp.arange(half_width, dtype=jnp.float32) / half_width)
    angles = positions.astype(jnp.float32)[:, None] * inverse_freq[None, :]
    angles = angles.reshape((angles.shape[0],) + (1,) * (values.ndim - 2) + (half_width,))
    cosine = jnp.cos(angles)
    sine_part = jnp.sin(angles)
    lower = values[..., :half_width]
    upper = values[..., half_width:]
    return jnp.concatenate(
        [lower * cosine - upper * sine_part, upper * cosine + lower * sine_part], axis=-1
    )


def mixer_terms(query_heads, key_heads, value_heads, diff_lambda, sub_gain, out_weight):
    row_count = query_heads.shape[0]
    local_heads = diff_lambda.shape[0]
    value_width = value_heads.shape[1] // local_heads
    key_width = query_heads.shape[1] // (2 * local_heads)
    score_scale = key_width ** (-0.5)
    offset = lax.axis_index("ep") * row_count
    positions = offset + jnp.arange(row_count, dtype=jnp.int32)
    last_row = offset + row_count - 1
    query_rot = rotate(
        query_heads.astype(jnp.float32).reshape(row_count, local_heads, 2, key_width), positions
    ).astype(jnp.bfloat16)
    queries = jnp.transpose(query_rot, (1, 2, 0, 3))
    key_rot = (
        rotate(
            key_heads.astype(jnp.float32).reshape(row_count, local_heads, 2, key_width), positions
        )
        .astype(jnp.bfloat16)
        .reshape(row_count, local_heads * 2 * key_width)
    )
    start_state = (
        jnp.full((local_heads, 2, row_count), MASKED, jnp.float32),
        jnp.zeros((local_heads, 2, row_count), jnp.float32),
        jnp.zeros((local_heads, 2, row_count, value_width), jnp.float32),
    )
    carried = start_state
    key_piece = lax.all_gather(key_rot, "ep", axis=0, tiled=True)
    value_piece = lax.all_gather(value_heads, "ep", axis=0, tiled=True)
    piece_rows = key_piece.shape[0]
    key_block = 512
    block_count = piece_rows // key_block
    key_blocks = key_piece.reshape(block_count, key_block, local_heads, 2, key_width)
    value_blocks = value_piece.reshape(block_count, key_block, local_heads, value_width)

    def block_step(running, block_item):
        key_rows, value_rows, block_index = block_item
        block_start = block_index * key_block

        def attend_block(partial_state):
            maxima, totals, weighted = partial_state
            key_positions = block_start + jnp.arange(key_block, dtype=jnp.int32)
            visible = key_positions[None, :] <= positions[:, None]
            scores = (
                jnp.einsum("hmqd,khmd->hmqk", queries, key_rows, preferred_element_type=jnp.float32)
                * score_scale
            )
            scores = jnp.where(visible, scores, MASKED)
            new_maxima = jnp.maximum(maxima, jnp.max(scores, axis=3))
            exp_weights = jnp.where(visible, jnp.exp(scores - new_maxima[..., None]), 0.0)
            shrink = jnp.exp(maxima - new_maxima)
            new_totals = totals * shrink + jnp.sum(exp_weights, axis=3)
            update = jnp.einsum(
                "hmqk,khw->hmqw",
                exp_weights.astype(jnp.bfloat16),
                value_rows,
                preferred_element_type=jnp.float32,
            )
            return (new_maxima, new_totals, weighted * shrink[..., None] + update)

        return (
            lax.cond(
                block_start <= last_row, attend_block, lambda partial_state: partial_state, running
            ),
            None,
        )

    carried, _ = lax.scan(
        block_step, carried, (key_blocks, value_blocks, jnp.arange(block_count, dtype=jnp.int32))
    )
    maxima, totals, weighted = carried
    attended = weighted / totals[..., None]
    mixed_heads = attended[:, 0] - diff_lambda[:, None, None] * attended[:, 1]
    normed = (
        mixed_heads
        * lax.rsqrt(jnp.mean(mixed_heads * mixed_heads, axis=2, keepdims=True) + NORM_EPS)
        * sub_gain
    )
    heads_out = jnp.transpose(normed.astype(jnp.bfloat16), (1, 0, 2)).reshape(
        row_count, local_heads * value_width
    )
    return jnp.dot(heads_out, out_weight, preferred_element_type=jnp.float32)


def expert_terms(
    routed_input, routes, expert_gate, expert_up, expert_down, shared_gate, shared_up, shared_down
):
    row_count, part_width = routed_input.shape
    top_count = routes.shape[1]
    local_experts = expert_gate.shape[0]
    groups = lax.axis_size("ep")
    experts = local_experts * groups
    capacity = 2 * row_count * top_count // experts
    copies = row_count * top_count
    flat_routes = routes.reshape(copies)
    onehot = (flat_routes[:, None] == jnp.arange(experts, dtype=jnp.int32)[None, :]).astype(
        jnp.int32
    )
    rank_within = jnp.sum((jnp.cumsum(onehot, axis=0) - onehot) * onehot, axis=1)
    slot_index = flat_routes * capacity + rank_within
    placer = (
        slot_index[:, None] == jnp.arange(experts * capacity, dtype=jnp.int32)[None, :]
    ).astype(jnp.bfloat16)
    token_slots = jnp.sum(placer.reshape(row_count, top_count, experts * capacity), axis=1)
    outgoing = jnp.dot(token_slots.T, routed_input, preferred_element_type=jnp.float32).astype(
        jnp.bfloat16
    )
    arrived = lax.all_to_all(
        outgoing.reshape(groups, local_experts * capacity, part_width),
        "ep",
        split_axis=0,
        concat_axis=0,
        tiled=True,
    )
    slot_count = groups * capacity
    slot_rows = jnp.transpose(
        arrived.reshape(groups, local_experts, capacity, part_width), (1, 0, 2, 3)
    ).reshape(local_experts, slot_count, part_width)
    slot_piece = lax.all_gather(slot_rows, "tp", axis=2, tiled=True)
    own_piece = lax.all_gather(routed_input[None], "tp", axis=2, tiled=True)
    own_rows = own_piece[0]
    gate_sum = jnp.einsum(
        "emc,ecf->emf", slot_piece, expert_gate, preferred_element_type=jnp.float32
    )
    up_sum = jnp.einsum("emc,ecf->emf", slot_piece, expert_up, preferred_element_type=jnp.float32)
    square_sum = jnp.sum(jnp.square(slot_piece.astype(jnp.float32)), axis=2)
    shared_gate_sum = jnp.dot(own_rows, shared_gate, preferred_element_type=jnp.float32)
    shared_up_sum = jnp.dot(own_rows, shared_up, preferred_element_type=jnp.float32)
    shared_square = jnp.sum(jnp.square(own_rows.astype(jnp.float32)), axis=1)
    full_width = expert_gate.shape[1]
    factor = lax.rsqrt(square_sum / full_width + NORM_EPS)[..., None]
    hidden = (jax.nn.silu(gate_sum * factor) * (up_sum * factor)).astype(jnp.bfloat16)
    shared_factor = lax.rsqrt(shared_square / full_width + NORM_EPS)[:, None]
    shared_hidden = (
        jax.nn.silu(shared_gate_sum * shared_factor) * (shared_up_sum * shared_factor)
    ).astype(jnp.bfloat16)
    shared_terms = jnp.dot(shared_hidden, shared_down, preferred_element_type=jnp.float32)
    routed_terms = jnp.einsum(
        "emf,efd->emd", hidden, expert_down, preferred_element_type=jnp.float32
    )
    routed_sum = lax.psum_scatter(
        routed_terms.astype(jnp.bfloat16), "tp", scatter_dimension=2, tiled=True
    ).astype(jnp.float32)
    return (routed_sum, shared_terms, placer)


def expert_finish(routed_sum, shared_sum, placer, route_weights):
    local_experts, slot_count, part_width = routed_sum.shape
    groups = lax.axis_size("ep")
    capacity = slot_count // groups
    leaving = jnp.transpose(
        routed_sum.astype(jnp.bfloat16).reshape(local_experts, groups, capacity, part_width),
        (1, 0, 2, 3),
    ).reshape(groups, local_experts * capacity, part_width)
    returned = lax.all_to_all(leaving, "ep", split_axis=0, concat_axis=0, tiled=True)
    copy_results = jnp.dot(
        placer,
        returned.reshape(groups * local_experts * capacity, part_width),
        preferred_element_type=jnp.float32,
    )
    row_count, top_count = route_weights.shape
    routed = jnp.sum(
        copy_results.reshape(row_count, top_count, part_width) * route_weights[:, :, None], axis=1
    )
    return (routed + shared_sum).astype(jnp.bfloat16)


def body(
    query_heads,
    key_heads,
    value_heads,
    diff_lambda,
    sub_gain,
    out_weight,
    routed_input,
    routes,
    route_weights,
    expert_gate,
    expert_up,
    expert_down,
    shared_gate,
    shared_up,
    shared_down,
):
    mixer_partial = mixer_terms(
        query_heads, key_heads, value_heads, diff_lambda, sub_gain, out_weight
    )
    routed_sum, shared_terms, placer = expert_terms(
        routed_input,
        routes,
        expert_gate,
        expert_up,
        expert_down,
        shared_gate,
        shared_up,
        shared_down,
    )
    mixer_sum, shared_sum = (
        lax.psum_scatter(
            mixer_partial.astype(jnp.bfloat16), "tp", scatter_dimension=1, tiled=True
        ).astype(jnp.float32),
        lax.psum_scatter(
            shared_terms.astype(jnp.bfloat16), "tp", scatter_dimension=1, tiled=True
        ).astype(jnp.float32),
    )
    return (
        mixer_sum.astype(jnp.bfloat16),
        expert_finish(routed_sum, shared_sum, placer, route_weights),
    )


MESH = pl.DeviceIdType.MESH
F32 = jnp.float32
BF16 = jnp.bfloat16
OWN, XB, YB, DB = 0, 1, 2, 3


def low(value):
    return value.astype(BF16)


def f32(value):
    return value.astype(F32)


def mm(left, right):
    return jnp.dot(left, right, preferred_element_type=F32)


def near_first(chips):
    rows = [sorted((s for s in range(chips) if s != z), key=lambda s: (abs(s - z), s if z < chips // 2 else -s)) for z in range(chips)]
    return [[row[j] for row in rows] for j in range(chips - 1)]


def far_first(chips):
    rows = []
    for z in range(chips):
        right = list(range(chips - 1, z, -1))
        left = list(range(0, z))
        first, second = (right, left) if z < chips // 2 else (left, right)
        row = []
        while first or second:
            if first:
                row.append(first.pop(0))
            if second:
                row.append(second.pop(0))
        rows.append(row)
    return [[row[j] for row in rows] for j in range(chips - 1)]


def layer_kernel(
    chips,
    lam_ref,
    q_hbm,
    k_hbm,
    v_hbm,
    gain_hbm,
    x_hbm,
    routes_hbm,
    rw_hbm,
    tab_hbm,
    ow_hbm,
    gw_hbm,
    uw_hbm,
    dw_hbm,
    sg_hbm,
    su_hbm,
    sd_hbm,
    mix_ref,
    out_ref,
    xall,
    guw,
    dw,
    sgu,
    sd,
    ow,
    tab,
    q_ref,
    k_ref,
    gain_ref,
    routes_ref,
    rw_ref,
    acc,
    sacc,
    ssq,
    hid,
    shid,
    oacc,
    dsend,
    esend,
    lsend,
    late,
    din,
    xyin,
    zin,
    zout,
    macc,
    kv,
    qrot,
    sc_s,
    sc_p,
    sc_m,
    sc_t,
    sc_o,
    sc_a,
    ho,
    shtab,
    shcol,
    w_l,
    w_s,
    w_r,
    ag_s,
    ag_r,
    xy_s,
    xy_r,
    dr_s,
    dr_r,
    pt_s,
    pt_r,
    kv_s,
    kv_r,
    sh_s,
    sh_r,
    h_s,
    h_r,
    d_s,
    d_r,
    e_s,
    e_r,
    z_s,
    z_r,
    in_l,
):
    rows, part = x_hbm.shape
    half = rows // 2
    wide = 2 * part
    hidden = gw_hbm.shape[1]
    shared = sg_hbm.shape[1]
    vwide = v_hbm.shape[1]
    kwide = k_hbm.shape[1]
    local_heads = lam_ref.shape[0]
    vd = vwide // local_heads
    qk = kwide // (2 * local_heads)
    e = lax.axis_index("ep")
    t = lax.axis_index("tp")
    z, c = t // 2, t % 2
    x, y = e % 2, e // 2
    pt = (e, t + 1 - 2 * c)
    xn = (e + 1 - 2 * x, t)
    yn = (e + 2 - 4 * y, t)
    zr = (e, t + 2)
    zl = (e, t - 2)
    has_r = z < chips - 1
    has_l = z > 0

    def chosen_by_z(column):
        return sum(order * (z == at).astype(jnp.int32) for at, order in enumerate(column))

    nears = [chosen_by_z(column) for column in near_first(chips)]
    fars = [chosen_by_z(column) for column in far_first(chips)] + [z]

    def remote(src, dst, send, recv, dev):
        pltpu.make_async_remote_copy(src, dst, send, recv, device_id=dev, device_id_type=MESH).start()

    def got(dst, recv):
        pltpu.make_async_remote_copy(dst, dst, recv, recv, device_id=pt, device_id_type=MESH).wait_recv()

    def sent(src, send):
        pltpu.make_async_remote_copy(src, src, send, send, device_id=pt, device_id_type=MESH).wait_send()

    def cols(index, width):
        return pl.ds(pl.multiple_of(index * width, width), width)

    own_rows = pl.ds(0, rows)
    own_x = pltpu.make_async_copy(
        x_hbm, xall.at[own_rows, pl.ds(pl.multiple_of(t * part, part), part)], in_l.at[0]
    )
    own_x.start()
    barrier = pltpu.get_barrier_semaphore()
    for dev in (pt, xn, yn):
        pl.semaphore_signal(barrier, inc=1, device_id=dev, device_id_type=MESH)

    @pl.when(has_r)
    def _():
        pl.semaphore_signal(barrier, inc=1, device_id=zr, device_id_type=MESH)

    @pl.when(has_l)
    def _():
        pl.semaphore_signal(barrier, inc=1, device_id=zl, device_id_type=MESH)

    loads = [
        pltpu.make_async_copy(gw_hbm, guw.at[:, pl.ds(0, hidden)], w_l.at[0]),
        pltpu.make_async_copy(uw_hbm, guw.at[:, pl.ds(hidden, hidden)], w_l.at[1]),
        pltpu.make_async_copy(sg_hbm, sgu.at[:, pl.ds(0, shared)], w_l.at[2]),
        pltpu.make_async_copy(su_hbm, sgu.at[:, pl.ds(shared, shared)], w_l.at[3]),
        pltpu.make_async_copy(tab_hbm.at[pl.ds(pl.multiple_of(e * rows, rows), rows), :], tab, w_l.at[4]),
    ]
    downs = [(ow_hbm, ow, vwide), (sd_hbm, sd, shared), (dw_hbm, dw, hidden)]
    for i, (src, dst, depth) in enumerate(downs):
        for p in range(chips):
            loads.append(
                pltpu.make_async_copy(
                    src.at[:, cols(2 * p + c, part)],
                    dst.at[cols(c, depth), pl.ds(p * part, part)],
                    w_l.at[5 + i],
                )
            )
    inputs = [
        own_x,
        pltpu.make_async_copy(q_hbm, q_ref, in_l.at[1]),
        pltpu.make_async_copy(k_hbm, k_ref, in_l.at[2]),
        pltpu.make_async_copy(v_hbm, kv.at[own_rows, pl.ds(kwide, vwide)], in_l.at[3]),
        pltpu.make_async_copy(routes_hbm, routes_ref, in_l.at[4]),
        pltpu.make_async_copy(rw_hbm, rw_ref, in_l.at[5]),
        pltpu.make_async_copy(gain_hbm, gain_ref, in_l.at[6]),
    ]
    inputs[1].start()
    inputs[2].start()
    loads[4].start()
    for copy in inputs[3:]:
        copy.start()


    def piece(block, s, core):
        return xall.at[pl.ds(block * rows, rows), cols(2 * s + core, part)]

    def base(block, h):
        if block in (OWN, DB):
            return block * rows + h * half
        early = h == (0 if block == XB else 1)
        return (rows if early else 2 * rows) + (0 if block == XB else half)

    def halved(block, s, h, core=None):
        return xall.at[pl.ds(base(block, h), half), cols(2 * s + (c if core is None else core), part)]

    def z_forward(src, kind, block, s, h, right, left):
        @pl.when(right)
        def _():
            remote(src, halved(block, s, h), ag_s.at[0], ag_r.at[kind, s, h], zr)

        @pl.when(left)
        def _():
            remote(src, halved(block, s, h), ag_s.at[0], ag_r.at[kind, s, h], zl)

    def to_pair(src, block, s):
        remote(src, piece(block, s, c), pt_s.at[0], pt_r.at[block, s], pt)

    def half_of(i, order):
        return order if i == 0 else 1 - order

    def to_side(i, order, s, src):
        block, dev = ((XB, xn), (YB, yn))[i]
        target = halved(block, s, half_of(i, order))
        remote(src, target, xy_s.at[i], xy_r.at[order, s], dev)

    def own_half(i, order):
        to_side(i, order, z, halved(OWN, z, half_of(i, order)))

    def to_xy(s, order):
        for i in range(2):
            to_side(i, order, s, halved(OWN, s, half_of(i, order)))

    def side_rows(order, s, core):
        return xall.at[pl.ds((1 + order) * rows, rows), cols(2 * s + core, part)]

    def side_arrival(s, order):
        mine = side_rows(order, s, c)
        got(mine, xy_r.at[order, s])
        remote(mine, mine, pt_s.at[0], pt_r.at[1 + order, s], pt)

    def paired(block, s):
        got(piece(block, s, 1 - c), pt_r.at[block, s])

    def paired_sides(order, s):
        got(side_rows(order, s, 1 - c), pt_r.at[1 + order, s])

    inputs[0].wait()
    loads[0].start()
    loads[1].start()
    pl.semaphore_wait(barrier, 3 + has_r.astype(jnp.int32) + has_l.astype(jnp.int32))

    for h in range(2):
        z_forward(halved(OWN, z, h), 0, OWN, z, h, has_r, has_l)
    own_half(0, 0)
    own_half(1, 0)
    to_pair(piece(OWN, z, c), OWN, z)

    expert_id = lax.broadcasted_iota(jnp.int32, (8, rows), 0)
    inputs[4].wait()
    inputs[5].wait()
    routes = routes_ref[...]
    weights = rw_ref[...]
    table = jnp.zeros((8, rows), F32)
    for k in range(routes.shape[0]):
        table = table + jnp.where(routes[k : k + 1, :] == expert_id, weights[k : k + 1, :], 0.0)
    shtab[OWN] = table
    remote(shtab.at[OWN], shtab.at[XB], sh_s.at[0], sh_r.at[0], xn)
    remote(shtab.at[OWN], shtab.at[YB], sh_s.at[0], sh_r.at[0], yn)

    for copy in inputs[1:4]:
        copy.wait()
    loads[4].wait()
    cosine, sine = tab[:, :128], tab[:, 128:]
    at_row = lax.broadcasted_iota(jnp.int32, (128, 128), 0)
    at_col = lax.broadcasted_iota(jnp.int32, (128, 128), 1)
    swapped = at_col + qk // 2 - qk * ((at_col // (qk // 2)) % 2)
    swap = jnp.where(at_row == swapped, 1.0, 0.0).astype(BF16)
    for i in range(kwide // 128):
        span = slice(i * 128, (i + 1) * 128)
        for src, dst in ((q_ref, qrot), (k_ref, None)):
            value = src[:, span]
            turned = low(f32(value) * cosine + mm(value, swap) * sine)
            if dst is None:
                kv[0:rows, span] = turned
            else:
                turned = turned * jnp.asarray(qk ** (-0.5), BF16)
                for m in range(2):
                    in_map = (lax.broadcasted_iota(jnp.int32, (rows, 128), 1) // qk) == m
                    dst[2 * i + m] = jnp.where(in_map, turned, jnp.zeros((rows, 128), BF16))

    def kv_rows(block, start, count):
        return kv.at[pl.ds(block * rows + start, count), :]

    remote(kv_rows(OWN, 0, rows), kv_rows(XB, 0, rows), kv_s.at[0], kv_r.at[0], xn)
    remote(kv_rows(OWN, 0, rows), kv_rows(YB, 0, rows), kv_s.at[0], kv_r.at[0], yn)

    own_half(0, 1)
    own_half(1, 1)
    for i in list(range(2, 4)) + list(range(5, len(loads))):
        loads[i].start()

    def give_down(i):
        src, dst, depth = downs[i]
        for p in range(chips):
            remote(
                src.at[:, cols(2 * p + 1 - c, part)],
                dst.at[cols(c, depth), pl.ds(p * part, part)],
                w_s.at[i],
                w_r.at[i],
                pt,
            )

    def down_ready(i):
        src, dst, depth = downs[i]
        mine = dst.at[cols(c, depth), :]
        pltpu.make_async_copy(mine, mine, w_l.at[5 + i]).wait()
        got(dst.at[cols(1 - c, depth), :], w_r.at[i])

    def chunk(start, count, at, depth, first, weight, target, width):
        tiles = target.shape[-1] // width
        span_rows = pl.ds(start, count)

        def tile(n, carry):
            span = cols(n, width)
            value = mm(xall[span_rows, cols(at, depth)], weight[cols(at, depth), span])
            if not first:
                value = value + target[span_rows, span]
            target[span_rows, span] = value
            return carry

        lax.fori_loop(0, tiles, tile, 0)

    def squares(start, count, at, depth, first):
        span = pl.ds(start, count)
        total = jnp.zeros((count, 128), F32) if first else ssq[span, :]
        for i in range(depth // 128):
            value = f32(xall[span, pl.ds(pl.multiple_of(at * depth + i * 128, 128), 128)])
            total = total + value * value
        ssq[span, :] = total

    def expert_rows(start, count, at, depth, first=False):
        chunk(start, count, at, depth, first, guw, acc, hidden)
        squares(start, count, at, depth, first)

    def expert_chunk(block, s, first, count=1):
        for b in range(block, block + count):
            if b in (OWN, DB):
                paired(b, s)
            else:
                paired_sides(b - XB, s)
        expert_rows(block * rows, count * rows, s, wide, first)

    def shared_chunk(s, first):
        chunk(0, rows, s, wide, first, sgu, sacc, 2 * shared)

    def activate(start, count, source, width, target, target_start, index):
        full = jnp.sum(ssq[pl.ds(start, count), :], axis=1, keepdims=True) / (chips * wide)
        factor = lax.rsqrt(full + NORM_EPS)
        span = pl.ds(target_start, count)
        gate = source[span, :width] * factor
        up = source[span, width:] * factor
        target[span, cols(c, width)] = low(gate / (1.0 + jnp.exp(-gate)) * up)
        mine = target.at[span, cols(c, width)]
        remote(mine, mine, h_s.at[0 if index < 4 else 1], h_r.at[index], pt)

    def expert_activate(start, count, index):
        activate(start, count, acc, hidden, hid, start, index)

    def expert_hidden(start, count, index):
        got(hid.at[pl.ds(start, count), cols(1 - c, hidden)], h_r.at[index])

    def z_arrival(kind, s, h):
        block = (OWN, DB)[kind]
        got(halved(block, s, h), ag_r.at[kind, s, h])
        z_forward(halved(block, s, h), kind, block, s, h, (s < z) & has_r, (s > z) & has_l)
        if h == 1:
            to_pair(piece(block, s, c), block, s)

    middle = has_l & has_r

    def at_middle(work):
        @pl.when(middle)
        def _():
            work()

    def at_edge(work):
        @pl.when(jnp.logical_not(middle))
        def _():
            work()

    def arrivals(kind, *orders):
        for h in range(2):
            for j in orders:
                z_arrival(kind, nears[j], h)

    def value_cols(h):
        return pl.ds(kwide + h * vd, vd)

    step_rows = 64
    ids = (e, xn[0], yn[0], xn[0] + yn[0] - e)
    bias = [jnp.where(ids[b] < e, 0.0, MASKED) for b in range(4)]

    inputs[6].wait()

    def attend_first(i):
        count = 3 * rows
        sc_s[...] = lax.dot_general(
            qrot[i], kv[0:count, cols(i // 2, 128)], (((1,), (1,)), ((), ())), preferred_element_type=F32
        )

        for r in range(0, rows, step_rows):
            at = slice(r, r + step_rows)
            key = lax.broadcasted_iota(jnp.int32, (step_rows, rows), 1)
            row = r + lax.broadcasted_iota(jnp.int32, (step_rows, rows), 0)
            scores = [
                jnp.where(key <= row, sc_s[at, 0:rows], MASKED),
                sc_s[at, rows : 2 * rows] + bias[XB],
                sc_s[at, 2 * rows :] + bias[YB],
            ]
            most = jnp.maximum(jnp.maximum(scores[0], scores[1]), scores[2])
            most = jnp.max(most, axis=1, keepdims=True)
            weight = [jnp.exp(score - most) for score in scores]
            total = jnp.sum(weight[0] + weight[1] + weight[2], axis=1, keepdims=True)
            for b in range(3):
                sc_p[at, b * rows : (b + 1) * rows] = low(weight[b])
            sc_m[i, at, :] = jnp.broadcast_to(most, (step_rows, 128))
            sc_t[i, at, :] = jnp.broadcast_to(total, (step_rows, 128))

        sc_o[i] = mm(sc_p[...], kv[0:count, value_cols(i // 2)])

    def attend_last(i):
        count = 3 * rows
        sc_s[:, 0:rows] = lax.dot_general(
            qrot[i], kv[count:, cols(i // 2, 128)], (((1,), (1,)), ((), ())), preferred_element_type=F32
        )

        for r in range(0, rows, step_rows):
            at = slice(r, r + step_rows)
            scores = sc_s[at, 0:rows] + bias[DB]
            before = sc_m[i, at, :]
            most = jnp.maximum(before, jnp.max(scores, axis=1, keepdims=True))
            weight = jnp.exp(scores - most[:, 0:1])
            shrink = jnp.exp(before - most)
            sc_p[at, 0:rows] = low(weight)
            sc_a[at, :] = shrink
            sc_t[i, at, :] = sc_t[i, at, :] * shrink + jnp.sum(weight, axis=1, keepdims=True)

        return (sc_o[i] * sc_a[...] + mm(sc_p[:, 0:rows], kv[count:, value_cols(i // 2)])) / sc_t[i]

    def finish_head(h):
        sc_o[2 * h] = attend_last(2 * h)
        mixed = sc_o[2 * h] - lam_ref[h] * attend_last(2 * h + 1)
        scale = lax.rsqrt(jnp.mean(mixed * mixed, axis=1, keepdims=True) + NORM_EPS)
        ho[:, pl.ds(pl.multiple_of(c * vwide + h * vd, 128), vd)] = low(mixed * scale * gain_ref[...])

    loads[0].wait()
    loads[1].wait()
    expert_chunk(OWN, z, True)
    at_middle(lambda: [z_arrival(0, nears[j], 0) for j in (0, 1)])
    loads[2].wait()
    loads[3].wait()
    shared_chunk(z, True)
    side_arrival(z, 0)
    remote(halved(XB, z, 0), halved(DB, z, 0), dr_s.at[0], dr_r.at[0], yn)
    remote(halved(YB, z, 1), halved(DB, z, 1), dr_s.at[0], dr_r.at[0], xn)
    at_middle(lambda: [z_arrival(0, nears[j], 1) for j in (0, 1)])
    at_edge(lambda: arrivals(0, 0))
    at_middle(lambda: z_arrival(0, nears[2], 0))
    expert_chunk(OWN, nears[0], False)
    shared_chunk(nears[0], False)
    got(kv_rows(XB, 0, 2 * rows), kv_r.at[0])
    remote(kv_rows(XB, 0, half), kv_rows(DB, 0, half), kv_s.at[0], kv_r.at[1], yn)
    remote(kv_rows(YB, half, half), kv_rows(DB, half, half), kv_s.at[0], kv_r.at[1], xn)
    got(shtab.at[pl.ds(XB, 2)], sh_r.at[0])
    remote(shtab.at[XB], shtab.at[DB], sh_s.at[0], sh_r.at[1], yn)
    to_xy(nears[0], 0)
    at_middle(lambda: to_xy(nears[1], 0))
    at_middle(lambda: z_arrival(0, nears[2], 1))
    at_middle(lambda: to_xy(nears[2], 0))
    attend_first(0)
    attend_first(1)
    side_arrival(z, 1)
    at_edge(lambda: arrivals(0, 1))
    at_edge(lambda: to_xy(nears[1], 0))
    got(piece(DB, z, c), dr_r.at[0])
    for h in range(2):
        z_forward(halved(DB, z, h), 1, DB, z, h, has_r, has_l)
    to_pair(piece(DB, z, c), DB, z)
    give_down(0)
    attend_first(2)
    attend_first(3)
    expert_chunk(OWN, nears[1], False)
    shared_chunk(nears[1], False)

    def last_own():
        arrivals(0, 2)
        to_xy(nears[2], 0)

    at_edge(last_own)
    for j in range(chips - 1):
        to_xy(nears[j], 1)
    give_down(1)
    give_down(2)
    expert_chunk(XB, z, True, 2)
    at_middle(lambda: [z_arrival(1, nears[j], 0) for j in (0, 1)])
    got(kv_rows(DB, 0, rows), kv_r.at[1])
    finish_head(0)
    finish_head(1)
    mine = ho.at[:, cols(c, vwide)]
    remote(mine, mine, h_s.at[2], h_r.at[5], pt)
    at_middle(lambda: [z_arrival(1, nears[j], 1) for j in (0, 1)])
    side_arrival(nears[0], 0)
    expert_chunk(DB, z, True)
    expert_chunk(OWN, nears[2], False)
    expert_activate(0, rows, 0)
    shared_chunk(nears[2], False)
    activate(0, rows, sacc, shared, shid, 0, 4)
    at_edge(lambda: arrivals(1, 0))
    side_arrival(nears[1], 0)
    down_ready(0)
    got(ho.at[:, cols(1 - c, vwide)], h_r.at[5])
    for j in range(chips):
        span = cols(fars[j], part)
        macc[:, span] = mm(ho[...], ow[:, span])

    def z_send(kind, j, p, h, value_of):
        upstream = ((p > z) & has_l) | ((p < z) & has_r)
        at = pl.ds(h * half, half)
        slot = zout.at[kind, j, at]

        @pl.when(upstream)
        def _():
            got(zin.at[kind, p, at], z_r.at[kind, p, h])
            zout[kind, j, at] = low(value_of(at) + f32(zin[kind, p, at]))

        @pl.when(jnp.logical_not(upstream))
        def _():
            zout[kind, j, at] = low(value_of(at))

        @pl.when(p > z)
        def _():
            remote(slot, zin.at[kind, p, at], z_s.at[kind], z_r.at[kind, p, h], zr)

        @pl.when((p < z) & (p != z - 1))
        def _():
            remote(slot, zin.at[kind, p, at], z_s.at[kind], z_r.at[kind, p, h], zl)

        @pl.when((p < z) & (p == z - 1))
        def _():
            remote(slot, zin.at[kind, chips, at], z_s.at[kind], z_r.at[kind, chips, h], zl)

    def z_finish(kind, value_of):
        target = (mix_ref, out_ref)[kind]
        for h in range(2):
            at = pl.ds(h * half, half)

            @pl.when(has_l)
            def _():
                got(zin.at[kind, z, at], z_r.at[kind, z, h])

            @pl.when(has_r)
            def _():
                got(zin.at[kind, chips, at], z_r.at[kind, chips, h])

            @pl.when(has_l & has_r)
            def _():
                target[at] = low(value_of(at) + f32(zin[kind, z, at]) + f32(zin[kind, chips, at]))

            @pl.when(jnp.logical_not(has_l))
            def _():
                target[at] = low(value_of(at) + f32(zin[kind, chips, at]))

            @pl.when(jnp.logical_not(has_r))
            def _():
                target[at] = low(value_of(at) + f32(zin[kind, z, at]))

    def mixer_send(j):
        p = fars[j]
        for h in range(2):
            z_send(0, j, p, h, lambda at: macc[at, cols(p, part)])

    at_edge(lambda: [mixer_send(j) for j in range(chips - 1)])
    at_middle(lambda: z_arrival(1, nears[2], 0))
    down_ready(1)
    down_ready(2)
    got(shtab.at[DB], sh_r.at[1])
    for block in range(4):
        line = jnp.sum(jnp.where(expert_id == e, shtab[block], 0.0), axis=0, keepdims=True)
        column = jnp.broadcast_to(line, (128, rows)).T
        for h in range(2):
            shcol[pl.ds(base(block, h), half), :] = column[h * half : (h + 1) * half]
    EARLY, LATE, FAR = rows, 2 * rows, 3 * rows

    paired_sides(0, nears[0])
    expert_rows(EARLY, rows, nears[0], wide)
    side_arrival(nears[2], 0)
    paired_sides(0, nears[1])
    expert_rows(EARLY, rows, nears[1], wide)
    at_middle(lambda: z_arrival(1, nears[2], 1))
    at_edge(lambda: arrivals(1, 1))
    expert_rows(EARLY, rows, 2 * nears[2] + c, part)
    paired_sides(0, nears[2])
    expert_rows(EARLY, rows, 2 * nears[2] + 1 - c, part)
    expert_activate(EARLY, rows, 1)
    side_arrival(nears[0], 1)
    paired(DB, nears[0])
    expert_rows(FAR, rows, nears[0], wide)

    def down(start, count, p):
        span = pl.ds(start, count)
        return mm(hid[span, :], dw[:, cols(p, part)]) * shcol[span, 0:1]

    def own_down(p, carry):
        span = cols(p, part)
        oacc[:, span] = down(0, rows, p) + mm(shid[...], sd[:, span])
        return carry

    top, rest = pl.ds(0, half), pl.ds(half, half)
    sides = ((0, XB, 0, 1, xn), (1, YB, 1, 0, yn))

    def far_share(j):
        span = cols(fars[j], part)
        dsend[:, span] = low(down(FAR, rows, fars[j]))
        remote(dsend.at[top, span], din.at[0, :, span], d_s.at[0], d_r.at[j], xn)
        remote(dsend.at[rest, span], din.at[1, :, span], d_s.at[1], d_r.at[j], yn)

    def early_share(j):
        span = cols(fars[j], part)
        value = low(down(EARLY, rows, fars[j]))
        for i, start, now, later, dev in sides:
            esend[i, :, span] = value[i * half : (i + 1) * half]
            target = xyin.at[i, pl.ds(now * half, half), span]
            remote(esend.at[i, :, span], target, e_s.at[i, 0], e_r.at[j], dev)

    def late_share(j):
        span = cols(fars[j], part)
        value = down(LATE, rows, fars[j])
        for i in range(2):
            late[i] = value[i * half : (i + 1) * half]
        got(din.at[:, :, span], d_r.at[j])
        for i, start, now, later, dev in sides:
            lsend[i, :, span] = low(late[i] + f32(din[1 - i, :, span]))
            target = xyin.at[i, pl.ds(later * half, half), span]
            remote(lsend.at[i, :, span], target, e_s.at[i, 1], e_r.at[j], dev)

    def total(j):
        span = cols(fars[j], part)
        return lambda at: oacc[at, span] + f32(xyin[0, at, span]) + f32(xyin[1, at, span])

    def total_ready(j):
        span = cols(fars[j], part)
        got(xyin.at[:, :, span], e_r.at[j])

    def total_half(j, h):
        z_send(1, j, fars[j], h, total(j))

    def total_share(j):
        total_ready(j)
        total_half(j, 0)
        total_half(j, 1)

    expert_hidden(EARLY, rows, 1)
    early_share(0)
    early_share(1)
    expert_rows(FAR, rows, 2 * nears[1] + c, part)
    paired(DB, nears[1])
    expert_rows(FAR, rows, 2 * nears[1] + 1 - c, part)
    at_edge(lambda: arrivals(1, 2))
    expert_rows(FAR, rows, 2 * nears[2] + c, part)
    side_arrival(nears[1], 1)
    paired_sides(1, nears[0])
    expert_rows(LATE, rows, nears[0], wide)
    side_arrival(nears[2], 1)
    paired(DB, nears[2])
    expert_rows(FAR, rows, 2 * nears[2] + 1 - c, part)
    expert_activate(FAR, rows, 2)
    paired_sides(1, nears[1])
    expert_rows(LATE, rows, nears[1], wide)
    expert_hidden(FAR, rows, 2)
    far_share(0)
    far_share(1)
    expert_rows(LATE, rows, 2 * nears[2] + c, part)
    paired_sides(1, nears[2])
    expert_rows(LATE, rows, 2 * nears[2] + 1 - c, part)
    expert_activate(LATE, rows, 3)
    at_middle(lambda: mixer_send(0))
    expert_hidden(0, rows, 0)
    got(shid.at[:, cols(1 - c, shared)], h_r.at[4])
    lax.fori_loop(0, chips, own_down, 0)
    expert_hidden(LATE, rows, 3)
    late_share(0)
    far_share(2)
    at_middle(lambda: mixer_send(1))
    late_share(1)
    early_share(2)
    at_middle(lambda: mixer_send(2))
    at_edge(lambda: total_share(0))
    late_share(2)
    far_share(3)
    at_middle(lambda: total_share(0))
    at_edge(lambda: total_share(1))
    early_share(3)
    at_edge(lambda: total_share(2))

    def middle_first():
        total_ready(1)
        total_half(1, 0)
        total_ready(2)
        total_half(2, 0)

    def middle_second():
        total_half(1, 1)
        total_half(2, 1)

    at_middle(middle_first)
    late_share(3)
    at_middle(middle_second)
    z_finish(0, lambda at: macc[at, cols(z, part)])
    total_ready(3)
    z_finish(1, total(3))

    at_middle(lambda: sent(zin, ag_s.at[0]))
    at_edge(lambda: sent(zin.at[0, pl.ds(0, 2)], ag_s.at[0]))
    for i in range(2):
        sent(dsend, xy_s.at[i])
        sent(dsend.at[top], d_s.at[i])
        sent(esend.at[i], e_s.at[i, 0])
        sent(lsend.at[i], e_s.at[i, 1])
        sent(zout.at[i], z_s.at[i])
    for i in range(3):
        src, dst, depth = downs[i]
        sent(dst.at[cols(c, depth), :], w_s.at[i])
    sent(xall.at[pl.ds(0, 2 * rows), :], pt_s.at[0])
    sent(piece(DB, z, c), dr_s.at[0])
    sent(kv_rows(OWN, 0, 3 * rows), kv_s.at[0])
    sent(shtab.at[pl.ds(OWN, 3)], sh_s.at[0])
    sent(hid.at[:, cols(c, hidden)], h_s.at[0])
    sent(shid.at[:, cols(c, shared)], h_s.at[1])
    sent(ho.at[:, cols(c, vwide)], h_s.at[2])


def emit_kernel(mixed, routed, mix_hbm, out_hbm, sems):
    stores = [
        pltpu.make_async_copy(mixed, mix_hbm, sems.at[0]),
        pltpu.make_async_copy(routed, out_hbm, sems.at[1]),
    ]
    for store in stores:
        store.start()
    for store in stores:
        store.wait()


def rotation_table(positions, key_width):
    half_width = key_width // 2
    freq = np.float32(ROPE_BASE) ** (-np.arange(half_width, dtype=np.float32) / np.float32(half_width))
    angles = np.arange(positions, dtype=np.float32)[:, None] * freq.astype(np.float32)[None, :]
    angles = angles.astype(np.float64)
    cosine, sine = np.cos(angles), np.sin(angles)
    copies = 128 // key_width
    cosine = np.tile(np.concatenate([cosine, cosine], axis=1), (1, copies))
    sine = np.tile(np.concatenate([-sine, sine], axis=1), (1, copies))
    return np.concatenate([cosine, sine], axis=1).astype(np.float32)


def kernel_body(
    query_heads,
    key_heads,
    value_heads,
    diff_lambda,
    sub_gain,
    out_weight,
    routed_input,
    routes,
    route_weights,
    expert_gate,
    expert_up,
    expert_down,
    shared_gate,
    shared_up,
    shared_down,
):
    rows, part = routed_input.shape
    chips = lax.axis_size("tp") // 2
    groups = lax.axis_size("ep")
    gate, up, down = expert_gate[0], expert_up[0], expert_down[0]
    width, hidden = gate.shape
    shared = shared_gate.shape[1]
    kwide, vwide = key_heads.shape[1], value_heads.shape[1]
    local_heads = diff_lambda.shape[0]
    half, mine = rows // 2, width // 2
    table = jnp.asarray(rotation_table(groups * rows, kwide // (2 * local_heads)))
    smem = pl.BlockSpec(memory_space=pltpu.SMEM)
    hbm = pl.BlockSpec(memory_space=pl.ANY)
    dma = pltpu.SemaphoreType.DMA
    out = jax.ShapeDtypeStruct((rows, part), BF16)
    held = pltpu.VMEM((rows, part), BF16)
    vmem = pl.BlockSpec(memory_space=pltpu.VMEM)
    mixed, routed = pl.pallas_call(
        functools.partial(layer_kernel, chips),
        out_shape=(held, held),
        in_specs=[smem] + [hbm] * 15,
        out_specs=(vmem, vmem),
        scratch_shapes=[
            pltpu.VMEM((groups * rows, width), BF16),
            pltpu.VMEM((width, 2 * hidden), BF16),
            pltpu.VMEM((2 * hidden, mine), BF16),
            pltpu.VMEM((width, 2 * shared), BF16),
            pltpu.VMEM((2 * shared, mine), BF16),
            pltpu.VMEM((2 * vwide, mine), BF16),
            pltpu.VMEM((rows, 256), F32),
            pltpu.VMEM(query_heads.shape, BF16),
            pltpu.VMEM(key_heads.shape, BF16),
            pltpu.VMEM((1, sub_gain.shape[0]), F32),
            pltpu.VMEM(routes.shape[::-1], routes.dtype),
            pltpu.VMEM(routes.shape[::-1], F32),
            pltpu.VMEM((groups * rows, 2 * hidden), F32),
            pltpu.VMEM((rows, 2 * shared), F32),
            pltpu.VMEM((groups * rows, 128), F32),
            pltpu.VMEM((groups * rows, 2 * hidden), BF16),
            pltpu.VMEM((rows, 2 * shared), BF16),
            pltpu.VMEM((rows, mine), F32),
            pltpu.VMEM((rows, mine), BF16),
            pltpu.VMEM((2, half, mine), BF16),
            pltpu.VMEM((2, half, mine), BF16),
            pltpu.VMEM((2, half, part), F32),
            pltpu.VMEM((2, half, mine), BF16),
            pltpu.VMEM((2, rows, mine), BF16),
            pltpu.VMEM((2, chips + 1, rows, part), BF16),
            pltpu.VMEM((2, chips - 1, rows, part), BF16),
            pltpu.VMEM((rows, mine), F32),
            pltpu.VMEM((groups * rows, kwide + vwide), BF16),
            pltpu.VMEM((2 * local_heads, rows, 128), BF16),
            pltpu.VMEM((rows, 3 * rows), F32),
            pltpu.VMEM((rows, 3 * rows), BF16),
            pltpu.VMEM((2 * local_heads, rows, 128), F32),
            pltpu.VMEM((2 * local_heads, rows, 128), F32),
            pltpu.VMEM((2 * local_heads, rows, 128), F32),
            pltpu.VMEM((rows, 128), F32),
            pltpu.VMEM((rows, 2 * vwide), BF16),
            pltpu.VMEM((groups, 8, rows), F32),
            pltpu.VMEM((groups * rows, 128), F32),
            dma((8,)),
            dma((3,)),
            dma((3,)),
            dma((1,)),
            dma((2, chips, 2)),
            dma((2,)),
            dma((2, chips)),
            dma((1,)),
            dma((1,)),
            dma((1,)),
            dma((4, chips)),
            dma((1,)),
            dma((2,)),
            dma((1,)),
            dma((2,)),
            dma((3,)),
            dma((6,)),
            dma((2,)),
            dma((chips,)),
            dma((2, 2)),
            dma((chips,)),
            dma((2,)),
            dma((2, chips + 1, 2)),
            dma((7,)),
        ],
        compiler_params=pltpu.CompilerParams(
            collective_id=0, has_side_effects=True, vmem_limit_bytes=61865984
        ),
        name="layer",
    )(
        diff_lambda,
        query_heads,
        key_heads,
        value_heads,
        sub_gain[None, :],
        routed_input,
        routes.T,
        route_weights.T,
        table,
        out_weight,
        gate,
        up,
        down,
        shared_gate,
        shared_up,
        shared_down,
    )
    return pl.pallas_call(
        emit_kernel,
        out_shape=(out, out),
        in_specs=[vmem, vmem],
        out_specs=(hbm, hbm),
        scratch_shapes=[dma((2,))],
        compiler_params=pltpu.CompilerParams(vmem_limit_bytes=1 << 20),
        name="emit",
    )(mixed, routed)


def solution(mesh):
    dense = mesh.shape["ep"] == 4 and mesh.shape["tp"] == 8

    def chosen(*arguments):
        fits = dense and arguments[9].shape[0] == 1 and arguments[6].shape[0] % 32 == 0
        return (kernel_body if fits else body)(*arguments)

    placed = (
        P("ep", "tp"),
        P("ep", "tp"),
        P("ep", "tp"),
        P("tp"),
        P(),
        P("tp", None),
        P("ep", "tp"),
        P("ep", None),
        P("ep", None),
        P("ep", None, "tp"),
        P("ep", None, "tp"),
        P("ep", "tp", None),
        P(None, "tp"),
        P(None, "tp"),
        P("tp", None),
    )
    return jax.shard_map(
        chosen, mesh=mesh, in_specs=placed, out_specs=(P("ep", "tp"), P("ep", "tp")), check_vma=False
    )
```

```python
import functools

import jax
import jax.numpy as jnp
import numpy as np
from jax import lax
from jax.experimental import pallas as pl
from jax.experimental.pallas import tpu as pltpu
from jax.sharding import PartitionSpec as P

ROPE_BASE = 10000.0
NORM_EPS = 1e-06
MASKED = -1e30


def rotate(values, positions):
    half_width = values.shape[-1] // 2
    inverse_freq = ROPE_BASE ** (-jnp.arange(half_width, dtype=jnp.float32) / half_width)
    angles = positions.astype(jnp.float32)[:, None] * inverse_freq[None, :]
    angles = angles.reshape((angles.shape[0],) + (1,) * (values.ndim - 2) + (half_width,))
    cosine = jnp.cos(angles)
    sine_part = jnp.sin(angles)
    lower = values[..., :half_width]
    upper = values[..., half_width:]
    return jnp.concatenate(
        [lower * cosine - upper * sine_part, upper * cosine + lower * sine_part], axis=-1
    )


def mixer_terms(query_heads, key_heads, value_heads, diff_lambda, sub_gain, out_weight):
    row_count = query_heads.shape[0]
    local_heads = diff_lambda.shape[0]
    value_width = value_heads.shape[1] // local_heads
    key_width = query_heads.shape[1] // (2 * local_heads)
    score_scale = key_width ** (-0.5)
    offset = lax.axis_index("ep") * row_count
    positions = offset + jnp.arange(row_count, dtype=jnp.int32)
    last_row = offset + row_count - 1
    query_rot = rotate(
        query_heads.astype(jnp.float32).reshape(row_count, local_heads, 2, key_width), positions
    ).astype(jnp.bfloat16)
    queries = jnp.transpose(query_rot, (1, 2, 0, 3))
    key_rot = (
        rotate(
            key_heads.astype(jnp.float32).reshape(row_count, local_heads, 2, key_width), positions
        )
        .astype(jnp.bfloat16)
        .reshape(row_count, local_heads * 2 * key_width)
    )
    start_state = (
        jnp.full((local_heads, 2, row_count), MASKED, jnp.float32),
        jnp.zeros((local_heads, 2, row_count), jnp.float32),
        jnp.zeros((local_heads, 2, row_count, value_width), jnp.float32),
    )
    carried = start_state
    key_piece = lax.all_gather(key_rot, "ep", axis=0, tiled=True)
    value_piece = lax.all_gather(value_heads, "ep", axis=0, tiled=True)
    piece_rows = key_piece.shape[0]
    key_block = 512
    block_count = piece_rows // key_block
    key_blocks = key_piece.reshape(block_count, key_block, local_heads, 2, key_width)
    value_blocks = value_piece.reshape(block_count, key_block, local_heads, value_width)

    def block_step(running, block_item):
        key_rows, value_rows, block_index = block_item
        block_start = block_index * key_block

        def attend_block(partial_state):
            maxima, totals, weighted = partial_state
            key_positions = block_start + jnp.arange(key_block, dtype=jnp.int32)
            visible = key_positions[None, :] <= positions[:, None]
            scores = (
                jnp.einsum("hmqd,khmd->hmqk", queries, key_rows, preferred_element_type=jnp.float32)
                * score_scale
            )
            scores = jnp.where(visible, scores, MASKED)
            new_maxima = jnp.maximum(maxima, jnp.max(scores, axis=3))
            exp_weights = jnp.where(visible, jnp.exp(scores - new_maxima[..., None]), 0.0)
            shrink = jnp.exp(maxima - new_maxima)
            new_totals = totals * shrink + jnp.sum(exp_weights, axis=3)
            update = jnp.einsum(
                "hmqk,khw->hmqw",
                exp_weights.astype(jnp.bfloat16),
                value_rows,
                preferred_element_type=jnp.float32,
            )
            return (new_maxima, new_totals, weighted * shrink[..., None] + update)

        return (
            lax.cond(
                block_start <= last_row, attend_block, lambda partial_state: partial_state, running
            ),
            None,
        )

    carried, _ = lax.scan(
        block_step, carried, (key_blocks, value_blocks, jnp.arange(block_count, dtype=jnp.int32))
    )
    maxima, totals, weighted = carried
    attended = weighted / totals[..., None]
    mixed_heads = attended[:, 0] - diff_lambda[:, None, None] * attended[:, 1]
    normed = (
        mixed_heads
        * lax.rsqrt(jnp.mean(mixed_heads * mixed_heads, axis=2, keepdims=True) + NORM_EPS)
        * sub_gain
    )
    heads_out = jnp.transpose(normed.astype(jnp.bfloat16), (1, 0, 2)).reshape(
        row_count, local_heads * value_width
    )
    return jnp.dot(heads_out, out_weight, preferred_element_type=jnp.float32)


def expert_terms(
    routed_input, routes, expert_gate, expert_up, expert_down, shared_gate, shared_up, shared_down
):
    row_count, part_width = routed_input.shape
    top_count = routes.shape[1]
    local_experts = expert_gate.shape[0]
    groups = lax.axis_size("ep")
    experts = local_experts * groups
    capacity = 2 * row_count * top_count // experts
    copies = row_count * top_count
    flat_routes = routes.reshape(copies)
    onehot = (flat_routes[:, None] == jnp.arange(experts, dtype=jnp.int32)[None, :]).astype(
        jnp.int32
    )
    rank_within = jnp.sum((jnp.cumsum(onehot, axis=0) - onehot) * onehot, axis=1)
    slot_index = flat_routes * capacity + rank_within
    placer = (
        slot_index[:, None] == jnp.arange(experts * capacity, dtype=jnp.int32)[None, :]
    ).astype(jnp.bfloat16)
    token_slots = jnp.sum(placer.reshape(row_count, top_count, experts * capacity), axis=1)
    outgoing = jnp.dot(token_slots.T, routed_input, preferred_element_type=jnp.float32).astype(
        jnp.bfloat16
    )
    arrived = lax.all_to_all(
        outgoing.reshape(groups, local_experts * capacity, part_width),
        "ep",
        split_axis=0,
        concat_axis=0,
        tiled=True,
    )
    slot_count = groups * capacity
    slot_rows = jnp.transpose(
        arrived.reshape(groups, local_experts, capacity, part_width), (1, 0, 2, 3)
    ).reshape(local_experts, slot_count, part_width)
    slot_piece = lax.all_gather(slot_rows, "tp", axis=2, tiled=True)
    own_piece = lax.all_gather(routed_input[None], "tp", axis=2, tiled=True)
    own_rows = own_piece[0]
    gate_sum = jnp.einsum(
        "emc,ecf->emf", slot_piece, expert_gate, preferred_element_type=jnp.float32
    )
    up_sum = jnp.einsum("emc,ecf->emf", slot_piece, expert_up, preferred_element_type=jnp.float32)
    square_sum = jnp.sum(jnp.square(slot_piece.astype(jnp.float32)), axis=2)
    shared_gate_sum = jnp.dot(own_rows, shared_gate, preferred_element_type=jnp.float32)
    shared_up_sum = jnp.dot(own_rows, shared_up, preferred_element_type=jnp.float32)
    shared_square = jnp.sum(jnp.square(own_rows.astype(jnp.float32)), axis=1)
    full_width = expert_gate.shape[1]
    factor = lax.rsqrt(square_sum / full_width + NORM_EPS)[..., None]
    hidden = (jax.nn.silu(gate_sum * factor) * (up_sum * factor)).astype(jnp.bfloat16)
    shared_factor = lax.rsqrt(shared_square / full_width + NORM_EPS)[:, None]
    shared_hidden = (
        jax.nn.silu(shared_gate_sum * shared_factor) * (shared_up_sum * shared_factor)
    ).astype(jnp.bfloat16)
    shared_terms = jnp.dot(shared_hidden, shared_down, preferred_element_type=jnp.float32)
    routed_terms = jnp.einsum(
        "emf,efd->emd", hidden, expert_down, preferred_element_type=jnp.float32
    )
    routed_sum = lax.psum_scatter(
        routed_terms.astype(jnp.bfloat16), "tp", scatter_dimension=2, tiled=True
    ).astype(jnp.float32)
    return (routed_sum, shared_terms, placer)


def expert_finish(routed_sum, shared_sum, placer, route_weights):
    local_experts, slot_count, part_width = routed_sum.shape
    groups = lax.axis_size("ep")
    capacity = slot_count // groups
    leaving = jnp.transpose(
        routed_sum.astype(jnp.bfloat16).reshape(local_experts, groups, capacity, part_width),
        (1, 0, 2, 3),
    ).reshape(groups, local_experts * capacity, part_width)
    returned = lax.all_to_all(leaving, "ep", split_axis=0, concat_axis=0, tiled=True)
    copy_results = jnp.dot(
        placer,
        returned.reshape(groups * local_experts * capacity, part_width),
        preferred_element_type=jnp.float32,
    )
    row_count, top_count = route_weights.shape
    routed = jnp.sum(
        copy_results.reshape(row_count, top_count, part_width) * route_weights[:, :, None], axis=1
    )
    return (routed + shared_sum).astype(jnp.bfloat16)


def body(
    query_heads,
    key_heads,
    value_heads,
    diff_lambda,
    sub_gain,
    out_weight,
    routed_input,
    routes,
    route_weights,
    expert_gate,
    expert_up,
    expert_down,
    shared_gate,
    shared_up,
    shared_down,
):
    mixer_partial = mixer_terms(
        query_heads, key_heads, value_heads, diff_lambda, sub_gain, out_weight
    )
    routed_sum, shared_terms, placer = expert_terms(
        routed_input,
        routes,
        expert_gate,
        expert_up,
        expert_down,
        shared_gate,
        shared_up,
        shared_down,
    )
    mixer_sum, shared_sum = (
        lax.psum_scatter(
            mixer_partial.astype(jnp.bfloat16), "tp", scatter_dimension=1, tiled=True
        ).astype(jnp.float32),
        lax.psum_scatter(
            shared_terms.astype(jnp.bfloat16), "tp", scatter_dimension=1, tiled=True
        ).astype(jnp.float32),
    )
    return (
        mixer_sum.astype(jnp.bfloat16),
        expert_finish(routed_sum, shared_sum, placer, route_weights),
    )


MESH = pl.DeviceIdType.MESH
F32 = jnp.float32
BF16 = jnp.bfloat16
OWN, XB, YB, DB = 0, 1, 2, 3


def low(value):
    return value.astype(BF16)


def f32(value):
    return value.astype(F32)


def mm(left, right):
    return jnp.dot(left, right, preferred_element_type=F32)


def near_first(chips):
    rows = [sorted((s for s in range(chips) if s != z), key=lambda s: (abs(s - z), s if z < chips // 2 else -s)) for z in range(chips)]
    return [[row[j] for row in rows] for j in range(chips - 1)]


def far_first(chips):
    rows = []
    for z in range(chips):
        right = list(range(chips - 1, z, -1))
        left = list(range(0, z))
        first, second = (right, left) if z < chips // 2 else (left, right)
        row = []
        while first or second:
            if first:
                row.append(first.pop(0))
            if second:
                row.append(second.pop(0))
        rows.append(row)
    return [[row[j] for row in rows] for j in range(chips - 1)]


def layer_kernel(
    chips,
    lam_ref,
    q_hbm,
    k_hbm,
    v_hbm,
    gain_hbm,
    x_hbm,
    routes_hbm,
    rw_hbm,
    tab_hbm,
    ow_hbm,
    gw_hbm,
    uw_hbm,
    dw_hbm,
    sg_hbm,
    su_hbm,
    sd_hbm,
    mix_ref,
    out_ref,
    xall,
    guw,
    dw,
    sgu,
    sd,
    ow,
    tab,
    q_ref,
    k_ref,
    gain_ref,
    routes_ref,
    rw_ref,
    acc,
    sacc,
    ssq,
    hid,
    shid,
    oacc,
    dsend,
    esend,
    lsend,
    late,
    din,
    xyin,
    zin,
    zout,
    macc,
    kv,
    qrot,
    sc_s,
    sc_p,
    sc_m,
    sc_t,
    sc_o,
    sc_a,
    ho,
    shtab,
    shcol,
    w_l,
    w_s,
    w_r,
    ag_s,
    ag_r,
    xy_s,
    xy_r,
    dr_s,
    dr_r,
    pt_s,
    pt_r,
    kv_s,
    kv_r,
    sh_s,
    sh_r,
    h_s,
    h_r,
    d_s,
    d_r,
    e_s,
    e_r,
    z_s,
    z_r,
    in_l,
):
    rows, part = x_hbm.shape
    half = rows // 2
    wide = 2 * part
    hidden = gw_hbm.shape[1]
    shared = sg_hbm.shape[1]
    vwide = v_hbm.shape[1]
    kwide = k_hbm.shape[1]
    local_heads = lam_ref.shape[0]
    vd = vwide // local_heads
    qk = kwide // (2 * local_heads)
    e = lax.axis_index("ep")
    t = lax.axis_index("tp")
    z, c = t // 2, t % 2
    x, y = e % 2, e // 2
    pt = (e, t + 1 - 2 * c)
    xn = (e + 1 - 2 * x, t)
    yn = (e + 2 - 4 * y, t)
    zr = (e, t + 2)
    zl = (e, t - 2)
    has_r = z < chips - 1
    has_l = z > 0

    def chosen_by_z(column):
        return sum(order * (z == at).astype(jnp.int32) for at, order in enumerate(column))

    nears = [chosen_by_z(column) for column in near_first(chips)]
    fars = [chosen_by_z(column) for column in far_first(chips)] + [z]

    def remote(src, dst, send, recv, dev):
        pltpu.make_async_remote_copy(src, dst, send, recv, device_id=dev, device_id_type=MESH).start()

    def got(dst, recv):
        pltpu.make_async_remote_copy(dst, dst, recv, recv, device_id=pt, device_id_type=MESH).wait_recv()

    def sent(src, send):
        pltpu.make_async_remote_copy(src, src, send, send, device_id=pt, device_id_type=MESH).wait_send()

    def cols(index, width):
        return pl.ds(pl.multiple_of(index * width, width), width)

    own_rows = pl.ds(0, rows)
    own_x = pltpu.make_async_copy(
        x_hbm, xall.at[own_rows, pl.ds(pl.multiple_of(t * part, part), part)], in_l.at[0]
    )
    own_x.start()
    barrier = pltpu.get_barrier_semaphore()
    for dev in (pt, xn, yn):
        pl.semaphore_signal(barrier, inc=1, device_id=dev, device_id_type=MESH)

    @pl.when(has_r)
    def _():
        pl.semaphore_signal(barrier, inc=1, device_id=zr, device_id_type=MESH)

    @pl.when(has_l)
    def _():
        pl.semaphore_signal(barrier, inc=1, device_id=zl, device_id_type=MESH)

    loads = [
        pltpu.make_async_copy(gw_hbm, guw.at[:, pl.ds(0, hidden)], w_l.at[0]),
        pltpu.make_async_copy(uw_hbm, guw.at[:, pl.ds(hidden, hidden)], w_l.at[1]),
        pltpu.make_async_copy(sg_hbm, sgu.at[:, pl.ds(0, shared)], w_l.at[2]),
        pltpu.make_async_copy(su_hbm, sgu.at[:, pl.ds(shared, shared)], w_l.at[3]),
        pltpu.make_async_copy(tab_hbm.at[pl.ds(pl.multiple_of(e * rows, rows), rows), :], tab, w_l.at[4]),
    ]
    downs = [(ow_hbm, ow, vwide), (sd_hbm, sd, shared), (dw_hbm, dw, hidden)]
    for i, (src, dst, depth) in enumerate(downs):
        for p in range(chips):
            loads.append(
                pltpu.make_async_copy(
                    src.at[:, cols(2 * p + c, part)],
                    dst.at[cols(c, depth), pl.ds(p * part, part)],
                    w_l.at[5 + i],
                )
            )
    inputs = [
        own_x,
        pltpu.make_async_copy(q_hbm, q_ref, in_l.at[1]),
        pltpu.make_async_copy(k_hbm, k_ref, in_l.at[2]),
        pltpu.make_async_copy(v_hbm, kv.at[own_rows, pl.ds(kwide, vwide)], in_l.at[3]),
        pltpu.make_async_copy(routes_hbm, routes_ref, in_l.at[4]),
        pltpu.make_async_copy(rw_hbm, rw_ref, in_l.at[5]),
        pltpu.make_async_copy(gain_hbm, gain_ref, in_l.at[6]),
    ]
    inputs[1].start()
    inputs[2].start()
    loads[4].start()
    for copy in inputs[3:]:
        copy.start()


    def piece(block, s, core):
        return xall.at[pl.ds(block * rows, rows), cols(2 * s + core, part)]

    def base(block, h):
        if block in (OWN, DB):
            return block * rows + h * half
        early = h == (0 if block == XB else 1)
        return (rows if early else 2 * rows) + (0 if block == XB else half)

    def halved(block, s, h, core=None):
        return xall.at[pl.ds(base(block, h), half), cols(2 * s + (c if core is None else core), part)]

    def z_forward(src, kind, block, s, h, right, left):
        @pl.when(right)
        def _():
            remote(src, halved(block, s, h), ag_s.at[0], ag_r.at[kind, s, h], zr)

        @pl.when(left)
        def _():
            remote(src, halved(block, s, h), ag_s.at[0], ag_r.at[kind, s, h], zl)

    def to_pair(src, block, s):
        remote(src, piece(block, s, c), pt_s.at[0], pt_r.at[block, s], pt)

    def half_of(i, order):
        return order if i == 0 else 1 - order

    def to_side(i, order, s, src):
        block, dev = ((XB, xn), (YB, yn))[i]
        target = halved(block, s, half_of(i, order))
        remote(src, target, xy_s.at[i], xy_r.at[order, s], dev)

    def own_half(i, order):
        to_side(i, order, z, halved(OWN, z, half_of(i, order)))

    def to_xy(s, order):
        for i in range(2):
            to_side(i, order, s, halved(OWN, s, half_of(i, order)))

    def side_rows(order, s, core):
        return xall.at[pl.ds((1 + order) * rows, rows), cols(2 * s + core, part)]

    def side_arrival(s, order):
        mine = side_rows(order, s, c)
        got(mine, xy_r.at[order, s])
        remote(mine, mine, pt_s.at[0], pt_r.at[1 + order, s], pt)

    def paired(block, s):
        got(piece(block, s, 1 - c), pt_r.at[block, s])

    def paired_sides(order, s):
        got(side_rows(order, s, 1 - c), pt_r.at[1 + order, s])

    inputs[0].wait()
    loads[0].start()
    loads[1].start()
    pl.semaphore_wait(barrier, 3 + has_r.astype(jnp.int32) + has_l.astype(jnp.int32))

    for h in range(2):
        z_forward(halved(OWN, z, h), 0, OWN, z, h, has_r, has_l)
    own_half(0, 0)
    own_half(1, 0)
    to_pair(piece(OWN, z, c), OWN, z)

    expert_id = lax.broadcasted_iota(jnp.int32, (8, rows), 0)
    inputs[4].wait()
    inputs[5].wait()
    routes = routes_ref[...]
    weights = rw_ref[...]
    table = jnp.zeros((8, rows), F32)
    for k in range(routes.shape[0]):
        table = table + jnp.where(routes[k : k + 1, :] == expert_id, weights[k : k + 1, :], 0.0)
    shtab[OWN] = table
    remote(shtab.at[OWN], shtab.at[XB], sh_s.at[0], sh_r.at[0], xn)
    remote(shtab.at[OWN], shtab.at[YB], sh_s.at[0], sh_r.at[0], yn)

    for copy in inputs[1:4]:
        copy.wait()
    loads[4].wait()
    cosine, sine = tab[:, :128], tab[:, 128:]
    at_row = lax.broadcasted_iota(jnp.int32, (128, 128), 0)
    at_col = lax.broadcasted_iota(jnp.int32, (128, 128), 1)
    swapped = at_col + qk // 2 - qk * ((at_col // (qk // 2)) % 2)
    swap = jnp.where(at_row == swapped, 1.0, 0.0).astype(BF16)
    for i in range(kwide // 128):
        span = slice(i * 128, (i + 1) * 128)
        for src, dst in ((q_ref, qrot), (k_ref, None)):
            value = src[:, span]
            turned = low(f32(value) * cosine + mm(value, swap) * sine)
            if dst is None:
                kv[0:rows, span] = turned
            else:
                turned = turned * jnp.asarray(qk ** (-0.5), BF16)
                for m in range(2):
                    in_map = (lax.broadcasted_iota(jnp.int32, (rows, 128), 1) // qk) == m
                    dst[2 * i + m] = jnp.where(in_map, turned, jnp.zeros((rows, 128), BF16))

    def kv_rows(block, start, count):
        return kv.at[pl.ds(block * rows + start, count), :]

    remote(kv_rows(OWN, 0, rows), kv_rows(XB, 0, rows), kv_s.at[0], kv_r.at[0], xn)
    remote(kv_rows(OWN, 0, rows), kv_rows(YB, 0, rows), kv_s.at[0], kv_r.at[0], yn)

    own_half(0, 1)
    own_half(1, 1)
    for i in list(range(2, 4)) + list(range(5, len(loads))):
        loads[i].start()

    def give_down(i):
        src, dst, depth = downs[i]
        for p in range(chips):
            remote(
                src.at[:, cols(2 * p + 1 - c, part)],
                dst.at[cols(c, depth), pl.ds(p * part, part)],
                w_s.at[i],
                w_r.at[i],
                pt,
            )

    def down_ready(i):
        src, dst, depth = downs[i]
        mine = dst.at[cols(c, depth), :]
        pltpu.make_async_copy(mine, mine, w_l.at[5 + i]).wait()
        got(dst.at[cols(1 - c, depth), :], w_r.at[i])

    def chunk(start, count, at, depth, first, weight, target, width):
        tiles = target.shape[-1] // width
        span_rows = pl.ds(start, count)

        def tile(n, carry):
            span = cols(n, width)
            value = mm(xall[span_rows, cols(at, depth)], weight[cols(at, depth), span])
            if not first:
                value = value + target[span_rows, span]
            target[span_rows, span] = value
            return carry

        lax.fori_loop(0, tiles, tile, 0)

    def squares(start, count, at, depth, first):
        span = pl.ds(start, count)
        total = jnp.zeros((count, 128), F32) if first else ssq[span, :]
        for i in range(depth // 128):
            value = f32(xall[span, pl.ds(pl.multiple_of(at * depth + i * 128, 128), 128)])
            total = total + value * value
        ssq[span, :] = total

    def expert_rows(start, count, at, depth, first=False):
        chunk(start, count, at, depth, first, guw, acc, hidden)
        squares(start, count, at, depth, first)

    def expert_chunk(block, s, first, count=1):
        for b in range(block, block + count):
            if b in (OWN, DB):
                paired(b, s)
            else:
                paired_sides(b - XB, s)
        expert_rows(block * rows, count * rows, s, wide, first)

    def shared_chunk(s, first):
        chunk(0, rows, s, wide, first, sgu, sacc, 2 * shared)

    def activate(start, count, source, width, target, target_start, index):
        full = jnp.sum(ssq[pl.ds(start, count), :], axis=1, keepdims=True) / (chips * wide)
        factor = lax.rsqrt(full + NORM_EPS)
        span = pl.ds(target_start, count)
        gate = source[span, :width] * factor
        up = source[span, width:] * factor
        target[span, cols(c, width)] = low(gate / (1.0 + jnp.exp(-gate)) * up)
        mine = target.at[span, cols(c, width)]
        remote(mine, mine, h_s.at[0 if index < 4 else 1], h_r.at[index], pt)

    def expert_activate(start, count, index):
        activate(start, count, acc, hidden, hid, start, index)

    def expert_hidden(start, count, index):
        got(hid.at[pl.ds(start, count), cols(1 - c, hidden)], h_r.at[index])

    def z_arrival(kind, s, h):
        block = (OWN, DB)[kind]
        got(halved(block, s, h), ag_r.at[kind, s, h])
        z_forward(halved(block, s, h), kind, block, s, h, (s < z) & has_r, (s > z) & has_l)
        if h == 1:
            to_pair(piece(block, s, c), block, s)

    middle = has_l & has_r

    def at_middle(work):
        @pl.when(middle)
        def _():
            work()

    def at_edge(work):
        @pl.when(jnp.logical_not(middle))
        def _():
            work()

    def arrivals(kind, *orders):
        for h in range(2):
            for j in orders:
                z_arrival(kind, nears[j], h)

    def value_cols(h):
        return pl.ds(kwide + h * vd, vd)

    step_rows = 64
    ids = (e, xn[0], yn[0], xn[0] + yn[0] - e)
    bias = [jnp.where(ids[b] < e, 0.0, MASKED) for b in range(4)]

    inputs[6].wait()

    def attend_first(i):
        count = 3 * rows
        sc_s[...] = lax.dot_general(
            qrot[i], kv[0:count, cols(i // 2, 128)], (((1,), (1,)), ((), ())), preferred_element_type=F32
        )

        for r in range(0, rows, step_rows):
            at = slice(r, r + step_rows)
            key = lax.broadcasted_iota(jnp.int32, (step_rows, rows), 1)
            row = r + lax.broadcasted_iota(jnp.int32, (step_rows, rows), 0)
            scores = [
                jnp.where(key <= row, sc_s[at, 0:rows], MASKED),
                sc_s[at, rows : 2 * rows] + bias[XB],
                sc_s[at, 2 * rows :] + bias[YB],
            ]
            most = jnp.maximum(jnp.maximum(scores[0], scores[1]), scores[2])
            most = jnp.max(most, axis=1, keepdims=True)
            weight = [jnp.exp(score - most) for score in scores]
            total = jnp.sum(weight[0] + weight[1] + weight[2], axis=1, keepdims=True)
            for b in range(3):
                sc_p[at, b * rows : (b + 1) * rows] = low(weight[b])
            sc_m[i, at, :] = jnp.broadcast_to(most, (step_rows, 128))
            sc_t[i, at, :] = jnp.broadcast_to(total, (step_rows, 128))

        sc_o[i] = mm(sc_p[...], kv[0:count, value_cols(i // 2)])

    def attend_last(i):
        count = 3 * rows
        sc_s[:, 0:rows] = lax.dot_general(
            qrot[i], kv[count:, cols(i // 2, 128)], (((1,), (1,)), ((), ())), preferred_element_type=F32
        )

        for r in range(0, rows, step_rows):
            at = slice(r, r + step_rows)
            scores = sc_s[at, 0:rows] + bias[DB]
            before = sc_m[i, at, :]
            most = jnp.maximum(before, jnp.max(scores, axis=1, keepdims=True))
            weight = jnp.exp(scores - most[:, 0:1])
            shrink = jnp.exp(before - most)
            sc_p[at, 0:rows] = low(weight)
            sc_a[at, :] = shrink
            sc_t[i, at, :] = sc_t[i, at, :] * shrink + jnp.sum(weight, axis=1, keepdims=True)

        return (sc_o[i] * sc_a[...] + mm(sc_p[:, 0:rows], kv[count:, value_cols(i // 2)])) / sc_t[i]

    def finish_head(h):
        sc_o[2 * h] = attend_last(2 * h)
        mixed = sc_o[2 * h] - lam_ref[h] * attend_last(2 * h + 1)
        scale = lax.rsqrt(jnp.mean(mixed * mixed, axis=1, keepdims=True) + NORM_EPS)
        ho[:, pl.ds(pl.multiple_of(c * vwide + h * vd, 128), vd)] = low(mixed * scale * gain_ref[...])

    loads[0].wait()
    loads[1].wait()
    expert_chunk(OWN, z, True)
    at_middle(lambda: [z_arrival(0, nears[j], 0) for j in (0, 1)])
    loads[2].wait()
    loads[3].wait()
    shared_chunk(z, True)
    side_arrival(z, 0)
    remote(halved(XB, z, 0), halved(DB, z, 0), dr_s.at[0], dr_r.at[0], yn)
    remote(halved(YB, z, 1), halved(DB, z, 1), dr_s.at[0], dr_r.at[0], xn)
    at_middle(lambda: [z_arrival(0, nears[j], 1) for j in (0, 1)])
    at_edge(lambda: arrivals(0, 0))
    at_middle(lambda: z_arrival(0, nears[2], 0))
    expert_chunk(OWN, nears[0], False)
    shared_chunk(nears[0], False)
    got(kv_rows(XB, 0, 2 * rows), kv_r.at[0])
    remote(kv_rows(XB, 0, half), kv_rows(DB, 0, half), kv_s.at[0], kv_r.at[1], yn)
    remote(kv_rows(YB, half, half), kv_rows(DB, half, half), kv_s.at[0], kv_r.at[1], xn)
    got(shtab.at[pl.ds(XB, 2)], sh_r.at[0])
    remote(shtab.at[XB], shtab.at[DB], sh_s.at[0], sh_r.at[1], yn)
    to_xy(nears[0], 0)
    at_middle(lambda: to_xy(nears[1], 0))
    at_middle(lambda: z_arrival(0, nears[2], 1))
    at_middle(lambda: to_xy(nears[2], 0))
    attend_first(0)
    attend_first(1)
    side_arrival(z, 1)
    at_edge(lambda: arrivals(0, 1))
    at_edge(lambda: to_xy(nears[1], 0))
    got(piece(DB, z, c), dr_r.at[0])
    for h in range(2):
        z_forward(halved(DB, z, h), 1, DB, z, h, has_r, has_l)
    to_pair(piece(DB, z, c), DB, z)
    give_down(0)
    attend_first(2)
    attend_first(3)
    expert_chunk(OWN, nears[1], False)
    shared_chunk(nears[1], False)

    def last_own():
        arrivals(0, 2)
        to_xy(nears[2], 0)

    at_edge(last_own)
    for j in range(chips - 1):
        to_xy(nears[j], 1)
    give_down(1)
    give_down(2)
    expert_chunk(XB, z, True, 2)
    at_middle(lambda: [z_arrival(1, nears[j], 0) for j in (0, 1)])
    got(kv_rows(DB, 0, rows), kv_r.at[1])
    finish_head(0)
    finish_head(1)
    mine = ho.at[:, cols(c, vwide)]
    remote(mine, mine, h_s.at[2], h_r.at[5], pt)
    at_middle(lambda: [z_arrival(1, nears[j], 1) for j in (0, 1)])
    side_arrival(nears[0], 0)
    expert_chunk(DB, z, True)
    expert_chunk(OWN, nears[2], False)
    expert_activate(0, rows, 0)
    shared_chunk(nears[2], False)
    activate(0, rows, sacc, shared, shid, 0, 4)
    at_edge(lambda: arrivals(1, 0))
    side_arrival(nears[1], 0)
    down_ready(0)
    got(ho.at[:, cols(1 - c, vwide)], h_r.at[5])
    for j in range(chips):
        span = cols(fars[j], part)
        macc[:, span] = mm(ho[...], ow[:, span])

    def z_send(kind, j, p, h, value_of):
        upstream = ((p > z) & has_l) | ((p < z) & has_r)
        at = pl.ds(h * half, half)
        slot = zout.at[kind, j, at]

        @pl.when(upstream)
        def _():
            got(zin.at[kind, p, at], z_r.at[kind, p, h])
            zout[kind, j, at] = low(value_of(at) + f32(zin[kind, p, at]))

        @pl.when(jnp.logical_not(upstream))
        def _():
            zout[kind, j, at] = low(value_of(at))

        @pl.when(p > z)
        def _():
            remote(slot, zin.at[kind, p, at], z_s.at[kind], z_r.at[kind, p, h], zr)

        @pl.when((p < z) & (p != z - 1))
        def _():
            remote(slot, zin.at[kind, p, at], z_s.at[kind], z_r.at[kind, p, h], zl)

        @pl.when((p < z) & (p == z - 1))
        def _():
            remote(slot, zin.at[kind, chips, at], z_s.at[kind], z_r.at[kind, chips, h], zl)

    def z_finish(kind, value_of):
        target = (mix_ref, out_ref)[kind]
        for h in range(2):
            at = pl.ds(h * half, half)

            @pl.when(has_l)
            def _():
                got(zin.at[kind, z, at], z_r.at[kind, z, h])

            @pl.when(has_r)
            def _():
                got(zin.at[kind, chips, at], z_r.at[kind, chips, h])

            @pl.when(has_l & has_r)
            def _():
                target[at] = low(value_of(at) + f32(zin[kind, z, at]) + f32(zin[kind, chips, at]))

            @pl.when(jnp.logical_not(has_l))
            def _():
                target[at] = low(value_of(at) + f32(zin[kind, chips, at]))

            @pl.when(jnp.logical_not(has_r))
            def _():
                target[at] = low(value_of(at) + f32(zin[kind, z, at]))

    def mixer_send(j):
        p = fars[j]
        for h in range(2):
            z_send(0, j, p, h, lambda at: macc[at, cols(p, part)])

    at_edge(lambda: [mixer_send(j) for j in range(chips - 1)])
    at_middle(lambda: z_arrival(1, nears[2], 0))
    down_ready(1)
    down_ready(2)
    got(shtab.at[DB], sh_r.at[1])
    for block in range(4):
        line = jnp.sum(jnp.where(expert_id == e, shtab[block], 0.0), axis=0, keepdims=True)
        column = jnp.broadcast_to(line, (128, rows)).T
        for h in range(2):
            shcol[pl.ds(base(block, h), half), :] = column[h * half : (h + 1) * half]
    EARLY, LATE, FAR = rows, 2 * rows, 3 * rows

    paired_sides(0, nears[0])
    expert_rows(EARLY, rows, nears[0], wide)
    side_arrival(nears[2], 0)
    paired_sides(0, nears[1])
    expert_rows(EARLY, rows, nears[1], wide)
    at_middle(lambda: z_arrival(1, nears[2], 1))
    at_edge(lambda: arrivals(1, 1))
    expert_rows(EARLY, rows, 2 * nears[2] + c, part)
    paired_sides(0, nears[2])
    expert_rows(EARLY, rows, 2 * nears[2] + 1 - c, part)
    expert_activate(EARLY, rows, 1)
    side_arrival(nears[0], 1)
    paired(DB, nears[0])
    expert_rows(FAR, rows, nears[0], wide)

    def down(start, count, p):
        span = pl.ds(start, count)
        return mm(hid[span, :], dw[:, cols(p, part)]) * shcol[span, 0:1]

    def own_down(p, carry):
        span = cols(p, part)
        oacc[:, span] = down(0, rows, p) + mm(shid[...], sd[:, span])
        return carry

    top, rest = pl.ds(0, half), pl.ds(half, half)
    sides = ((0, XB, 0, 1, xn), (1, YB, 1, 0, yn))

    def far_share(j):
        span = cols(fars[j], part)
        dsend[:, span] = low(down(FAR, rows, fars[j]))
        remote(dsend.at[top, span], din.at[0, :, span], d_s.at[0], d_r.at[j], xn)
        remote(dsend.at[rest, span], din.at[1, :, span], d_s.at[1], d_r.at[j], yn)

    def early_share(j):
        span = cols(fars[j], part)
        value = low(down(EARLY, rows, fars[j]))
        for i, start, now, later, dev in sides:
            esend[i, :, span] = value[i * half : (i + 1) * half]
            target = xyin.at[i, pl.ds(now * half, half), span]
            remote(esend.at[i, :, span], target, e_s.at[i, 0], e_r.at[j], dev)

    def late_share(j):
        span = cols(fars[j], part)
        value = down(LATE, rows, fars[j])
        for i in range(2):
            late[i] = value[i * half : (i + 1) * half]
        got(din.at[:, :, span], d_r.at[j])
        for i, start, now, later, dev in sides:
            lsend[i, :, span] = low(late[i] + f32(din[1 - i, :, span]))
            target = xyin.at[i, pl.ds(later * half, half), span]
            remote(lsend.at[i, :, span], target, e_s.at[i, 1], e_r.at[j], dev)

    def total(j):
        span = cols(fars[j], part)
        return lambda at: oacc[at, span] + f32(xyin[0, at, span]) + f32(xyin[1, at, span])

    def total_ready(j):
        span = cols(fars[j], part)
        got(xyin.at[:, :, span], e_r.at[j])

    def total_half(j, h):
        z_send(1, j, fars[j], h, total(j))

    def total_share(j):
        total_ready(j)
        total_half(j, 0)
        total_half(j, 1)

    expert_hidden(EARLY, rows, 1)
    early_share(0)
    expert_chunk(DB, nears[1], False)
    at_edge(lambda: arrivals(1, 2))
    side_arrival(nears[1], 1)
    early_share(1)
    expert_rows(FAR, rows, 2 * nears[2] + c, part)
    side_arrival(nears[2], 1)
    paired(DB, nears[2])
    expert_rows(FAR, rows, 2 * nears[2] + 1 - c, part)
    expert_activate(FAR, rows, 2)
    paired_sides(1, nears[0])
    expert_rows(LATE, rows, nears[0], wide)
    expert_hidden(FAR, rows, 2)
    far_share(0)
    far_share(1)
    paired_sides(1, nears[1])
    expert_rows(LATE, rows, nears[1], wide)
    expert_rows(LATE, rows, 2 * nears[2] + c, part)
    paired_sides(1, nears[2])
    expert_rows(LATE, rows, 2 * nears[2] + 1 - c, part)
    expert_activate(LATE, rows, 3)
    at_middle(lambda: mixer_send(0))
    expert_hidden(0, rows, 0)
    got(shid.at[:, cols(1 - c, shared)], h_r.at[4])
    lax.fori_loop(0, chips, own_down, 0)
    expert_hidden(LATE, rows, 3)
    late_share(0)
    far_share(2)
    at_middle(lambda: mixer_send(1))
    late_share(1)
    early_share(2)
    at_middle(lambda: mixer_send(2))
    at_edge(lambda: total_share(0))
    late_share(2)
    far_share(3)
    at_middle(lambda: total_share(0))
    at_edge(lambda: total_share(1))
    early_share(3)
    at_edge(lambda: total_share(2))

    def middle_first():
        total_ready(1)
        total_half(1, 0)
        total_ready(2)
        total_half(2, 0)

    def middle_second():
        total_half(1, 1)
        total_half(2, 1)

    at_middle(middle_first)
    late_share(3)
    at_middle(middle_second)
    z_finish(0, lambda at: macc[at, cols(z, part)])
    total_ready(3)
    z_finish(1, total(3))

    at_middle(lambda: sent(zin, ag_s.at[0]))
    at_edge(lambda: sent(zin.at[0, pl.ds(0, 2)], ag_s.at[0]))
    for i in range(2):
        sent(dsend, xy_s.at[i])
        sent(dsend.at[top], d_s.at[i])
        sent(esend.at[i], e_s.at[i, 0])
        sent(lsend.at[i], e_s.at[i, 1])
        sent(zout.at[i], z_s.at[i])
    for i in range(3):
        src, dst, depth = downs[i]
        sent(dst.at[cols(c, depth), :], w_s.at[i])
    sent(xall.at[pl.ds(0, 2 * rows), :], pt_s.at[0])
    sent(piece(DB, z, c), dr_s.at[0])
    sent(kv_rows(OWN, 0, 3 * rows), kv_s.at[0])
    sent(shtab.at[pl.ds(OWN, 3)], sh_s.at[0])
    sent(hid.at[:, cols(c, hidden)], h_s.at[0])
    sent(shid.at[:, cols(c, shared)], h_s.at[1])
    sent(ho.at[:, cols(c, vwide)], h_s.at[2])


def emit_kernel(mixed, routed, mix_hbm, out_hbm, sems):
    stores = [
        pltpu.make_async_copy(mixed, mix_hbm, sems.at[0]),
        pltpu.make_async_copy(routed, out_hbm, sems.at[1]),
    ]
    for store in stores:
        store.start()
    for store in stores:
        store.wait()


def rotation_table(positions, key_width):
    half_width = key_width // 2
    freq = np.float32(ROPE_BASE) ** (-np.arange(half_width, dtype=np.float32) / np.float32(half_width))
    angles = np.arange(positions, dtype=np.float32)[:, None] * freq.astype(np.float32)[None, :]
    angles = angles.astype(np.float64)
    cosine, sine = np.cos(angles), np.sin(angles)
    copies = 128 // key_width
    cosine = np.tile(np.concatenate([cosine, cosine], axis=1), (1, copies))
    sine = np.tile(np.concatenate([-sine, sine], axis=1), (1, copies))
    return np.concatenate([cosine, sine], axis=1).astype(np.float32)


def kernel_body(
    query_heads,
    key_heads,
    value_heads,
    diff_lambda,
    sub_gain,
    out_weight,
    routed_input,
    routes,
    route_weights,
    expert_gate,
    expert_up,
    expert_down,
    shared_gate,
    shared_up,
    shared_down,
):
    rows, part = routed_input.shape
    chips = lax.axis_size("tp") // 2
    groups = lax.axis_size("ep")
    gate, up, down = expert_gate[0], expert_up[0], expert_down[0]
    width, hidden = gate.shape
    shared = shared_gate.shape[1]
    kwide, vwide = key_heads.shape[1], value_heads.shape[1]
    local_heads = diff_lambda.shape[0]
    half, mine = rows // 2, width // 2
    table = jnp.asarray(rotation_table(groups * rows, kwide // (2 * local_heads)))
    smem = pl.BlockSpec(memory_space=pltpu.SMEM)
    hbm = pl.BlockSpec(memory_space=pl.ANY)
    dma = pltpu.SemaphoreType.DMA
    out = jax.ShapeDtypeStruct((rows, part), BF16)
    held = pltpu.VMEM((rows, part), BF16)
    vmem = pl.BlockSpec(memory_space=pltpu.VMEM)
    mixed, routed = pl.pallas_call(
        functools.partial(layer_kernel, chips),
        out_shape=(held, held),
        in_specs=[smem] + [hbm] * 15,
        out_specs=(vmem, vmem),
        scratch_shapes=[
            pltpu.VMEM((groups * rows, width), BF16),
            pltpu.VMEM((width, 2 * hidden), BF16),
            pltpu.VMEM((2 * hidden, mine), BF16),
            pltpu.VMEM((width, 2 * shared), BF16),
            pltpu.VMEM((2 * shared, mine), BF16),
            pltpu.VMEM((2 * vwide, mine), BF16),
            pltpu.VMEM((rows, 256), F32),
            pltpu.VMEM(query_heads.shape, BF16),
            pltpu.VMEM(key_heads.shape, BF16),
            pltpu.VMEM((1, sub_gain.shape[0]), F32),
            pltpu.VMEM(routes.shape[::-1], routes.dtype),
            pltpu.VMEM(routes.shape[::-1], F32),
            pltpu.VMEM((groups * rows, 2 * hidden), F32),
            pltpu.VMEM((rows, 2 * shared), F32),
            pltpu.VMEM((groups * rows, 128), F32),
            pltpu.VMEM((groups * rows, 2 * hidden), BF16),
            pltpu.VMEM((rows, 2 * shared), BF16),
            pltpu.VMEM((rows, mine), F32),
            pltpu.VMEM((rows, mine), BF16),
            pltpu.VMEM((2, half, mine), BF16),
            pltpu.VMEM((2, half, mine), BF16),
            pltpu.VMEM((2, half, part), F32),
            pltpu.VMEM((2, half, mine), BF16),
            pltpu.VMEM((2, rows, mine), BF16),
            pltpu.VMEM((2, chips + 1, rows, part), BF16),
            pltpu.VMEM((2, chips - 1, rows, part), BF16),
            pltpu.VMEM((rows, mine), F32),
            pltpu.VMEM((groups * rows, kwide + vwide), BF16),
            pltpu.VMEM((2 * local_heads, rows, 128), BF16),
            pltpu.VMEM((rows, 3 * rows), F32),
            pltpu.VMEM((rows, 3 * rows), BF16),
            pltpu.VMEM((2 * local_heads, rows, 128), F32),
            pltpu.VMEM((2 * local_heads, rows, 128), F32),
            pltpu.VMEM((2 * local_heads, rows, 128), F32),
            pltpu.VMEM((rows, 128), F32),
            pltpu.VMEM((rows, 2 * vwide), BF16),
            pltpu.VMEM((groups, 8, rows), F32),
            pltpu.VMEM((groups * rows, 128), F32),
            dma((8,)),
            dma((3,)),
            dma((3,)),
            dma((1,)),
            dma((2, chips, 2)),
            dma((2,)),
            dma((2, chips)),
            dma((1,)),
            dma((1,)),
            dma((1,)),
            dma((4, chips)),
            dma((1,)),
            dma((2,)),
            dma((1,)),
            dma((2,)),
            dma((3,)),
            dma((6,)),
            dma((2,)),
            dma((chips,)),
            dma((2, 2)),
            dma((chips,)),
            dma((2,)),
            dma((2, chips + 1, 2)),
            dma((7,)),
        ],
        compiler_params=pltpu.CompilerParams(
            collective_id=0, has_side_effects=True, vmem_limit_bytes=61865984
        ),
        name="layer",
    )(
        diff_lambda,
        query_heads,
        key_heads,
        value_heads,
        sub_gain[None, :],
        routed_input,
        routes.T,
        route_weights.T,
        table,
        out_weight,
        gate,
        up,
        down,
        shared_gate,
        shared_up,
        shared_down,
    )
    return pl.pallas_call(
        emit_kernel,
        out_shape=(out, out),
        in_specs=[vmem, vmem],
        out_specs=(hbm, hbm),
        scratch_shapes=[dma((2,))],
        compiler_params=pltpu.CompilerParams(vmem_limit_bytes=1 << 20),
        name="emit",
    )(mixed, routed)


def solution(mesh):
    dense = mesh.shape["ep"] == 4 and mesh.shape["tp"] == 8

    def chosen(*arguments):
        fits = dense and arguments[9].shape[0] == 1 and arguments[6].shape[0] % 32 == 0
        return (kernel_body if fits else body)(*arguments)

    placed = (
        P("ep", "tp"),
        P("ep", "tp"),
        P("ep", "tp"),
        P("tp"),
        P(),
        P("tp", None),
        P("ep", "tp"),
        P("ep", None),
        P("ep", None),
        P("ep", None, "tp"),
        P("ep", None, "tp"),
        P("ep", "tp", None),
        P(None, "tp"),
        P(None, "tp"),
        P("tp", None),
    )
    return jax.shard_map(
        chosen, mesh=mesh, in_specs=placed, out_specs=(P("ep", "tp"), P("ep", "tp")), check_vma=False
    )
```
